256 devices in a mesh: ep: 128 (over z, y, x), tp: 2 (over core).
Axes of the slice: x: 4, y: 4, z: 8, core: 2. Of those that a mesh axis runs over, the one named last changes fastest.
Arguments:
- tokens: bfloat16 [256, 2048], P('ep'), may hold values from -6 to 6
- head_state: float32 [256, 32, 64, 128], P('ep', 'tp'), may hold values from -4 to 4
- conv_state: bfloat16 [256, 3, 2048], P('ep', None, 'tp'), may hold values from -6 to 6
- conv_proj_state: bfloat16 [256, 3, 2, 512], P('ep', None, None, 'tp'), may hold values from -6 to 6
- first_gain: float32 [2048], replicated, may hold values from 0.1 to 1.9
- gate_weight: bfloat16 [2048, 2048], P('ep', 'tp'), may hold values from -0.125 to 0.125
- inner_weight: bfloat16 [2048, 2048], P('ep', 'tp'), may hold values from -0.125 to 0.125
- write_weight: bfloat16 [2048, 512], P(None, 'tp'), may hold values from -0.125 to 0.125
- read_weight: bfloat16 [2048, 512], P(None, 'tp'), may hold values from -0.125 to 0.125
- step_weight: bfloat16 [2048, 32], P(None, 'tp'), may hold values from -0.125 to 0.125
- conv_kernel: float32 [4, 2048], P(None, 'tp'), may hold values from -3 to 3
- conv_proj_kernel: float32 [4, 2, 512], P(None, None, 'tp'), may hold values from -3 to 3
- step_bias: float32 [32], P('tp'), may hold values from -2 to 1
- log_rate: float32 [32], P('tp'), may hold values from -4.5 to 1.5
- skip_gain: float32 [32], P('tp'), may hold values from 0.5 to 2
- group_gain: float32 [2048], P('tp'), may hold values from 0.1 to 1.9
- out_weight: bfloat16 [2048, 2048], P('tp', 'ep'), may hold values from -0.125 to 0.125
- second_gain: float32 [2048], replicated, may hold values from 0.1 to 1.9
- routes: int32 [256, 4], P('ep'), may hold values from 0 to 127, all different within a row; in each aligned block of 256 rows (0 to 255, 256 to 511, ...) at most 32 rows name the same one
- route_logits: bfloat16 [256, 4], P('ep'), may hold values from -8 to 300
- expert_gate: bfloat16 [128, 2048, 1024], P('ep', None, 'tp'), may hold values from -0.5 to 0.5
- expert_up: bfloat16 [128, 2048, 1024], P('ep', None, 'tp'), may hold values from -0.5 to 0.5
- expert_down: bfloat16 [128, 1024, 2048], P('ep', 'tp'), may hold values from -0.0234375 to 0.0234375
- dense_up: bfloat16 [2048, 4096], P(None, ('ep', 'tp')), may hold values from -0.125 to 0.125
- dense_down: bfloat16 [4096, 2048], P(('ep', 'tp')), may hold values from -0.09375 to 0.09375
- dense_gate: float32 [2048], replicated, may hold values from -0.125 to 0.125
Outputs:
- layer_out: bfloat16 [256, 2048], P(('ep', 'tp'))
- state_out: float32 [256, 32, 64, 128], P('ep', 'tp')
- conv_out: bfloat16 [256, 3, 2048], P('ep', None, 'tp')
- conv_proj_out: bfloat16 [256, 3, 2, 512], P('ep', None, None, 'tp')
The draws below stay inside these ranges and needn't reach their ends.
Inputs may be any that keep to these rules, and one draw needn't show every extreme that they name: `routes`: each token names 4 different experts; over the whole batch no expert is named by more than 32 rows, a bound that some block reaches.
All inputs are finite; a program needn't handle non-finite values.
Results may differ from the reference program's by a relative error of at most 0.015.
Values may be sent and summed in bfloat16 or wider, within the bound.
A program may use at most 64 MiB of HBM per device.

```python
import math
import jax
import jax.numpy as jnp
import numpy as np
from jax import lax

D = 2048
HEADS = 32
HEAD_DIM = 64
STATE = 128
GROUPS = 4
KCONV = 4
DE = 1024
FD = 4096
TOPK = 4
INNER = 2048
GS = 512
EXPERTS = 128
TOKENS = 256
CAPACITY = 32


def draw_log_rate(key, part):
    return jax.random.uniform(key, (HEADS,), jnp.float32, -3.5, 1.5)


def draw_route_logits(key, part):
    base_key = jax.random.fold_in(key, 11)
    values = jnp.clip(1.5 * jax.random.normal(base_key, (TOKENS, TOPK), jnp.float32), -6.0, 6.0)
    return values.astype(jnp.bfloat16)


def steps_of(key, dims, split, low, high):
    level = 1.0
    for axis_at, parts in split:
        heights = jax.random.uniform(jax.random.fold_in(jax.random.fold_in(key, 6), axis_at), (parts,), jnp.float32, low / len(split), high / len(split))
        level = level * jnp.repeat(jnp.exp(heights), dims[axis_at] // parts).reshape((-1,) + (1,) * (len(dims) - 1 - axis_at))
    return level


def deal_out(stream_key, own, number, rows, amount, top, bound, slope):
    order = jax.random.permutation(stream_key, amount)
    packed, common = shares(amount, rows * top, bound, slope, True), shares(amount, rows * top, bound, slope, False)
    places = jnp.arange(amount)

    def named(sizes, rotation):
        used = int((sizes > 0).sum())
        fixed = max(1, used // 4)
        moved = fixed + (places - fixed + rotation * (used - fixed)) % max(1, amount - fixed)
        return jnp.zeros((amount,), jnp.int32).at[order[jnp.where(places < fixed, places, moved)]].set(jnp.asarray(sizes, jnp.int32))

    sizes = jnp.where(number % 4 == 0, named(packed, number // 4), named(common, number - number // 4 - 1))
    mixed = jax.random.permutation(jax.random.fold_in(own, 3), amount)
    giver, taker = mixed[0:amount // 2 * 2:2], mixed[1:amount // 2 * 2:2]
    room = jnp.minimum(sizes[giver] - 1, bound - sizes[taker]) // 2
    room = jnp.where((giver == order[0]) | (taker == order[0]) | (sizes[taker] == 0), 0, jnp.maximum(room, 0))
    moved = jax.random.randint(jax.random.fold_in(own, 4), (amount // 2,), 0, 1 << 20) % (room + 1)
    sizes = sizes.at[giver].add(-moved).at[taker].add(moved)
    items = jnp.searchsorted(jnp.cumsum(sizes), jnp.arange(rows * top), side="right").astype(jnp.int32)
    grid = items.reshape(top, rows).T
    grid = grid[jax.random.permutation(jax.random.fold_in(own, 1), rows)]
    rotation = jax.random.randint(jax.random.fold_in(own, 2), (rows, 1), 0, top)
    return jnp.take_along_axis(grid, (jnp.arange(top)[None, :] + rotation) % top, axis=1)


def shares(count, total, bound, skew, full):
    weights = [(1 << 20) // math.isqrt(rank ** skew) + 1 for rank in range(1, count + 1)]
    largest = bound if full else min(bound, max(-(-total // count), total * weights[0] // sum(weights)))
    least = 1 if total - largest >= count - 1 else 0
    holding, rest = [largest] + [least] * (count - 1), total - largest - least * (count - 1)
    while rest > 0:
        free = [i for i in range(1, count) if holding[i] < largest] or [i for i in range(1, count) if holding[i] < bound]
        mass, remaining = sum([weights[i] for i in free]), rest
        for i in free:
            addition = min(bound - holding[i], max(1, remaining * weights[i] // mass), rest)
            holding[i] = holding[i] + addition
            rest = rest - addition
    return np.array(holding)


def centred(key, extent, width, limit, cuts=(), kind=jnp.bfloat16):
    array = jax.random.normal(key, extent, jnp.float32) * width
    if len(cuts) > 0:
        array = steps_of(key, extent, cuts, -0.22, 0.18) * array
    return jnp.clip(array, min=-limit, max=limit).astype(kind)


def setup_inputs(seed: int = 0) -> dict:
    streams_of = jax.random.split(jax.random.key(seed), 27)
    tokens = centred(streams_of[0], (TOKENS, D), 1.0, 6.0, ((0, 128),))
    head_state = centred(streams_of[1], (TOKENS, HEADS, HEAD_DIM, STATE), 0.5, 4.0, ((0, 128), (1, 2)), jnp.float32)
    conv_state = centred(streams_of[2], (TOKENS, KCONV - 1, INNER), 1.0, 6.0, ((0, 128), (2, 2)))
    conv_proj_state = centred(streams_of[3], (TOKENS, KCONV - 1, 2, GS), 1.0, 6.0, ((0, 128), (3, 2)))
    first_gain = jnp.clip(1.0 + 0.18 * jax.random.normal(streams_of[4], (D,), jnp.float32), 0.1, 1.9)
    gate_weight = centred(streams_of[5], (D, INNER), D ** -0.5, 0.125, ((0, 128), (1, 2)))
    inner_weight = centred(streams_of[6], (D, INNER), D ** -0.5, 0.125, ((0, 128), (1, 2)))
    write_weight = centred(streams_of[7], (D, GS), D ** -0.5, 0.125, ((1, 2),))
    read_weight = centred(streams_of[8], (D, GS), D ** -0.5, 0.125, ((1, 2),))
    step_weight = centred(streams_of[9], (D, HEADS), D ** -0.5, 0.125, ((1, 2),))
    conv_kernel = centred(streams_of[10], (KCONV, INNER), 0.5, 3.0, ((1, 2),), jnp.float32)
    conv_proj_kernel = centred(streams_of[11], (KCONV, 2, GS), 0.5, 3.0, ((2, 2),), jnp.float32)
    step_bias = jnp.clip(-2.0 + 3.0 * jax.random.uniform(streams_of[12], (HEADS,), jnp.float32) ** steps_of(streams_of[12], (HEADS,), ((0, 2),), -0.2, 0.2), -2.0, 1.0)
    log_rate = draw_log_rate(jax.random.fold_in(streams_of[26], 71), 0)
    skip_gain = jnp.clip(0.5 + 1.5 * jax.random.uniform(streams_of[14], (HEADS,), jnp.float32) ** steps_of(streams_of[14], (HEADS,), ((0, 2),), -0.2, 0.2), 0.5, 2.0)
    group_gain = jnp.clip(1.0 + 0.18 * jax.random.normal(streams_of[15], (INNER,), jnp.float32), 0.1, 1.9)
    out_weight = centred(streams_of[16], (INNER, D), INNER ** -0.5, 0.125, ((0, 2), (1, 128)))
    second_gain = jnp.clip(1.0 + 0.18 * jax.random.normal(streams_of[17], (D,), jnp.float32), 0.1, 1.9)
    routes_keys = jax.random.split(jax.random.fold_in(streams_of[18], 1), TOKENS // TOKENS)
    routes_turns = jax.random.permutation(jax.random.fold_in(streams_of[18], 3), TOKENS // TOKENS)
    routes = jax.vmap(lambda own, number: deal_out(jax.random.fold_in(streams_of[18], 2), own, number, TOKENS, EXPERTS, TOPK, CAPACITY, 2))(routes_keys, routes_turns).reshape((TOKENS, TOPK))
    route_logits = draw_route_logits(jax.random.fold_in(streams_of[26], 71), 0)
    expert_gate = centred(streams_of[20], (EXPERTS, D, DE), (D // 16) ** -0.5, 0.5, ((0, 128), (2, 2)))
    expert_up = centred(streams_of[21], (EXPERTS, D, DE), (D // 16) ** -0.5, 0.5, ((0, 128), (2, 2)))
    expert_down = centred(streams_of[22], (EXPERTS, DE, D), (DE * 64) ** -0.5, 0.0234375, ((0, 128), (1, 2)))
    dense_up = centred(streams_of[23], (D, FD), D ** -0.5, 0.125, ((1, 256),))
    dense_down = centred(streams_of[24], (FD, D), FD ** -0.5, 0.09375, ((0, 256),))
    dense_gate = centred(streams_of[25], (D,), D ** -0.5, 0.125, (), jnp.float32)
    return dict(tokens=tokens, head_state=head_state, conv_state=conv_state, conv_proj_state=conv_proj_state, first_gain=first_gain, gate_weight=gate_weight, inner_weight=inner_weight, write_weight=write_weight, read_weight=read_weight, step_weight=step_weight, conv_kernel=conv_kernel, conv_proj_kernel=conv_proj_kernel, step_bias=step_bias, log_rate=log_rate, skip_gain=skip_gain, group_gain=group_gain, out_weight=out_weight, second_gain=second_gain, routes=routes, route_logits=route_logits, expert_gate=expert_gate, expert_up=expert_up, expert_down=expert_down, dense_up=dense_up, dense_down=dense_down, dense_gate=dense_gate)


norm_eps = 1e-05
clamp_limit = 7.0
glu_alpha = 1.702
highest = lax.Precision.HIGHEST

def rms_scale(values, gain_vec):
    return values * lax.rsqrt(lax.optimization_barrier(jnp.mean(values * values, axis=-1, keepdims=True)) + norm_eps) * gain_vec

def clamped_unit(gate_pre, up_pre):
    glu_part = jnp.minimum(gate_pre, clamp_limit)
    lin_part = jnp.clip(up_pre, -clamp_limit, clamp_limit)
    return glu_part * jax.nn.sigmoid(glu_alpha * glu_part) * (lin_part + 1.0)

def state_step(inner_proj, gate_proj, write_proj, read_proj, step_raw, conv_state, conv_proj_state, conv_kernel, conv_proj_kernel, step_bias, log_rate, skip_gain, group_gain, head_state, group_count):
    window_inner = jnp.concatenate([conv_state, inner_proj[:, None, :]], axis=1)
    window_proj = jnp.concatenate([conv_proj_state, jnp.stack([write_proj, read_proj], axis=1)[:, None]], axis=1)
    conv_inner = jax.nn.silu(lax.optimization_barrier(jnp.sum(window_inner.astype(jnp.float32) * conv_kernel[None], axis=1)))
    conv_proj = jax.nn.silu(lax.optimization_barrier(jnp.sum(window_proj.astype(jnp.float32) * conv_proj_kernel[None], axis=1)))
    seq_count, channels = conv_inner.shape
    head_count = step_raw.shape[1]
    head_width = channels // head_count
    state_width = conv_proj.shape[2] // group_count
    per_group = head_count // group_count
    head_input = conv_inner.reshape(seq_count, head_count, head_width)
    write_heads = jnp.repeat(conv_proj[:, 0].reshape(seq_count, group_count, state_width), per_group, axis=1)
    read_heads = jnp.repeat(conv_proj[:, 1].reshape(seq_count, group_count, state_width), per_group, axis=1)
    step_size = jax.nn.softplus(step_raw + step_bias)
    decay_rate = jnp.exp(-jnp.exp(log_rate) * step_size)
    state_out = decay_rate[:, :, None, None] * head_state + (step_size[:, :, None] * head_input)[:, :, :, None] * write_heads[:, :, None, :]
    read_out = jnp.einsum('shpn,shn->shp', state_out, read_heads, precision=highest) + skip_gain[None, :, None] * head_input
    gated_rows = read_out.reshape(seq_count, channels) * jax.nn.silu(gate_proj.astype(jnp.float32))
    grouped = gated_rows.reshape(seq_count, group_count, channels // group_count)
    grouped = grouped * lax.rsqrt(lax.optimization_barrier(jnp.mean(grouped * grouped, axis=-1, keepdims=True)) + norm_eps)
    mixer_rows = (grouped.reshape(seq_count, channels) * group_gain).astype(jnp.bfloat16)
    return (mixer_rows, state_out, window_inner[:, 1:], window_proj[:, 1:])

def reference(tokens, head_state, conv_state, conv_proj_state, first_gain, gate_weight, inner_weight, write_weight, read_weight, step_weight, conv_kernel, conv_proj_kernel, step_bias, log_rate, skip_gain, group_gain, out_weight, second_gain, routes, route_logits, expert_gate, expert_up, expert_down, dense_up, dense_down, dense_gate):
    normed_in = rms_scale(tokens.astype(jnp.float32), first_gain).astype(jnp.bfloat16)
    gate_proj = jnp.dot(normed_in, gate_weight, preferred_element_type=jnp.float32).astype(jnp.bfloat16)
    inner_proj = jnp.dot(normed_in, inner_weight, preferred_element_type=jnp.float32).astype(jnp.bfloat16)
    write_proj = jnp.dot(normed_in, write_weight, preferred_element_type=jnp.float32).astype(jnp.bfloat16)
    read_proj = jnp.dot(normed_in, read_weight, preferred_element_type=jnp.float32).astype(jnp.bfloat16)
    step_raw = jnp.dot(normed_in, step_weight, preferred_element_type=jnp.float32)
    mixer_rows, state_out, conv_out, conv_proj_out = state_step(inner_proj, gate_proj, write_proj, read_proj, step_raw, conv_state, conv_proj_state, conv_kernel, conv_proj_kernel, step_bias, log_rate, skip_gain, group_gain, head_state, GROUPS)
    mixed = jnp.dot(mixer_rows, out_weight, preferred_element_type=jnp.float32)
    hidden = (tokens.astype(jnp.float32) + mixed).astype(jnp.bfloat16)
    normed_mid = rms_scale(hidden.astype(jnp.float32), second_gain).astype(jnp.bfloat16)
    route_gates = jax.nn.softmax(route_logits.astype(jnp.float32), axis=-1)
    row_ids = jnp.arange(TOKENS, dtype=jnp.int32)

    def expert_pass(running, inputs):
        gate_block, up_block, down_block, expert_id = inputs
        route_hits = routes == expert_id
        row_weight = lax.optimization_barrier(jnp.sum(jnp.where(route_hits, route_gates, 0.0), axis=1))
        chosen = jnp.any(route_hits, axis=1)
        picked = jnp.argsort(jnp.where(chosen, row_ids, row_ids + TOKENS)).astype(jnp.int32)[:CAPACITY]
        picked_rows = normed_mid[picked]
        activated = clamped_unit(jnp.dot(picked_rows, gate_block, preferred_element_type=jnp.float32), jnp.dot(picked_rows, up_block, preferred_element_type=jnp.float32)).astype(jnp.bfloat16)
        expert_rows = jnp.dot(activated, down_block, preferred_element_type=jnp.float32) * row_weight[picked][:, None]
        return (running.at[picked].add(expert_rows), None)
    expert_ids = jnp.arange(EXPERTS, dtype=jnp.int32)
    expert_mix = lax.scan(expert_pass, jnp.zeros((TOKENS, D), jnp.float32), (expert_gate, expert_up, expert_down, expert_ids))[0]
    dense_act = jax.nn.silu(jnp.dot(normed_mid, dense_up, preferred_element_type=jnp.float32)).astype(jnp.bfloat16)
    dense_weight = jax.nn.sigmoid(jnp.dot(normed_mid.astype(jnp.float32), dense_gate, precision=highest))
    dense_value = jnp.dot(dense_act, dense_down, preferred_element_type=jnp.float32)
    layer_out = (hidden.astype(jnp.float32) + expert_mix + dense_weight[:, None] * dense_value).astype(jnp.bfloat16)
    return (layer_out, state_out, conv_out, conv_proj_out)
```

```python
import functools

import jax
import jax.numpy as jnp
from jax import lax
from jax.experimental import pallas as pl
from jax.experimental.pallas import tpu as pltpu
from jax.sharding import Mesh
from jax.sharding import PartitionSpec as P

EP = ("ep_0", "ep_1", "ep_2")
EP_TP = ("ep_0", "ep_1", "ep_2", "tp")
MESH = pl.DeviceIdType.MESH
F32 = jnp.float32
BF16 = jnp.bfloat16
norm_eps = 1e-05
clamp_limit = 7.0
glu_alpha = 1.702
highest = lax.Precision.HIGHEST
NZ, NY, NX = 8, 4, 4
NZY, NYX = NZ * NY, NY * NX


sigmoid = jax.nn.sigmoid
silu = jax.nn.silu


def softplus(v):
    return jnp.maximum(v, 0.0) + jnp.log1p(jnp.exp(-jnp.abs(v)))


def dot(a, b, ca=1, cb=0, precision=None):
    return lax.dot_general(
        a, b, (((ca,), (cb,)), ((), ())), precision=precision, preferred_element_type=F32
    )


def rms_scale(values, gain_vec):
    return values * lax.rsqrt(jnp.mean(values * values, axis=-1, keepdims=True) + norm_eps) * gain_vec


def layer_kernel(
    tokens, conv_state, conv_proj_state, first_gain, step_weight, conv_kernel, conv_proj_kernel,
    step_bias, log_rate, skip_gain, group_gain, out_weight, second_gain, routing, dense_up,
    dense_down, dense_gate,
    head_state, gate_weight, inner_weight, write_weight, read_weight, expert_gate, expert_up,
    expert_down,
    layer_out, inner_out, proj_out, state_out,
    hs, ww, rw, eg, eu, ed, wg, wi, nblk, tok, psend_i, psend_g, precv_i, precv_g, rts, wo, mx,
    osend, orecv, rows, ddp, dact, dactp, epart, epartp, tsum, prs, fsend, frecv,
    lsem, ssem, rsem, planesem,
):
    z, y, x, c = [lax.axis_index(n) for n in EP_TP]
    zy = z * NY + y
    yx = y * NX + x
    zc = z * 2 + c
    expert = zy * NX + x
    base = yx * NZ
    other = 1 - c
    partner = (z, y, x, other)

    def zy_dev(i):
        return (i // NY, i % NY, x, c)

    def yx_dev(i):
        return (z, i // NX, i % NX, c)

    def zc_dev(i):
        return (i // 2, y, x, i % 2)

    def send(src, dst, s, r, device):
        pltpu.make_async_remote_copy(
            src_ref=src, dst_ref=dst, send_sem=s, recv_sem=r, device_id=device, device_id_type=MESH
        ).start()

    def landed(ref, sem):
        pltpu.make_async_copy(ref, ref, sem).wait()

    def around(me, n, fn):
        def step(r, carry):
            fn((me + r) % n)
            return carry

        lax.fori_loop(1, n, step, 0)

    loads = [
        (write_weight, ww), (read_weight, rw), (head_state, hs), (expert_gate.at[0], eg),
        (expert_up.at[0], eu), (expert_down.at[0], ed), (gate_weight, wg.at[x]),
        (inner_weight, wi.at[x]),
    ]
    copies = [pltpu.make_async_copy(a, b, lsem.at[i]) for i, (a, b) in enumerate(loads)]
    for i in (7, 6, 0, 1, 2, 3, 4, 5):
        copies[i].start()

    barrier = pltpu.get_barrier_semaphore()

    def hello(device):
        pl.semaphore_signal(barrier, inc=1, device_id=device, device_id_type=MESH)

    around(zy, NZY, lambda i: hello(zy_dev(i)))
    around(yx, NYX, lambda i: hello(yx_dev(i)))
    around(z, NZ, lambda i: hello((i, y, x, other)))
    hello(partner)

    normed = rms_scale(tokens[...].astype(F32), first_gain[...]).astype(BF16)
    for b in range(16):
        nblk[b] = normed[:, b * 128 : (b + 1) * 128]
    tok[zy] = nblk[zy // 2]
    rts[base + z] = routing[...]
    wo[yx] = jnp.transpose(out_weight[...])

    pl.semaphore_wait(barrier, (NZY - 1) + (NYX - 1) + (NZ - 1) + 1)

    around(zy, NZY, lambda i: send(nblk.at[i // 2], tok.at[zy], ssem.at[0], rsem.at[0], zy_dev(i)))
    around(x, NX, lambda i: send(inner_weight, wi.at[x], ssem.at[1], rsem.at[1], (z, y, i, c)))
    around(x, NX, lambda i: send(gate_weight, wg.at[x], ssem.at[2], rsem.at[2], (z, y, i, c)))
    around(z, NZ, lambda i: send(rts.at[base + z], rts.at[base + z], ssem.at[3], rsem.at[3], (i, y, x, c)))

    copies[0].wait()
    copies[1].wait()
    write_proj = dot(normed, ww[...]).astype(BF16)
    read_proj = dot(normed, rw[...]).astype(BF16)
    step_raw = dot(normed, step_weight[...])
    proj_out[0] = write_proj
    proj_out[1] = read_proj

    copies[6].wait()
    copies[7].wait()
    landed(tok.at[pl.ds(0, NZY - 1)], rsem.at[0])
    landed(wi.at[pl.ds(0, NX - 1)], rsem.at[1])
    all_tok = tok.reshape(2 * NZY, 128)[...]
    low = (y % 2) == 0

    def padded(weight):
        zero = jnp.zeros_like(weight)
        return jnp.concatenate([jnp.where(low, weight, zero), jnp.where(low, zero, weight)], axis=0)

    psend_i.reshape(2 * NZY, 1024)[...] = dot(all_tok, padded(wi.reshape(64, 1024)[...])).astype(BF16)
    around(zy, NZY, lambda i: send(psend_i.at[i], precv_i.at[zy], ssem.at[4], rsem.at[4], zy_dev(i)))
    precv_i[zy] = psend_i[zy]
    landed(wg.at[pl.ds(0, NX - 1)], rsem.at[2])
    psend_g.reshape(2 * NZY, 1024)[...] = dot(all_tok, padded(wg.reshape(64, 1024)[...])).astype(BF16)
    around(zy, NZY, lambda i: send(psend_g.at[i], precv_g.at[zy], ssem.at[5], rsem.at[5], zy_dev(i)))
    precv_g[zy] = psend_g[zy]
    landed(rts.at[pl.ds(0, NZ - 1)], rsem.at[3])
    mine8 = pl.ds(base, NZ)
    around(yx, NYX, lambda i: send(rts.at[mine8], rts.at[mine8], ssem.at[6], rsem.at[6], yx_dev(i)))
    around(yx, NYX, lambda i: send(wo.at[yx], wo.at[yx], ssem.at[7], rsem.at[7], yx_dev(i)))
    send(dense_down.at[other], ddp, ssem.at[8], rsem.at[8], partner)

    cps = conv_proj_state[...].astype(F32)
    cpk = conv_proj_kernel[...]

    def conv_of(w, fresh):
        total = fresh.astype(F32) * cpk[3, w : w + 1]
        for i in range(3):
            total = total + cps[:, i, w, :] * cpk[i, w : w + 1]
        return silu(total)

    write_vec = conv_of(0, write_proj)
    read_vec = conv_of(1, read_proj)
    step_size = softplus(step_raw + step_bias[...])
    decay = jnp.exp(-jnp.exp(log_rate[...]) * step_size)
    head_of = lax.broadcasted_iota(jnp.int32, (16, 1024), 1) // 64
    spread = (head_of == lax.broadcasted_iota(jnp.int32, (16, 1024), 0)).astype(F32)
    step_wide = dot(step_size, spread, precision=highest)
    skip_wide = dot(skip_gain[...], spread, precision=highest)
    cs = conv_state[...].astype(F32)
    ck = conv_kernel[...]
    early = cs[:, 0, :] * ck[0:1] + cs[:, 1, :] * ck[1:2] + cs[:, 2, :] * ck[2:3]
    copies[2].wait()

    landed(precv_i.at[pl.ds(0, NZY - 1)], rsem.at[4])
    inner_proj = jnp.sum(precv_i[...].astype(F32), axis=0).astype(BF16)
    inner_out[...] = inner_proj
    conv_inner = silu(early + inner_proj.astype(F32) * ck[3:4])
    driven = step_wide * conv_inner
    first_row = lax.broadcasted_iota(jnp.int32, (8, 512), 0) == 0
    read_rows = []
    for s in range(2):
        for g in range(2):
            lhs = jnp.where(first_row, driven[s : s + 1, g * 512 : (g + 1) * 512], 0.0)
            rhs = jnp.broadcast_to(write_vec[s : s + 1, g * 128 : (g + 1) * 128], (8, 128))
            update = dot(lhs, rhs, 0, 0, highest).reshape(8, 64, 128)
            blocks = []
            for h in range(8):
                head = g * 8 + h
                rate = jnp.broadcast_to(decay[s : s + 1, head : head + 1], (64, 128))
                fresh = rate * hs[s, head] + update[h]
                hs[s, head] = fresh
                blocks.append(fresh)
            group = jnp.concatenate(blocks, axis=0)
            reader = jnp.broadcast_to(read_vec[s : s + 1, g * 128 : (g + 1) * 128], (8, 128))
            read_rows.append(dot(reader, group, 1, 1, highest)[0:1])
    state_copy = pltpu.make_async_copy(hs, state_out, lsem.at[2])
    state_copy.start()
    read_out = jnp.concatenate(
        [jnp.concatenate(read_rows[0:2], axis=1), jnp.concatenate(read_rows[2:4], axis=1)], axis=0
    ) + skip_wide * conv_inner

    landed(precv_g.at[pl.ds(0, NZY - 1)], rsem.at[5])
    gate_proj = jnp.sum(precv_g[...].astype(F32), axis=0).astype(BF16)
    gated = read_out * silu(gate_proj.astype(F32))
    parts = []
    for g in range(2):
        part = gated[:, g * 512 : (g + 1) * 512]
        parts.append(part * lax.rsqrt(jnp.mean(part * part, axis=-1, keepdims=True) + norm_eps))
    mx[z] = (jnp.concatenate(parts, axis=1) * group_gain[...]).astype(BF16)
    around(z, NZ, lambda i: send(mx.at[z], mx.at[z], ssem.at[9], rsem.at[9], (i, y, x, c)))

    landed(rts.at[pl.ds(0, 120)], rsem.at[6])
    table = rts.reshape(256, 256)[...].astype(F32)
    names, scores = table[:, 0:128], table[:, 128:256]
    lane = lax.broadcasted_iota(jnp.int32, (256, 128), 1)
    live = lane < 4
    hit = jnp.where(live & (names == expert.astype(F32)), 1.0, 0.0)
    shifted = jnp.where(live, scores, -3e38)
    grown = jnp.where(live, jnp.exp(shifted - jnp.max(shifted, axis=1, keepdims=True)), 0.0)
    row_weight = jnp.sum(hit * grown, axis=1, keepdims=True) / jnp.sum(grown, axis=1, keepdims=True)
    chosen = jnp.broadcast_to(jnp.sum(hit, axis=1, keepdims=True), (256, 128))
    rr = lax.broadcasted_iota(jnp.int32, (256, 256), 0)
    cc = lax.broadcasted_iota(jnp.int32, (256, 256), 1)
    chosen16 = chosen.astype(BF16)
    count_col = dot((cc <= rr).astype(BF16), chosen16)
    count_row = dot(chosen16, (rr <= cc).astype(BF16), 0, 0)[0:32]
    chosen_row = dot(chosen16, (rr == cc).astype(BF16), 0, 0)[0:32]
    slot = lax.broadcasted_iota(jnp.int32, (32, 256), 0).astype(F32)
    picks = jnp.where((count_row - 1.0 == slot) & (chosen_row > 0.5), 1.0, 0.0)
    picks_t = jnp.where((count_col - 1.0 == lane.astype(F32)) & (chosen > 0.5), 1.0, 0.0)
    slot_weight = dot(picks, jnp.broadcast_to(row_weight, (256, 128)), precision=highest)[:, 0:1]
    picks16 = picks.astype(BF16)

    landed(wo.at[pl.ds(0, NYX - 1)], rsem.at[7])
    landed(mx.at[pl.ds(0, NZ - 1)], rsem.at[9])
    osend.reshape(16, 256)[...] = dot(mx.reshape(16, 1024)[...], wo.reshape(256, 1024)[...], 1, 1)
    around(zc, 2 * NZ, lambda i: send(osend.at[i // 2], orecv.at[zc], ssem.at[10], rsem.at[10], zc_dev(i)))
    orecv[zc] = osend[z]
    landed(orecv.at[pl.ds(0, 15)], rsem.at[10])
    mixed = jnp.concatenate([orecv[2 * k] + orecv[2 * k + 1] for k in range(NZ)], axis=1)
    hidden = (tokens[...].astype(F32) + mixed).astype(BF16)
    normed_mid = rms_scale(hidden.astype(F32), second_gain[...]).astype(BF16)
    rows[c, base + z] = jnp.where(c == 0, normed_mid[:, 0:1024], normed_mid[:, 1024:2048])
    around(z, NZ, lambda i: send(rows.at[c, base + z], rows.at[c, base + z], ssem.at[11], rsem.at[11], (i, y, x, c)))
    landed(rows.at[c, pl.ds(0, NZ - 1)], rsem.at[11])
    around(yx, NYX, lambda i: send(rows.at[c, mine8], rows.at[c, mine8], ssem.at[12], planesem.at[yx], yx_dev(i)))
    send(rows.at[c, mine8], rows.at[c, mine8], ssem.at[13], rsem.at[13], partner)

    def forward(r, carry):
        i = (yx + NYX - r) % NYX
        block = rows.at[c, pl.ds(i * NZ, NZ)]
        landed(block, planesem.at[i])
        send(block, block, ssem.at[13], rsem.at[13], partner)
        return carry

    lax.fori_loop(1, NYX, forward, 0)
    copies[3].wait()
    copies[4].wait()
    copies[5].wait()
    landed(rows.at[other], rsem.at[13])

    halves = [rows[k].reshape(256, 1024) for k in range(2)]
    gate_line = dense_gate[...]
    g_hi = gate_line.astype(BF16)
    g_mid = (gate_line - g_hi.astype(F32)).astype(BF16)
    g_lo = (gate_line - g_hi.astype(F32) - g_mid.astype(F32)).astype(BF16)
    lines = jnp.concatenate([g_hi, g_mid, g_lo, jnp.zeros((5, 2048), BF16)], axis=0)
    picked = [dot(picks16, halves[k]).astype(BF16) for k in range(2)]
    gate_pre = dot(picked[0], eg[0:1024]) + dot(picked[1], eg[1024:2048])
    up_pre = dot(picked[0], eu[0:1024]) + dot(picked[1], eu[1024:2048])
    glu_part = jnp.minimum(gate_pre, clamp_limit)
    lin_part = jnp.clip(up_pre, -clamp_limit, clamp_limit)
    activated = (glu_part * sigmoid(glu_alpha * glu_part) * (lin_part + 1.0)).astype(BF16)
    part = dot(activated, ed[...]) * slot_weight
    epart[...] = jnp.where(c == 0, part[:, 1024:2048], part[:, 0:1024]).astype(BF16)
    send(epart, epartp, ssem.at[14], rsem.at[14], partner)
    own_part = jnp.where(c == 0, part[:, 0:1024], part[:, 1024:2048])
    up = dense_up[...]
    pre = dot(halves[0], up[0:1024]) + dot(halves[1], up[1024:2048])
    weigh = dot(halves[0], lines[:, 0:1024], 1, 1) + dot(halves[1], lines[:, 1024:2048], 1, 1)
    weight = sigmoid(jnp.sum(weigh, axis=1, keepdims=True))
    dense_act = silu(pre).astype(BF16).astype(F32) * weight
    dact[...] = dense_act.astype(BF16)
    send(dact, dactp, ssem.at[15], rsem.at[15], partner)
    landed(ddp, rsem.at[8])
    landed(epartp, rsem.at[14])
    both = (own_part + epartp[...].astype(F32)).astype(BF16)
    landed(dactp, rsem.at[15])
    left = jnp.concatenate([dact[...], dactp[...], picks_t[:, 0:32].astype(BF16)], axis=1)
    own_down = jnp.where(c == 0, dense_down[0], dense_down[1])
    right = jnp.concatenate([own_down, ddp[...], both], axis=0)
    tsum.reshape(256, 1024)[...] = dot(left, right).astype(BF16)

    around(yx, NYX, lambda i: send(tsum.at[pl.ds(i * NZ, NZ)], prs.at[yx], ssem.at[16], rsem.at[16], yx_dev(i)))
    prs[yx] = tsum[mine8]
    landed(prs.at[pl.ds(0, NYX - 1)], rsem.at[16])
    fsend[...] = jnp.sum(prs[...].astype(F32), axis=0).astype(BF16)
    around(zc, 2 * NZ, lambda i: send(fsend.at[i // 2], frecv.at[zc], ssem.at[17], rsem.at[17], zc_dev(i)))
    frecv[zc] = fsend[z]
    landed(frecv.at[pl.ds(0, 15)], rsem.at[17])
    final = []
    for k in range(2):
        total = frecv[k].astype(F32)
        for i in range(1, NZ):
            total = total + frecv[2 * i + k].astype(F32)
        final.append(total)
    result = hidden.astype(F32) + jnp.concatenate(final, axis=1)
    layer_out[...] = jnp.where(c == 0, result[0:1], result[1:2]).astype(BF16)

    state_copy.wait()
    for i, ref in enumerate((
        tok.at[pl.ds(0, NZY - 1)], wi.at[pl.ds(0, NX - 1)], wg.at[pl.ds(0, NX - 1)],
        rts.at[pl.ds(0, NZ - 1)], psend_i.at[pl.ds(0, NZY - 1)], psend_g.at[pl.ds(0, NZY - 1)],
        rts.at[pl.ds(0, 120)], wo.at[pl.ds(0, NYX - 1)], ddp, mx.at[pl.ds(0, NZ - 1)],
        orecv.at[pl.ds(0, 15)], mx.at[pl.ds(0, NZ - 1)], rows.at[0, pl.ds(0, 120)], rows.at[0],
        epart, dact, prs.at[pl.ds(0, NYX - 1)], frecv.at[pl.ds(0, 15)],
    )):
        landed(ref, ssem.at[i])


def local(
    tokens, head_state, conv_state, conv_proj_state, first_gain, gate_weight, inner_weight,
    write_weight, read_weight, step_weight, conv_kernel, conv_proj_kernel, step_bias, log_rate,
    skip_gain, group_gain, out_weight, second_gain, routes, route_logits, expert_gate, expert_up,
    expert_down, dense_up, dense_down, dense_gate,
):
    wide = ((0, 0), (0, 124))
    routing = jnp.concatenate(
        [jnp.pad(routes.astype(BF16), wide), jnp.pad(route_logits, wide)], axis=1
    )
    near = [
        tokens, conv_state, conv_proj_state, first_gain[None], step_weight, conv_kernel,
        conv_proj_kernel, step_bias[None], log_rate[None], skip_gain[None], group_gain[None],
        out_weight, second_gain[None], routing, dense_up,
        jnp.stack([dense_down[:, 0:1024], dense_down[:, 1024:2048]]), dense_gate[None],
    ]
    far = [
        head_state, gate_weight, inner_weight, write_weight, read_weight, expert_gate, expert_up,
        expert_down,
    ]
    vmem = pl.BlockSpec(memory_space=pltpu.VMEM)
    anywhere = pl.BlockSpec(memory_space=pl.ANY)
    V = pltpu.VMEM
    layer_out, inner_proj, proj, state_out = pl.pallas_call(
        layer_kernel,
        out_shape=(
            jax.ShapeDtypeStruct((1, 2048), BF16),
            jax.ShapeDtypeStruct((2, 1024), BF16),
            jax.ShapeDtypeStruct((2, 2, 256), BF16),
            jax.ShapeDtypeStruct((2, 16, 64, 128), F32),
        ),
        in_specs=[vmem] * len(near) + [anywhere] * len(far),
        out_specs=(vmem, vmem, vmem, anywhere),
        scratch_shapes=[
            V((2, 16, 64, 128), F32), V((2048, 256), BF16), V((2048, 256), BF16),
            V((2048, 512), BF16), V((2048, 512), BF16), V((512, 2048), BF16),
            V((NX, 16, 1024), BF16), V((NX, 16, 1024), BF16),
            V((16, 2, 128), BF16), V((NZY, 2, 128), BF16),
            V((NZY, 2, 1024), BF16), V((NZY, 2, 1024), BF16),
            V((NZY, 2, 1024), BF16), V((NZY, 2, 1024), BF16),
            V((128, 2, 256), BF16), V((NYX, 16, 1024), BF16), V((NZ, 2, 1024), BF16),
            V((NZ, 2, 256), F32), V((2 * NZ, 2, 256), F32),
            V((2, 128, 2, 1024), BF16), V((16, 1024), BF16), V((256, 16), BF16), V((256, 16), BF16),
            V((32, 1024), BF16), V((32, 1024), BF16),
            V((128, 2, 1024), BF16), V((NYX, NZ, 2, 1024), BF16), V((NZ, 2, 1024), BF16),
            V((2 * NZ, 2, 1024), BF16),
            pltpu.SemaphoreType.DMA((8,)), pltpu.SemaphoreType.DMA((18,)),
            pltpu.SemaphoreType.DMA((18,)), pltpu.SemaphoreType.DMA((NYX,)),
        ],
        compiler_params=pltpu.CompilerParams(
            collective_id=0, has_side_effects=True, vmem_limit_bytes=56 * 1024 * 1024
        ),
        cost_estimate=pl.CostEstimate(flops=2 * 10**9, bytes_accessed=16 * 2**20, transcendentals=10**5),
        name="layer",
    )(*near, *far)
    conv_out = jnp.concatenate([conv_state[:, 1:], inner_proj[:, None]], axis=1)
    conv_proj_out = jnp.concatenate(
        [conv_proj_state[:, 1:], jnp.stack([proj[0], proj[1]], axis=1)[:, None]], axis=1
    )
    return (layer_out, state_out, conv_out, conv_proj_out)


def solution(mesh):
    torus = Mesh(mesh.devices.reshape(NZ, NY, NX, mesh.shape["tp"]), EP_TP)
    return jax.shard_map(
        local,
        mesh=torus,
        in_specs=(
            P(EP, None), P(EP, "tp", None, None), P(EP, None, "tp"), P(EP, None, None, "tp"), P(),
            P(EP, "tp"), P(EP, "tp"), P(None, "tp"), P(None, "tp"), P(None, "tp"), P(None, "tp"),
            P(None, None, "tp"), P("tp"), P("tp"), P("tp"), P("tp"), P("tp", EP), P(), P(EP, None),
            P(EP, None), P(EP, None, "tp"), P(EP, None, "tp"), P(EP, "tp", None), P(None, EP_TP),
            P(EP_TP, None), P(),
        ),
        out_specs=(
            P(EP_TP, None), P(EP, "tp", None, None), P(EP, None, "tp"), P(EP, None, None, "tp"),
        ),
        check_vma=False,
    )
```

```python
import functools

import jax
import jax.numpy as jnp
from jax import lax
from jax.experimental import pallas as pl
from jax.experimental.pallas import tpu as pltpu
from jax.sharding import Mesh
from jax.sharding import PartitionSpec as P

EP = ("ep_0", "ep_1", "ep_2")
EP_TP = ("ep_0", "ep_1", "ep_2", "tp")
MESH = pl.DeviceIdType.MESH
F32 = jnp.float32
BF16 = jnp.bfloat16
norm_eps = 1e-05
clamp_limit = 7.0
glu_alpha = 1.702
highest = lax.Precision.HIGHEST
NZ, NY, NX = 8, 4, 4
NZY, NYX = NZ * NY, NY * NX


sigmoid = jax.nn.sigmoid
silu = jax.nn.silu


def softplus(v):
    return jnp.maximum(v, 0.0) + jnp.log1p(jnp.exp(-jnp.abs(v)))


def dot(a, b, ca=1, cb=0, precision=None):
    return lax.dot_general(
        a, b, (((ca,), (cb,)), ((), ())), precision=precision, preferred_element_type=F32
    )


def rms_scale(values, gain_vec):
    return values * lax.rsqrt(jnp.mean(values * values, axis=-1, keepdims=True) + norm_eps) * gain_vec


NEAR = 17


def layer_kernel(*refs):
    near_hbm, refs = refs[:NEAR], refs[NEAR:]
    (
        out_weight, head_state, gate_weight, inner_weight, write_weight, read_weight, expert_gate,
        expert_up, expert_down, layer_out, conv_out, conv_proj_out, hs,
    ) = refs[:13]
    near, refs = refs[13 : 13 + NEAR], refs[13 + NEAR :]
    (
        tokens, first_gain, step_weight, conv_state, conv_proj_state, conv_kernel, conv_proj_kernel,
        step_bias, log_rate, skip_gain, group_gain, second_gain, routes, route_logits, dense_up,
        dense_down, dense_gate,
    ) = near
    (
        ww, rw, eg, eu, ed, wg, wi, nblk, tok, psend_i, psend_g, precv_i, precv_g, rts, wo, mx,
        osend, orecv, tkz, hid, rows, ddp, dact, dactp, epart, epartp, tsum, prs, fsend, frecv,
        nsem, lsem, ssem, rsem, planesem,
    ) = refs
    z, y, x, c = [lax.axis_index(n) for n in EP_TP]
    zy = z * NY + y
    yx = y * NX + x
    zc = z * 2 + c
    expert = zy * NX + x
    base = yx * NZ
    other = 1 - c
    partner = (z, y, x, other)

    def zy_dev(i):
        return (i // NY, i % NY, x, c)

    def yx_dev(i):
        return (z, i // NX, i % NX, c)

    def pair_dev(i):
        return (z, i // (2 * NX), (i // 2) % NX, i % 2)

    def zc_dev(i):
        return (i // 2, y, x, i % 2)

    def send(src, dst, s, r, device):
        pltpu.make_async_remote_copy(
            src_ref=src, dst_ref=dst, send_sem=s, recv_sem=r, device_id=device, device_id_type=MESH
        ).start()

    def landed(ref, sem, name="tail"):
        with jax.named_scope(name):
            pltpu.make_async_copy(ref, ref, sem).wait()

    def around(me, n, fn):
        def step(r, carry):
            fn((me + r) % n)
            return carry

        lax.fori_loop(1, n, step, 0)

    barrier = pltpu.get_barrier_semaphore()

    def hello(device):
        pl.semaphore_signal(barrier, inc=1, device_id=device, device_id_type=MESH)

    around(zy, NZY, lambda i: hello(zy_dev(i)))
    around(yx * 2 + c, 2 * NYX, lambda i: hello(pair_dev(i)))
    around(z, NZ, lambda i: hello((i, y, x, other)))

    small = [pltpu.make_async_copy(a, b, nsem.at[i]) for i, (a, b) in enumerate(zip(near_hbm, near))]
    loads = [
        (write_weight, ww), (read_weight, rw), (head_state, hs), (expert_gate.at[0], eg),
        (expert_up.at[0], eu), (expert_down.at[0], ed), (gate_weight, wg.at[x]),
        (inner_weight, wi.at[x]),
    ]
    copies = [pltpu.make_async_copy(a, b, lsem.at[i]) for i, (a, b) in enumerate(loads)]
    for copy in small:
        copy.start()
    for i in (7, 6, 0, 1, 2, 3, 4, 5):
        copies[i].start()
    small[0].wait()
    small[1].wait()

    normed = rms_scale(tokens[...].astype(F32), first_gain[...]).astype(BF16)
    for b in range(16):
        nblk[b] = normed[:, b * 128 : (b + 1) * 128]
    tok[zy] = nblk[zy // 2]
    tkz[z] = tokens[...]
    small[12].wait()
    small[13].wait()
    blank = jnp.zeros((2, 124), F32)
    rts[base + z] = jnp.concatenate(
        [routes[...].astype(F32), blank, route_logits[...].astype(F32), blank], axis=1
    ).astype(BF16)

    with jax.named_scope("barrier"):
        pl.semaphore_wait(barrier, (NZY - 1) + (2 * NYX - 1) + (NZ - 1))

    around(zy, NZY, lambda i: send(nblk.at[i // 2], tok.at[zy], ssem.at[0], rsem.at[0], zy_dev(i)))
    around(x, NX, lambda i: send(inner_weight, wi.at[x], ssem.at[1], rsem.at[1], (z, y, i, c)))
    around(x, NX, lambda i: send(gate_weight, wg.at[x], ssem.at[2], rsem.at[2], (z, y, i, c)))
    around(z, NZ, lambda i: send(rts.at[base + z], rts.at[base + z], ssem.at[3], rsem.at[3], (i, y, x, c)))
    around(z, NZ, lambda i: send(tkz.at[z], tkz.at[z], ssem.at[11], rsem.at[11], (i, y, x, c)))
    keeper = yx // 8
    place = wo.at[c, yx % 8]

    def columns(r, carry):
        i = (yx + r) % NYX
        send(out_weight, place, ssem.at[7], rsem.at[7], (z, i // NX, i % NX, keeper))
        return carry

    lax.fori_loop(1, NYX, columns, 0)

    @pl.when(keeper == c)
    def _():
        pltpu.make_async_copy(out_weight, place, rsem.at[7]).start()

    @pl.when(keeper != c)
    def _():
        send(out_weight, place, ssem.at[7], rsem.at[7], partner)

    for copy in small[2:12] + small[14:]:
        copy.wait()

    with jax.named_scope("ww"):
        copies[0].wait()
        copies[1].wait()
    write_proj = dot(normed, ww[...]).astype(BF16)
    read_proj = dot(normed, rw[...]).astype(BF16)
    step_raw = dot(normed, step_weight[...], 1, 1)

    copies[6].wait()
    copies[7].wait()
    landed(tok.at[pl.ds(0, NZY - 1)], rsem.at[0], "tok")
    landed(wi.at[pl.ds(0, NX - 1)], rsem.at[1], "wi")
    all_tok = tok.reshape(2 * NZY, 128)[...]
    low = (y % 2) == 0

    def padded(weight):
        zero = jnp.zeros_like(weight)
        return jnp.concatenate([jnp.where(low, weight, zero), jnp.where(low, zero, weight)], axis=0)

    psend_i.reshape(2 * NZY, 1024)[...] = dot(all_tok, padded(wi.reshape(64, 1024)[...])).astype(BF16)
    around(zy, NZY, lambda i: send(psend_i.at[i], precv_i.at[zy], ssem.at[4], rsem.at[4], zy_dev(i)))
    precv_i[zy] = psend_i[zy]
    landed(wg.at[pl.ds(0, NX - 1)], rsem.at[2], "wg")
    psend_g.reshape(2 * NZY, 1024)[...] = dot(all_tok, padded(wg.reshape(64, 1024)[...])).astype(BF16)
    around(zy, NZY, lambda i: send(psend_g.at[i], precv_g.at[zy], ssem.at[5], rsem.at[5], zy_dev(i)))
    precv_g[zy] = psend_g[zy]
    landed(rts.at[pl.ds(0, NZ - 1)], rsem.at[3], "rt_z")
    mine8 = pl.ds(base, NZ)
    around(yx, NYX, lambda i: send(rts.at[mine8], rts.at[mine8], ssem.at[6], rsem.at[6], yx_dev(i)))
    send(dense_down.at[:, pl.ds(pl.multiple_of(other * 1024, 1024), 1024)], ddp, ssem.at[8], rsem.at[8], partner)

    cps = conv_proj_state[...].astype(F32)
    cpk = conv_proj_kernel[...]

    def conv_of(w, fresh):
        total = fresh.astype(F32) * cpk[3, w : w + 1]
        for i in range(3):
            total = total + cps[:, i, w, :] * cpk[i, w : w + 1]
        return silu(total)

    write_vec = conv_of(0, write_proj)
    read_vec = conv_of(1, read_proj)
    step_size = softplus(step_raw + step_bias[...])
    decay = jnp.exp(-jnp.exp(log_rate[...]) * step_size)
    head_of = lax.broadcasted_iota(jnp.int32, (16, 1024), 1) // 64
    spread = (head_of == lax.broadcasted_iota(jnp.int32, (16, 1024), 0)).astype(F32)
    step_wide = dot(step_size, spread, precision=highest)
    skip_wide = dot(skip_gain[...], spread, precision=highest)
    decay_wide = dot(decay, spread, precision=highest)
    ck = conv_kernel[...]
    early = sum(conv_state[i].astype(F32) * ck[i : i + 1] for i in range(3))
    for i in range(2):
        conv_out[i] = conv_state[i + 1]
        conv_proj_out[:, i] = conv_proj_state[:, i + 1]
    for s in range(2):
        conv_proj_out[s, 2] = jnp.concatenate([write_proj[s : s + 1], read_proj[s : s + 1]], axis=0)
    copies[2].wait()
    held, met = [], []
    for s in range(2):
        for g in range(2):
            span = slice(g * 128, (g + 1) * 128)
            reader = read_vec[s : s + 1, span]
            group = hs[s, g * 8 : (g + 1) * 8].reshape(512, 128)
            held.append(dot(jnp.broadcast_to(reader, (8, 128)), group, 1, 1, highest)[0:1])
            product = jnp.sum(write_vec[s : s + 1, span] * reader, axis=1, keepdims=True)
            met.append(jnp.broadcast_to(product, (1, 512)))

    def by_sequence(four):
        return jnp.concatenate(
            [jnp.concatenate(four[0:2], axis=1), jnp.concatenate(four[2:4], axis=1)], axis=0
        )

    kept = decay_wide * by_sequence(held)
    direct = step_wide * by_sequence(met) + skip_wide

    landed(precv_i.at[pl.ds(0, NZY - 1)], rsem.at[4], "p_inner")
    inner_proj = jnp.sum(precv_i[...].astype(F32), axis=0).astype(BF16)
    conv_out[2] = inner_proj
    conv_inner = silu(early + inner_proj.astype(F32) * ck[3:4])
    read_out = kept + direct * conv_inner

    landed(precv_g.at[pl.ds(0, NZY - 1)], rsem.at[5], "p_gate")
    gate_proj = jnp.sum(precv_g[...].astype(F32), axis=0).astype(BF16)
    gated = read_out * silu(gate_proj.astype(F32))
    parts = []
    for g in range(2):
        part = gated[:, g * 512 : (g + 1) * 512]
        parts.append(part * lax.rsqrt(jnp.mean(part * part, axis=-1, keepdims=True) + norm_eps))
    mx[c, z] = (jnp.concatenate(parts, axis=1) * group_gain[...]).astype(BF16)
    around(zc, 2 * NZ, lambda i: send(mx.at[c, z], mx.at[c, z], ssem.at[9], rsem.at[9], zc_dev(i)))

    landed(rts.at[pl.ds(0, 120)], rsem.at[6], "rt_yx")
    table = rts.reshape(256, 256)[...].astype(F32)
    names, scores = table[:, 0:128], table[:, 128:256]
    lane = lax.broadcasted_iota(jnp.int32, (256, 128), 1)
    live = lane < 4
    hit = jnp.where(live & (names == expert.astype(F32)), 1.0, 0.0)
    shifted = jnp.where(live, scores, -3e38)
    grown = jnp.where(live, jnp.exp(shifted - jnp.max(shifted, axis=1, keepdims=True)), 0.0)
    row_weight = jnp.sum(hit * grown, axis=1, keepdims=True) / jnp.sum(grown, axis=1, keepdims=True)
    chosen = jnp.broadcast_to(jnp.sum(hit, axis=1, keepdims=True), (256, 128))
    rr = lax.broadcasted_iota(jnp.int32, (256, 256), 0)
    cc = lax.broadcasted_iota(jnp.int32, (256, 256), 1)
    chosen16 = chosen.astype(BF16)
    count_col = dot((cc <= rr).astype(BF16), chosen16)
    count_row = dot(chosen16, (rr <= cc).astype(BF16), 0, 0)[0:32]
    chosen_row = dot(chosen16, (rr == cc).astype(BF16), 0, 0)[0:32]
    slot = lax.broadcasted_iota(jnp.int32, (32, 256), 0).astype(F32)
    picks = jnp.where((count_row - 1.0 == slot) & (chosen_row > 0.5), 1.0, 0.0)
    picks_t = jnp.where((count_col - 1.0 == lane.astype(F32)) & (chosen > 0.5), 1.0, 0.0)
    slot_weight = dot(picks, jnp.broadcast_to(row_weight, (256, 128)), precision=highest)[:, 0:1]
    picks16 = picks.astype(BF16)

    landed(wo, rsem.at[7], "wo")
    landed(frecv.at[pl.ds(0, 15)], rsem.at[9], "mixer")
    columns_out = [dot(mx[k].reshape(16, 1024), wo[k].reshape(128, 1024), 1, 1) for k in range(2)]
    osend[...] = (columns_out[0] + columns_out[1]).astype(BF16)
    around(zc, 2 * NZ, lambda i: send(osend, orecv.at[zc], ssem.at[10], rsem.at[10], zc_dev(i)))
    orecv[zc] = osend[...]
    landed(tkz.at[pl.ds(0, NZ - 1)], rsem.at[11], "tkz")
    landed(orecv.at[pl.ds(0, 15)], rsem.at[10], "out")
    mixed = jnp.concatenate([orecv[k].astype(F32) for k in range(2 * NZ)], axis=1)
    hidden = (tkz[...].reshape(16, 2048).astype(F32) + mixed).astype(BF16)
    hid[...] = hidden.reshape(NZ, 2, 2048)
    normed_mid = rms_scale(hidden.astype(F32), second_gain[...]).astype(BF16)
    for k in range(2):
        rows[k, mine8] = normed_mid[:, k * 1024 : (k + 1) * 1024].reshape(NZ, 2, 1024)
    around(yx, NYX, lambda i: send(rows.at[c, mine8], rows.at[c, mine8], ssem.at[12], planesem.at[yx], yx_dev(i)))

    driven = step_wide * conv_inner
    first_row = lax.broadcasted_iota(jnp.int32, (8, 512), 0) == 0
    for s in range(2):
        for g in range(2):
            lhs = jnp.where(first_row, driven[s : s + 1, g * 512 : (g + 1) * 512], 0.0)
            rhs = jnp.broadcast_to(write_vec[s : s + 1, g * 128 : (g + 1) * 128], (8, 128))
            update = dot(lhs, rhs, 0, 0, highest).reshape(8, 64, 128)
            for h in range(8):
                head = g * 8 + h
                rate = jnp.broadcast_to(decay[s : s + 1, head : head + 1], (64, 128))
                hs[s, head] = rate * hs[s, head] + update[h]

    def forward(r, carry):
        i = (yx + NYX - r) % NYX
        block = rows.at[c, pl.ds(i * NZ, NZ)]
        landed(block, planesem.at[i], "rows_yx")
        send(block, block, ssem.at[13], rsem.at[13], partner)
        return carry

    lax.fori_loop(1, NYX, forward, 0)
    copies[3].wait()
    copies[4].wait()
    copies[5].wait()

    gate_line = dense_gate[...]
    g_hi = gate_line.astype(BF16)
    g_mid = (gate_line - g_hi.astype(F32)).astype(BF16)
    g_lo = (gate_line - g_hi.astype(F32) - g_mid.astype(F32)).astype(BF16)
    lines = jnp.concatenate([g_hi, g_mid, g_lo, jnp.zeros((5, 2048), BF16)], axis=0)
    lines = jnp.stack([lines[:, 0:1024], lines[:, 1024:2048]])

    def half_terms(k):
        half = rows[k].reshape(256, 1024)
        span = pl.ds(pl.multiple_of(k * 1024, 1024), 1024)
        picked = dot(picks16, half).astype(BF16)
        line = jnp.where(k == 0, lines[0], lines[1])
        return (
            dot(picked, eg[span]), dot(picked, eu[span]), dot(half, dense_up[:, span], 1, 1),
            dot(half, line, 1, 1),
        )

    own_terms = half_terms(c)
    landed(rows.at[other, pl.ds(0, 120)], rsem.at[13], "rows_d2d")
    gate_pre, up_pre, pre, weigh = [a + b for a, b in zip(own_terms, half_terms(other))]
    glu_part = jnp.minimum(gate_pre, clamp_limit)
    lin_part = jnp.clip(up_pre, -clamp_limit, clamp_limit)
    activated = (glu_part * sigmoid(glu_alpha * glu_part) * (lin_part + 1.0)).astype(BF16)
    part = dot(activated, ed[...]) * slot_weight
    epart[...] = jnp.where(c == 0, part[:, 1024:2048], part[:, 0:1024]).astype(BF16)
    send(epart, epartp, ssem.at[14], rsem.at[14], partner)
    own_part = jnp.where(c == 0, part[:, 0:1024], part[:, 1024:2048])
    weight = sigmoid(jnp.sum(weigh, axis=1, keepdims=True))
    dense_act = silu(pre).astype(BF16).astype(F32) * weight
    dact[...] = dense_act.astype(BF16)
    send(dact, dactp, ssem.at[15], rsem.at[15], partner)
    landed(ddp, rsem.at[8], "ddp")
    landed(epartp, rsem.at[14], "epart")
    both = (own_part + epartp[...].astype(F32)).astype(BF16)
    landed(dactp, rsem.at[15], "dact")
    left = jnp.concatenate([dact[...], dactp[...], picks_t[:, 0:32].astype(BF16)], axis=1)
    own_down = jnp.where(c == 0, dense_down[:, 0:1024], dense_down[:, 1024:2048])
    right = jnp.concatenate([own_down, ddp[...], both], axis=0)
    tsum.reshape(256, 1024)[...] = dot(left, right).astype(BF16)

    around(yx, NYX, lambda i: send(tsum.at[pl.ds(i * NZ, NZ)], prs.at[yx], ssem.at[16], rsem.at[16], yx_dev(i)))
    prs[yx] = tsum[mine8]
    landed(prs.at[pl.ds(0, NYX - 1)], rsem.at[16], "sum_yx")
    fsend[...] = jnp.sum(prs[...].astype(F32), axis=0).astype(BF16)
    around(zc, 2 * NZ, lambda i: send(fsend.at[i // 2], frecv.at[zc], ssem.at[17], rsem.at[17], zc_dev(i)))
    frecv[zc] = fsend[z]
    landed(frecv.at[pl.ds(0, 15)], rsem.at[17], "sum_z")
    final = []
    for k in range(2):
        total = frecv[k].astype(F32)
        for i in range(1, NZ):
            total = total + frecv[2 * i + k].astype(F32)
        final.append(total)
    result = hid[z].astype(F32) + jnp.concatenate(final, axis=1)
    layer_out[...] = jnp.where(c == 0, result[0:1], result[1:2]).astype(BF16)

    for i, ref in enumerate((
        tok.at[pl.ds(0, NZY - 1)], wi.at[pl.ds(0, NX - 1)], wg.at[pl.ds(0, NX - 1)],
        rts.at[pl.ds(0, NZ - 1)], psend_i.at[pl.ds(0, NZY - 1)], psend_g.at[pl.ds(0, NZY - 1)],
        rts.at[pl.ds(0, 120)], None, ddp, frecv.at[pl.ds(0, 15)],
        orecv.at[pl.ds(0, 15)], tkz.at[pl.ds(0, NZ - 1)], rows.at[0, pl.ds(0, 120)],
        rows.at[0, pl.ds(0, 120)],
        epart, dact, prs.at[pl.ds(0, NYX - 1)], frecv.at[pl.ds(0, 15)],
    )):
        if ref is not None:
            landed(ref, ssem.at[i])

    @pl.when(keeper == c)
    def _():
        landed(prs.at[pl.ds(0, NYX - 1)], ssem.at[7])

    @pl.when(keeper != c)
    def _():
        landed(wo, ssem.at[7])


def local(
    tokens, head_state, conv_state, conv_proj_state, first_gain, gate_weight, inner_weight,
    write_weight, read_weight, step_weight, conv_kernel, conv_proj_kernel, step_bias, log_rate,
    skip_gain, group_gain, out_weight, second_gain, routes, route_logits, expert_gate, expert_up,
    expert_down, dense_up, dense_down, dense_gate,
):
    near = [
        tokens, first_gain[None], step_weight.T, conv_state.transpose(1, 0, 2), conv_proj_state,
        conv_kernel, conv_proj_kernel, step_bias[None], log_rate[None], skip_gain[None],
        group_gain[None], second_gain[None], routes, route_logits, dense_up.T, dense_down,
        dense_gate[None],
    ]
    far = [
        out_weight.T, head_state, gate_weight, inner_weight, write_weight, read_weight, expert_gate,
        expert_up, expert_down,
    ]
    vmem = pl.BlockSpec(memory_space=pltpu.VMEM)
    anywhere = pl.BlockSpec(memory_space=pltpu.HBM)
    V = pltpu.VMEM
    outs = (
        jax.ShapeDtypeStruct((1, 2048), BF16),
        jax.ShapeDtypeStruct((3, 2, 1024), BF16),
        jax.ShapeDtypeStruct((2, 3, 2, 256), BF16),
        jax.ShapeDtypeStruct((2, 16, 64, 128), F32),
    )
    layer_out, conv_out, conv_proj_out, state_out = pl.pallas_call(
        layer_kernel,
        out_shape=tuple(V(o.shape, o.dtype) for o in outs),
        in_specs=[anywhere] * (len(near) + len(far)),
        out_specs=(vmem, vmem, vmem, vmem),
        scratch_shapes=[
            *[V(a.shape, a.dtype) for a in near],
            V((2048, 256), BF16), V((2048, 256), BF16),
            V((2048, 512), BF16), V((2048, 512), BF16), V((512, 2048), BF16),
            V((NX, 16, 1024), BF16), V((NX, 16, 1024), BF16),
            V((16, 2, 128), BF16), V((NZY, 2, 128), BF16),
            V((NZY, 2, 1024), BF16), V((NZY, 2, 1024), BF16),
            V((NZY, 2, 1024), BF16), V((NZY, 2, 1024), BF16),
            V((128, 2, 256), BF16), V((2, 8, 16, 1024), BF16), V((2, NZ, 2, 1024), BF16),
            V((16, 128), BF16), V((2 * NZ, 16, 128), BF16), V((NZ, 2, 2048), BF16), V((NZ, 2, 2048), BF16),
            V((2, 128, 2, 1024), BF16), V((16, 1024), BF16), V((256, 16), BF16), V((256, 16), BF16),
            V((32, 1024), BF16), V((32, 1024), BF16),
            V((128, 2, 1024), BF16), V((NYX, NZ, 2, 1024), BF16), V((NZ, 2, 1024), BF16),
            V((2 * NZ, 2, 1024), BF16),
            pltpu.SemaphoreType.DMA((NEAR,)), pltpu.SemaphoreType.DMA((8,)), pltpu.SemaphoreType.DMA((18,)),
            pltpu.SemaphoreType.DMA((18,)), pltpu.SemaphoreType.DMA((NYX,)),
        ],
        compiler_params=pltpu.CompilerParams(
            collective_id=0, has_side_effects=True, vmem_limit_bytes=56 * 1024 * 1024
        ),
        cost_estimate=pl.CostEstimate(flops=2 * 10**9, bytes_accessed=16 * 2**20, transcendentals=10**5),
        name="layer",
    )(*near, *far)
    return (layer_out, state_out, conv_out.transpose(1, 0, 2), conv_proj_out)


def solution(mesh):
    torus = Mesh(mesh.devices.reshape(NZ, NY, NX, mesh.shape["tp"]), EP_TP)
    return jax.shard_map(
        local,
        mesh=torus,
        in_specs=(
            P(EP, None), P(EP, "tp", None, None), P(EP, None, "tp"), P(EP, None, None, "tp"), P(),
            P(EP, "tp"), P(EP, "tp"), P(None, "tp"), P(None, "tp"), P(None, "tp"), P(None, "tp"),
            P(None, None, "tp"), P("tp"), P("tp"), P("tp"), P("tp"), P("tp", EP), P(), P(EP, None),
            P(EP, None), P(EP, None, "tp"), P(EP, None, "tp"), P(EP, "tp", None), P(None, EP_TP),
            P(EP_TP, None), P(),
        ),
        out_specs=(
            P(EP_TP, None), P(EP, "tp", None, None), P(EP, None, "tp"), P(EP, None, None, "tp"),
        ),
        check_vma=False,
    )
```

```python
import functools

import jax
import jax.numpy as jnp
from jax import lax
from jax.experimental import pallas as pl
from jax.experimental.pallas import tpu as pltpu
from jax.sharding import Mesh
from jax.sharding import PartitionSpec as P

EP = ("ep_0", "ep_1", "ep_2")
EP_TP = ("ep_0", "ep_1", "ep_2", "tp")
MESH = pl.DeviceIdType.MESH
F32 = jnp.float32
BF16 = jnp.bfloat16
norm_eps = 1e-05
clamp_limit = 7.0
glu_alpha = 1.702
highest = lax.Precision.HIGHEST
NZ, NY, NX = 8, 4, 4
NZY, NYX = NZ * NY, NY * NX


sigmoid = jax.nn.sigmoid
silu = jax.nn.silu


def softplus(v):
    return jnp.maximum(v, 0.0) + jnp.log1p(jnp.exp(-jnp.abs(v)))


def dot(a, b, ca=1, cb=0, precision=None):
    return lax.dot_general(
        a, b, (((ca,), (cb,)), ((), ())), precision=precision, preferred_element_type=F32
    )


def rms_scale(values, gain_vec):
    return values * lax.rsqrt(jnp.mean(values * values, axis=-1, keepdims=True) + norm_eps) * gain_vec


NEAR = 17


def layer_kernel(*refs):
    near_hbm, refs = refs[:NEAR], refs[NEAR:]
    (
        out_weight, head_state, gate_weight, inner_weight, write_weight, read_weight, expert_gate,
        expert_up, expert_down, layer_out, conv_out, conv_proj_out, hs,
    ) = refs[:13]
    near, refs = refs[13 : 13 + NEAR], refs[13 + NEAR :]
    (
        tokens, first_gain, step_weight, conv_state, conv_proj_state, conv_kernel, conv_proj_kernel,
        step_bias, log_rate, skip_gain, group_gain, second_gain, routes, route_logits, dense_up,
        dense_down, dense_gate,
    ) = near
    (
        ww, rw, eg, eu, ed, wg, wi, nblk, tok, psend_i, psend_g, precv_i, precv_g, rts, wo, mx,
        osend, orecv, tkz, hid, rows, ddp, dact, dactp, epart, epartp, tsum, prs, fsend, frecv,
        pt, upl, pbuf, dterm, nsem, lsem, ssem, rsem, planesem, fsem,
    ) = refs
    z, y, x, c = [lax.axis_index(n) for n in EP_TP]
    zy = z * NY + y
    yx = y * NX + x
    zc = z * 2 + c
    expert = zy * NX + x
    base = yx * NZ
    other = 1 - c
    partner = (z, y, x, other)

    z_at = [lax.rem(z + d, NZ) for d in range(NZ)]
    y_at = [lax.rem(y + d, NY) for d in range(NY)]
    x_at = [lax.rem(x + d, NX) for d in range(NX)]
    c_at = [c, other]
    zy_peers = [(z_at[d], y_at[e]) for d in (4, 3, 5, 2, 6, 1, 7, 0) for e in (2, 1, 3, 0)][:-1]
    yx_peers = [(y_at[d], x_at[e]) for d in (2, 1, 3, 0) for e in (2, 1, 3, 0)][:-1]
    zc_peers = [(z_at[d], c_at[e]) for d in (4, 3, 5, 2, 6, 1, 7, 0) for e in (1, 0)][:-1]
    z_peers = [z_at[d] for d in (4, 3, 5, 2, 6, 1, 7)]

    def send(src, dst, s, r, device):
        pltpu.make_async_remote_copy(
            src_ref=src, dst_ref=dst, send_sem=s, recv_sem=r, device_id=device, device_id_type=MESH
        ).start()

    def landed(ref, sem, name="tail"):
        with jax.named_scope(name):
            pltpu.make_async_copy(ref, ref, sem).wait()

    barrier = pltpu.get_barrier_semaphore()

    def hello(device):
        pl.semaphore_signal(barrier, inc=1, device_id=device, device_id_type=MESH)

    for k, j in zy_peers:
        hello((k, j, x, c))
    for j, i in yx_peers:
        hello((z, j, i, c))
        hello((z, j, i, other))
    hello(partner)
    for k in z_peers:
        hello((k, y, x, other))

    small = [pltpu.make_async_copy(a, b, nsem.at[i]) for i, (a, b) in enumerate(zip(near_hbm, near))]
    loads = [
        (write_weight, ww), (read_weight, rw), (head_state, hs), (expert_gate.at[0], eg),
        (expert_up.at[0], eu), (expert_down.at[0], ed), (gate_weight, wg.at[x]),
        (inner_weight, wi.at[x]),
    ]
    copies = [pltpu.make_async_copy(a, b, lsem.at[i]) for i, (a, b) in enumerate(loads)]
    for copy in small:
        copy.start()
    for i in (7, 6, 0, 1, 2, 3, 4, 5):
        copies[i].start()
    small[0].wait()
    small[1].wait()

    normed = rms_scale(tokens[...].astype(F32), first_gain[...]).astype(BF16)
    for b in range(16):
        nblk[b] = normed[:, b * 128 : (b + 1) * 128]
    tok[zy] = nblk[zy // 2]
    tkz[z] = tokens[...]
    small[12].wait()
    small[13].wait()
    blank = jnp.zeros((2, 124), F32)
    rts[base + z] = jnp.concatenate(
        [routes[...].astype(F32), blank, route_logits[...].astype(F32), blank], axis=1
    ).astype(BF16)

    with jax.named_scope("barrier"):
        pl.semaphore_wait(barrier, (NZY - 1) + (2 * NYX - 1) + (NZ - 1))

    for k, j in zy_peers:
        send(nblk.at[k * 2 + j // 2], tok.at[zy], ssem.at[0], rsem.at[0], (k, j, x, c))
    for k in z_peers:
        send(rts.at[base + z], rts.at[base + z], ssem.at[3], rsem.at[3], (k, y, x, c))
    for i in (x_at[2], x_at[1], x_at[3]):
        send(inner_weight, wi.at[x], ssem.at[1], rsem.at[1], (z, y, i, c))
    for i in (x_at[2], x_at[1], x_at[3]):
        send(gate_weight, wg.at[x], ssem.at[2], rsem.at[2], (z, y, i, c))
    for k in z_peers:
        send(tkz.at[z], tkz.at[z], ssem.at[11], rsem.at[11], (k, y, x, c))
    keeper = yx // 8
    place = wo.at[c, yx % 8]

    for j, i in yx_peers:
        send(out_weight, place, ssem.at[7], rsem.at[7], (z, j, i, keeper))

    @pl.when(keeper == c)
    def _():
        pltpu.make_async_copy(out_weight, place, rsem.at[7]).start()

    @pl.when(keeper != c)
    def _():
        send(out_weight, place, ssem.at[7], rsem.at[7], partner)

    for copy in small[2:12] + small[14:]:
        copy.wait()

    with jax.named_scope("ww"):
        copies[0].wait()
        copies[1].wait()
    write_proj = dot(normed, ww[...]).astype(BF16)
    read_proj = dot(normed, rw[...]).astype(BF16)
    step_raw = dot(normed, step_weight[...], 1, 1)

    copies[6].wait()
    copies[7].wait()
    landed(tok.at[pl.ds(0, NZY - 1)], rsem.at[0], "tok")
    landed(rts.at[pl.ds(0, NZ - 1)], rsem.at[3], "rt_z")
    mine8 = pl.ds(base, NZ)
    for j, i in yx_peers:
        send(rts.at[mine8], rts.at[mine8], ssem.at[6], rsem.at[6], (z, j, i, c))
    landed(wi.at[pl.ds(0, NX - 1)], rsem.at[1], "wi")
    all_tok = tok.reshape(2 * NZY, 128)[...]
    low = (y % 2) == 0

    def padded(weight):
        zero = jnp.zeros_like(weight)
        return jnp.concatenate([jnp.where(low, weight, zero), jnp.where(low, zero, weight)], axis=0)

    psend_i.reshape(2 * NZY, 1024)[...] = dot(all_tok, padded(wi.reshape(64, 1024)[...])).astype(BF16)
    for k, j in zy_peers:
        send(psend_i.at[k * NY + j], precv_i.at[zy], ssem.at[4], rsem.at[4], (k, j, x, c))
    precv_i[zy] = psend_i[zy]
    landed(wg.at[pl.ds(0, NX - 1)], rsem.at[2], "wg")
    psend_g.reshape(2 * NZY, 1024)[...] = dot(all_tok, padded(wg.reshape(64, 1024)[...])).astype(BF16)
    for k, j in zy_peers:
        send(psend_g.at[k * NY + j], precv_g.at[zy], ssem.at[5], rsem.at[5], (k, j, x, c))
    precv_g[zy] = psend_g[zy]
    send(dense_down.at[:, pl.ds(pl.multiple_of(other * 1024, 1024), 1024)], ddp, ssem.at[8], rsem.at[8], partner)

    cps = conv_proj_state[...].astype(F32)
    cpk = conv_proj_kernel[...]

    def conv_of(w, fresh):
        total = fresh.astype(F32) * cpk[3, w : w + 1]
        for i in range(3):
            total = total + cps[:, i, w, :] * cpk[i, w : w + 1]
        return silu(total)

    write_vec = conv_of(0, write_proj)
    read_vec = conv_of(1, read_proj)
    step_size = softplus(step_raw + step_bias[...])
    decay = jnp.exp(-jnp.exp(log_rate[...]) * step_size)
    head_of = lax.broadcasted_iota(jnp.int32, (16, 1024), 1) // 64
    spread = (head_of == lax.broadcasted_iota(jnp.int32, (16, 1024), 0)).astype(F32)
    step_wide = dot(step_size, spread, precision=highest)
    skip_wide = dot(skip_gain[...], spread, precision=highest)
    decay_wide = dot(decay, spread, precision=highest)
    ck = conv_kernel[...]
    early = sum(conv_state[i].astype(F32) * ck[i : i + 1] for i in range(3))
    for i in range(2):
        conv_out[i] = conv_state[i + 1]
        conv_proj_out[:, i] = conv_proj_state[:, i + 1]
    for s in range(2):
        conv_proj_out[s, 2] = jnp.concatenate([write_proj[s : s + 1], read_proj[s : s + 1]], axis=0)
    copies[2].wait()
    held, met = [], []
    for s in range(2):
        for g in range(2):
            span = slice(g * 128, (g + 1) * 128)
            reader = read_vec[s : s + 1, span]
            group = hs[s, g * 8 : (g + 1) * 8].reshape(512, 128)
            held.append(dot(jnp.broadcast_to(reader, (8, 128)), group, 1, 1, highest)[0:1])
            product = jnp.sum(write_vec[s : s + 1, span] * reader, axis=1, keepdims=True)
            met.append(jnp.broadcast_to(product, (1, 512)))

    def by_sequence(four):
        return jnp.concatenate(
            [jnp.concatenate(four[0:2], axis=1), jnp.concatenate(four[2:4], axis=1)], axis=0
        )

    kept = decay_wide * by_sequence(held)
    direct = step_wide * by_sequence(met) + skip_wide

    landed(precv_i.at[pl.ds(0, NZY - 1)], rsem.at[4], "p_inner")
    inner_proj = jnp.sum(precv_i[...].astype(F32), axis=0).astype(BF16)
    conv_out[2] = inner_proj
    conv_inner = silu(early + inner_proj.astype(F32) * ck[3:4])
    read_out = kept + direct * conv_inner

    landed(precv_g.at[pl.ds(0, NZY - 1)], rsem.at[5], "p_gate")
    gate_proj = jnp.sum(precv_g[...].astype(F32), axis=0).astype(BF16)
    gated = read_out * silu(gate_proj.astype(F32))
    parts = []
    for g in range(2):
        part = gated[:, g * 512 : (g + 1) * 512]
        parts.append(part * lax.rsqrt(jnp.mean(part * part, axis=-1, keepdims=True) + norm_eps))
    mx[c, z] = (jnp.concatenate(parts, axis=1) * group_gain[...]).astype(BF16)
    for k, e in zc_peers:
        send(mx.at[c, z], mx.at[c, z], ssem.at[9], rsem.at[9], (k, y, x, e))

    landed(rts.at[pl.ds(0, 120)], rsem.at[6], "rt_yx")
    table = rts.reshape(256, 256)[...].astype(F32)
    names, scores = table[:, 0:128], table[:, 128:256]
    lane = lax.broadcasted_iota(jnp.int32, (256, 128), 1)
    live = lane < 4
    hit = jnp.where(live & (names == expert.astype(F32)), 1.0, 0.0)
    shifted = jnp.where(live, scores, -3e38)
    grown = jnp.where(live, jnp.exp(shifted - jnp.max(shifted, axis=1, keepdims=True)), 0.0)
    row_weight = jnp.sum(hit * grown, axis=1, keepdims=True) / jnp.sum(grown, axis=1, keepdims=True)
    chosen = jnp.broadcast_to(jnp.sum(hit, axis=1, keepdims=True), (256, 128))
    rr = lax.broadcasted_iota(jnp.int32, (256, 256), 0)
    cc = lax.broadcasted_iota(jnp.int32, (256, 256), 1)
    chosen16 = chosen.astype(BF16)
    count_col = dot((cc <= rr).astype(BF16), chosen16)
    count_row = dot(chosen16, (rr <= cc).astype(BF16), 0, 0)[0:32]
    chosen_row = dot(chosen16, (rr == cc).astype(BF16), 0, 0)[0:32]
    slot = lax.broadcasted_iota(jnp.int32, (32, 256), 0).astype(F32)
    picks = jnp.where((count_row - 1.0 == slot) & (chosen_row > 0.5), 1.0, 0.0)
    picks_t = jnp.where((count_col - 1.0 == lane.astype(F32)) & (chosen > 0.5), 1.0, 0.0)
    slot_weight = dot(picks, jnp.broadcast_to(row_weight, (256, 128)), precision=highest)[:, 0:1]
    pt[...] = picks_t.astype(BF16)
    gate_line = dense_gate[...]
    g_hi = gate_line.astype(BF16)
    g_mid = (gate_line - g_hi.astype(F32)).astype(BF16)
    g_lo = (gate_line - g_hi.astype(F32) - g_mid.astype(F32)).astype(BF16)
    lines = jnp.concatenate([dense_up[...], g_hi, g_mid, g_lo, jnp.zeros((13, 2048), BF16)], axis=0)
    for k in range(2):
        upl[k] = lines[:, k * 1024 : (k + 1) * 1024]

    landed(wo, rsem.at[7], "wo")
    landed(frecv.at[pl.ds(0, 15)], rsem.at[9], "mixer")
    columns_out = [dot(mx[k].reshape(16, 1024), wo[k].reshape(128, 1024), 1, 1) for k in range(2)]
    osend[...] = (columns_out[0] + columns_out[1]).astype(BF16)
    for k, e in zc_peers:
        send(osend, orecv.at[zc], ssem.at[10], rsem.at[10], (k, y, x, e))
    orecv[zc] = osend[...]
    landed(tkz.at[pl.ds(0, NZ - 1)], rsem.at[11], "tkz")
    landed(orecv.at[pl.ds(0, 15)], rsem.at[10], "out")
    mixed = jnp.concatenate([orecv[k].astype(F32) for k in range(2 * NZ)], axis=1)
    hidden = (tkz[...].reshape(16, 2048).astype(F32) + mixed).astype(BF16)
    hid[...] = hidden.reshape(NZ, 2, 2048)
    normed_mid = rms_scale(hidden.astype(F32), second_gain[...]).astype(BF16)
    rows[c, yx] = jnp.where(c == 0, normed_mid[:, 0:1024], normed_mid[:, 1024:2048])
    for j, i in yx_peers:
        send(rows.at[c, yx], rows.at[c, yx], ssem.at[12], planesem.at[yx], (z, j, i, c))

    driven = step_wide * conv_inner
    first_row = lax.broadcasted_iota(jnp.int32, (8, 512), 0) == 0
    for s in range(2):
        for g in range(2):
            lhs = jnp.where(first_row, driven[s : s + 1, g * 512 : (g + 1) * 512], 0.0)
            rhs = jnp.broadcast_to(write_vec[s : s + 1, g * 128 : (g + 1) * 128], (8, 128))
            update = dot(lhs, rhs, 0, 0, highest).reshape(8, 64, 128)
            for h in range(8):
                head = g * 8 + h
                rate = jnp.broadcast_to(decay[s : s + 1, head : head + 1], (64, 128))
                hs[s, head] = rate * hs[s, head] + update[h]

    for i in (3, 4, 5):
        copies[i].wait()

    def use(k, j):
        block = rows[k, pl.ds(j * NX, NX)].reshape(64, 1024)
        span = pl.ds(pl.multiple_of(j * 64, 64), 64)
        return dot(pt[span][:, 0:32], block, 0, 0), dot(block, upl[k], 1, 1)

    def gather_of(j):
        return pl.ds(j * NX, NX)

    order = (0, 1, 3, 2)
    picked_own, picked_other = None, None
    pending = None

    def take_other(j, total):
        landed(rows.at[other, gather_of(j)], fsem.at[j], "rows_d2d")
        got, pre = use(other, j)
        pbuf[j] = pbuf[j] + pre
        return got if total is None else total + got

    for d in order:
        j = y_at[d]
        for e in (1, 3, 2) if d == 0 else (0, 1, 3, 2):
            i = j * NX + x_at[e]
            landed(rows.at[c, i], planesem.at[i], "rows_yx")
        block = rows.at[c, gather_of(j)]
        send(block, block, ssem.at[13], fsem.at[j], partner)
        got, pre = use(c, j)
        picked_own = got if picked_own is None else picked_own + got
        pbuf[j] = pre
        if pending is not None:
            picked_other = take_other(pending, picked_other)
        pending = j
    picked_other = take_other(pending, picked_other)

    pre = pbuf[...].reshape(256, 32)
    weight = sigmoid(jnp.sum(pre[:, 16:19], axis=1, keepdims=True))
    dense_act = silu(pre[:, 0:16]).astype(BF16).astype(F32) * weight
    dact[...] = dense_act.astype(BF16)
    send(dact, dactp, ssem.at[15], rsem.at[15], partner)
    own16, other16 = picked_own.astype(BF16), picked_other.astype(BF16)
    own_span = pl.ds(pl.multiple_of(c * 1024, 1024), 1024)
    other_span = pl.ds(pl.multiple_of(other * 1024, 1024), 1024)
    gate_pre = dot(own16, eg[own_span]) + dot(other16, eg[other_span])
    up_pre = dot(own16, eu[own_span]) + dot(other16, eu[other_span])
    glu_part = jnp.minimum(gate_pre, clamp_limit)
    lin_part = jnp.clip(up_pre, -clamp_limit, clamp_limit)
    activated = (glu_part * sigmoid(glu_alpha * glu_part) * (lin_part + 1.0)).astype(BF16)
    epart[...] = (dot(activated, ed[:, other_span]) * slot_weight).astype(BF16)
    send(epart, epartp, ssem.at[14], rsem.at[14], partner)
    own_part = dot(activated, ed[:, own_span]) * slot_weight
    landed(ddp, rsem.at[8], "ddp")
    landed(dactp, rsem.at[15], "dact")
    down = jnp.concatenate([dense_down[:, own_span], ddp[...]], axis=0)
    dense_term = dot(jnp.concatenate([dact[...], dactp[...]], axis=1), down)
    landed(epartp, rsem.at[14], "epart")
    both = (own_part + epartp[...].astype(F32)).astype(BF16)

    dterm[...] = dense_term.reshape(NY, 64, 1024)
    for d in (2, 1, 3, 0):
        j = y_at[d]
        span = pl.ds(pl.multiple_of(j * 64, 64), 64)
        total = dterm[j] + dot(pt[span][:, 0:32], both)
        tsum[gather_of(j)] = total.astype(BF16).reshape(NX, 16, 1024)
        for e in (2, 1, 3) if d == 0 else (2, 1, 3, 0):
            i = x_at[e]
            send(tsum.at[j * NX + i], prs.at[yx], ssem.at[16], rsem.at[16], (z, j, i, c))
    prs[yx] = tsum[yx]
    landed(prs.at[pl.ds(0, NYX - 1)], rsem.at[16], "sum_yx")
    fsend[...] = jnp.sum(prs[...].astype(F32), axis=0).astype(BF16).reshape(NZ, 2, 1024)
    for k, e in zc_peers:
        send(fsend.at[k], frecv.at[zc], ssem.at[17], rsem.at[17], (k, y, x, e))
    frecv[zc] = fsend[z]
    landed(frecv.at[pl.ds(0, 15)], rsem.at[17], "sum_z")
    final = []
    for k in range(2):
        total = frecv[k].astype(F32)
        for i in range(1, NZ):
            total = total + frecv[2 * i + k].astype(F32)
        final.append(total)
    result = hid[z].astype(F32) + jnp.concatenate(final, axis=1)
    layer_out[...] = jnp.where(c == 0, result[0:1], result[1:2]).astype(BF16)

    for i, ref in enumerate((
        tok.at[pl.ds(0, NZY - 1)], wi.at[pl.ds(0, NX - 1)], wg.at[pl.ds(0, NX - 1)],
        rts.at[pl.ds(0, NZ - 1)], psend_i.at[pl.ds(0, NZY - 1)], psend_g.at[pl.ds(0, NZY - 1)],
        rts.at[pl.ds(0, 120)], None, ddp, frecv.at[pl.ds(0, 15)],
        orecv.at[pl.ds(0, 15)], tkz.at[pl.ds(0, NZ - 1)], rows.at[0, pl.ds(0, NYX - 1)],
        rows.at[0],
        epart, dact, prs.at[pl.ds(0, NYX - 1)], frecv.at[pl.ds(0, 15)],
    )):
        if ref is not None:
            landed(ref, ssem.at[i])

    @pl.when(keeper == c)
    def _():
        landed(prs.at[pl.ds(0, NYX - 1)], ssem.at[7])

    @pl.when(keeper != c)
    def _():
        landed(wo, ssem.at[7])


def write_kernel(*refs):
    sems = refs[8]
    copies = [pltpu.make_async_copy(refs[i], refs[4 + i], sems.at[i]) for i in range(4)]
    for i in (3, 0, 1, 2):
        copies[i].start()
    for copy in copies:
        copy.wait()


def local(
    tokens, head_state, conv_state, conv_proj_state, first_gain, gate_weight, inner_weight,
    write_weight, read_weight, step_weight, conv_kernel, conv_proj_kernel, step_bias, log_rate,
    skip_gain, group_gain, out_weight, second_gain, routes, route_logits, expert_gate, expert_up,
    expert_down, dense_up, dense_down, dense_gate,
):
    near = [
        tokens, first_gain[None], step_weight.T, conv_state.transpose(1, 0, 2), conv_proj_state,
        conv_kernel, conv_proj_kernel, step_bias[None], log_rate[None], skip_gain[None],
        group_gain[None], second_gain[None], routes, route_logits, dense_up.T, dense_down,
        dense_gate[None],
    ]
    far = [
        out_weight.T, head_state, gate_weight, inner_weight, write_weight, read_weight, expert_gate,
        expert_up, expert_down,
    ]
    vmem = pl.BlockSpec(memory_space=pltpu.VMEM)
    anywhere = pl.BlockSpec(memory_space=pltpu.HBM)
    V = pltpu.VMEM
    outs = (
        jax.ShapeDtypeStruct((1, 2048), BF16),
        jax.ShapeDtypeStruct((3, 2, 1024), BF16),
        jax.ShapeDtypeStruct((2, 3, 2, 256), BF16),
        jax.ShapeDtypeStruct((2, 16, 64, 128), F32),
    )
    results = pl.pallas_call(
        layer_kernel,
        out_shape=tuple(V(o.shape, o.dtype) for o in outs),
        in_specs=[anywhere] * (len(near) + len(far)),
        out_specs=(vmem, vmem, vmem, vmem),
        scratch_shapes=[
            *[V(a.shape, a.dtype) for a in near],
            V((2048, 256), BF16), V((2048, 256), BF16),
            V((2048, 512), BF16), V((2048, 512), BF16), V((512, 2048), BF16),
            V((NX, 16, 1024), BF16), V((NX, 16, 1024), BF16),
            V((16, 2, 128), BF16), V((NZY, 2, 128), BF16),
            V((NZY, 2, 1024), BF16), V((NZY, 2, 1024), BF16),
            V((NZY, 2, 1024), BF16), V((NZY, 2, 1024), BF16),
            V((128, 2, 256), BF16), V((2, 8, 16, 1024), BF16), V((2, NZ, 2, 1024), BF16),
            V((16, 128), BF16), V((2 * NZ, 16, 128), BF16), V((NZ, 2, 2048), BF16), V((NZ, 2, 2048), BF16),
            V((2, NYX, 16, 1024), BF16), V((16, 1024), BF16), V((256, 16), BF16), V((256, 16), BF16),
            V((32, 1024), BF16), V((32, 1024), BF16),
            V((NYX, 16, 1024), BF16), V((NYX, 16, 1024), BF16), V((NZ, 2, 1024), BF16),
            V((2 * NZ, 2, 1024), BF16), V((256, 128), BF16), V((2, 32, 1024), BF16),
            V((NY, 64, 32), F32), V((NY, 64, 1024), F32),
            pltpu.SemaphoreType.DMA((NEAR,)), pltpu.SemaphoreType.DMA((8,)), pltpu.SemaphoreType.DMA((18,)),
            pltpu.SemaphoreType.DMA((18,)), pltpu.SemaphoreType.DMA((NYX,)), pltpu.SemaphoreType.DMA((NY,)),
        ],
        compiler_params=pltpu.CompilerParams(
            collective_id=0, has_side_effects=True, vmem_limit_bytes=56 * 1024 * 1024
        ),
        cost_estimate=pl.CostEstimate(flops=2 * 10**9, bytes_accessed=16 * 2**20, transcendentals=10**5),
        name="layer",
    )(*near, *far)
    results = [pltpu.with_memory_space_constraint(r, V) for r in results]
    layer_out, conv_out, conv_proj_out, state_out = pl.pallas_call(
        write_kernel,
        out_shape=outs,
        in_specs=[vmem] * 4,
        out_specs=[anywhere] * 4,
        scratch_shapes=[pltpu.SemaphoreType.DMA((4,))],
        name="write",
    )(*results)
    return (layer_out, state_out, conv_out.transpose(1, 0, 2), conv_proj_out)


def solution(mesh):
    torus = Mesh(mesh.devices.reshape(NZ, NY, NX, mesh.shape["tp"]), EP_TP)
    return jax.shard_map(
        local,
        mesh=torus,
        in_specs=(
            P(EP, None), P(EP, "tp", None, None), P(EP, None, "tp"), P(EP, None, None, "tp"), P(),
            P(EP, "tp"), P(EP, "tp"), P(None, "tp"), P(None, "tp"), P(None, "tp"), P(None, "tp"),
            P(None, None, "tp"), P("tp"), P("tp"), P("tp"), P("tp"), P("tp", EP), P(), P(EP, None),
            P(EP, None), P(EP, None, "tp"), P(EP, None, "tp"), P(EP, "tp", None), P(None, EP_TP),
            P(EP_TP, None), P(),
        ),
        out_specs=(
            P(EP_TP, None), P(EP, "tp", None, None), P(EP, None, "tp"), P(EP, None, None, "tp"),
        ),
        check_vma=False,
    )
```

```python
import functools

import jax
import jax.numpy as jnp
from jax import lax
from jax.experimental import pallas as pl
from jax.experimental.pallas import tpu as pltpu
from jax.sharding import Mesh
from jax.sharding import PartitionSpec as P

EP = ("ep_0", "ep_1", "ep_2")
EP_TP = ("ep_0", "ep_1", "ep_2", "tp")
MESH = pl.DeviceIdType.MESH
F32 = jnp.float32
BF16 = jnp.bfloat16
norm_eps = 1e-05
clamp_limit = 7.0
glu_alpha = 1.702
highest = lax.Precision.HIGHEST
NZ, NY, NX = 8, 4, 4
NZY, NYX = NZ * NY, NY * NX
WIDE = 768


sigmoid = jax.nn.sigmoid
silu = jax.nn.silu


def softplus(v):
    return jnp.maximum(v, 0.0) + jnp.log1p(jnp.exp(-jnp.abs(v)))


def dot(a, b, ca=1, cb=0, precision=None):
    return lax.dot_general(
        a, b, (((ca,), (cb,)), ((), ())), precision=precision, preferred_element_type=F32
    )


def rms_scale(values, gain_vec):
    return values * lax.rsqrt(jnp.mean(values * values, axis=-1, keepdims=True) + norm_eps) * gain_vec


NEAR = 17


def layer_kernel(*refs):
    near_hbm, refs = refs[:NEAR], refs[NEAR:]
    (
        out_weight, head_state, gate_weight, inner_weight, write_weight, read_weight, expert_gate,
        expert_up, expert_down, layer_out, conv_out, conv_proj_out, hs,
    ) = refs[:13]
    near, refs = refs[13 : 13 + NEAR], refs[13 + NEAR :]
    (
        tokens, first_gain, step_weight, conv_state, conv_proj_state, conv_kernel, conv_proj_kernel,
        step_bias, log_rate, skip_gain, group_gain, second_gain, routes, route_logits, dense_up,
        dense_down, dense_gate,
    ) = near
    (
        ww, rw, eg, eu, ed, wg, wi, nblk, tok, psend_i, psend_g, precv_i, precv_g, rts, wo, mx,
        osend, orecv, tkz, hid, rows, ddp, dact, dactp, epart, epartp, tsum, prs, fsend, frecv,
        pt, upl, upp, pbuf, pmsg, pgot, pickm, pickp, dterm, perm, pz, zsum,
        zrs, zsend, zrecv, lsem, ssem, rsem, planesem,
    ) = refs
    z, y, x, c = [lax.axis_index(n) for n in EP_TP]
    zy = z * NY + y
    yx = y * NX + x
    zc = z * 2 + c
    expert = zy * NX + x
    base = yx * NZ
    other = 1 - c
    partner = (z, y, x, other)

    z_at = [lax.rem(z + d, NZ) for d in range(NZ)]
    y_at = [lax.rem(y + d, NY) for d in range(NY)]
    x_at = [lax.rem(x + d, NX) for d in range(NX)]
    c_at = [c, other]
    zy_peers = [(z_at[d], y_at[e]) for d in (4, 3, 5, 2, 6, 1, 7, 0) for e in (2, 1, 3, 0)][:-1]
    yx_peers = [(y_at[d], x_at[e]) for d in (2, 1, 3, 0) for e in (2, 1, 3, 0)][:-1]
    zc_peers = [(z_at[d], c_at[e]) for d in (4, 3, 5, 2, 6, 1, 7, 0) for e in (1, 0)][:-1]
    z_peers = [z_at[d] for d in (4, 3, 5, 2, 6, 1, 7)]

    def send(src, dst, s, r, device):
        pltpu.make_async_remote_copy(
            src_ref=src, dst_ref=dst, send_sem=s, recv_sem=r, device_id=device, device_id_type=MESH
        ).start()

    def landed(ref, sem, name="tail"):
        with jax.named_scope(name):
            pltpu.make_async_copy(ref, ref, sem).wait()

    barrier = pltpu.get_barrier_semaphore()

    def hello(device):
        pl.semaphore_signal(barrier, inc=1, device_id=device, device_id_type=MESH)

    for k, j in zy_peers:
        hello((k, j, x, c))
    for j, i in yx_peers:
        hello((z, j, i, c))
        hello((z, j, i, other))
    hello(partner)
    for k in z_peers:
        hello((k, y, x, other))

    small = [pltpu.make_async_copy(a, b, ssem.at[i]) for i, (a, b) in enumerate(zip(near_hbm, near))]
    loads = [
        (write_weight, ww), (read_weight, rw), (head_state, hs), (expert_gate.at[0], eg),
        (expert_up.at[0], eu), (expert_down.at[0], ed), (gate_weight, wg.at[x]),
        (inner_weight, wi.at[x]),
    ]
    copies = [pltpu.make_async_copy(a, b, lsem.at[i]) for i, (a, b) in enumerate(loads)]
    for copy in [*small, copies[7], copies[6]]:
        copy.start()
    small[0].wait()
    small[1].wait()

    normed = rms_scale(tokens[...].astype(F32), first_gain[...]).astype(BF16)
    for b in range(16):
        nblk[b] = normed[:, b * 128 : (b + 1) * 128]
    tok[zy] = nblk[zy // 2]
    tkz[z] = tokens[...]
    with jax.named_scope("small"):
        for copy in [*small[2:], copies[7], copies[6]]:
            copy.wait()
    blank = jnp.zeros((2, 124), F32)
    rts[base + z] = jnp.concatenate(
        [routes[...].astype(F32), blank, route_logits[...].astype(F32), blank], axis=1
    ).astype(BF16)

    with jax.named_scope("barrier"):
        pl.semaphore_wait(barrier, (NZY - 1) + (2 * NYX - 1) + (NZ - 1))

    for k, j in zy_peers:
        send(nblk.at[k * 2 + j // 2], tok.at[zy], ssem.at[0], rsem.at[0], (k, j, x, c))
    for k in z_peers:
        send(rts.at[base + z], rts.at[base + z], ssem.at[3], rsem.at[3], (k, y, x, c))
    for i in (x_at[2], x_at[1], x_at[3]):
        send(wi.at[x], wi.at[x], ssem.at[1], rsem.at[1], (z, y, i, c))
    for i in (x_at[2], x_at[1], x_at[3]):
        send(wg.at[x], wg.at[x], ssem.at[2], rsem.at[2], (z, y, i, c))
    for k in z_peers:
        send(tkz.at[z], tkz.at[z], ssem.at[11], rsem.at[11], (k, y, x, c))
    keeper = yx // 8
    place = wo.at[c, yx % 8]

    for j, i in yx_peers:
        send(out_weight, place, ssem.at[7], rsem.at[7], (z, j, i, keeper))

    @pl.when(keeper == c)
    def _():
        pltpu.make_async_copy(out_weight, place, rsem.at[7]).start()

    @pl.when(keeper != c)
    def _():
        send(out_weight, place, ssem.at[7], rsem.at[7], partner)


    for i in (0, 1, 2, 3, 4, 5):
        copies[i].start()
    with jax.named_scope("ww"):
        copies[0].wait()
        copies[1].wait()
    write_proj = dot(normed, ww[...]).astype(BF16)
    read_proj = dot(normed, rw[...]).astype(BF16)
    step_raw = dot(normed, step_weight[...], 1, 1)

    landed(tok.at[pl.ds(0, NZY - 1)], rsem.at[0], "tok")
    landed(rts.at[pl.ds(0, NZ - 1)], rsem.at[3], "rt_z")
    mine8 = pl.ds(base, NZ)
    for j, i in yx_peers:
        send(rts.at[mine8], rts.at[mine8], ssem.at[6], rsem.at[6], (z, j, i, c))
    landed(wi.at[pl.ds(0, NX - 1)], rsem.at[1], "wi")
    all_tok = tok.reshape(2 * NZY, 128)[...]
    low = (y % 2) == 0

    def padded(weight):
        zero = jnp.zeros_like(weight)
        return jnp.concatenate([jnp.where(low, weight, zero), jnp.where(low, zero, weight)], axis=0)

    psend_i.reshape(2 * NZY, 1024)[...] = dot(all_tok, padded(wi.reshape(64, 1024)[...])).astype(BF16)
    for k, j in zy_peers:
        send(psend_i.at[k * NY + j], precv_i.at[zy], ssem.at[4], rsem.at[4], (k, j, x, c))
    precv_i[zy] = psend_i[zy]
    landed(wg.at[pl.ds(0, NX - 1)], rsem.at[2], "wg")
    psend_g.reshape(2 * NZY, 1024)[...] = dot(all_tok, padded(wg.reshape(64, 1024)[...])).astype(BF16)
    for k, j in zy_peers:
        send(psend_g.at[k * NY + j], precv_g.at[zy], ssem.at[5], rsem.at[5], (k, j, x, c))
    precv_g[zy] = psend_g[zy]
    own_span = pl.ds(pl.multiple_of(c * 1024, 1024), 1024)
    other_span = pl.ds(pl.multiple_of(other * 1024, 1024), 1024)
    send(dense_down.at[:, other_span], ddp, ssem.at[8], rsem.at[8], partner)
    send(dense_up.at[:, other_span], upp, ssem.at[19], rsem.at[12], partner)

    cps = conv_proj_state[...].astype(F32)
    cpk = conv_proj_kernel[...]

    def conv_of(w, fresh):
        total = fresh.astype(F32) * cpk[3, w : w + 1]
        for i in range(3):
            total = total + cps[:, i, w, :] * cpk[i, w : w + 1]
        return silu(total)

    write_vec = conv_of(0, write_proj)
    read_vec = conv_of(1, read_proj)
    step_size = softplus(step_raw + step_bias[...])
    decay = jnp.exp(-jnp.exp(log_rate[...]) * step_size)
    head_of = lax.broadcasted_iota(jnp.int32, (16, 1024), 1) // 64
    spread = (head_of == lax.broadcasted_iota(jnp.int32, (16, 1024), 0)).astype(F32)
    step_wide = dot(step_size, spread, precision=highest)
    skip_wide = dot(skip_gain[...], spread, precision=highest)
    decay_wide = dot(decay, spread, precision=highest)
    ck = conv_kernel[...]
    early = sum(conv_state[i].astype(F32) * ck[i : i + 1] for i in range(3))
    for i in range(2):
        conv_out[i] = conv_state[i + 1]
        conv_proj_out[:, i] = conv_proj_state[:, i + 1]
    for s in range(2):
        conv_proj_out[s, 2] = jnp.concatenate([write_proj[s : s + 1], read_proj[s : s + 1]], axis=0)
    copies[2].wait()
    held, met = [], []
    for s in range(2):
        for g in range(2):
            span = slice(g * 128, (g + 1) * 128)
            reader = read_vec[s : s + 1, span]
            group = hs[s, g * 8 : (g + 1) * 8].reshape(512, 128)
            held.append(dot(jnp.broadcast_to(reader, (8, 128)), group, 1, 1, highest)[0:1])
            product = jnp.sum(write_vec[s : s + 1, span] * reader, axis=1, keepdims=True)
            met.append(jnp.broadcast_to(product, (1, 512)))

    def by_sequence(four):
        return jnp.concatenate(
            [jnp.concatenate(four[0:2], axis=1), jnp.concatenate(four[2:4], axis=1)], axis=0
        )

    kept = decay_wide * by_sequence(held)
    direct = step_wide * by_sequence(met) + skip_wide

    landed(precv_i.at[pl.ds(0, NZY - 1)], rsem.at[4], "p_inner")
    inner_proj = jnp.sum(precv_i[...].astype(F32), axis=0).astype(BF16)
    conv_out[2] = inner_proj
    conv_inner = silu(early + inner_proj.astype(F32) * ck[3:4])
    read_out = kept + direct * conv_inner

    landed(precv_g.at[pl.ds(0, NZY - 1)], rsem.at[5], "p_gate")
    gate_proj = jnp.sum(precv_g[...].astype(F32), axis=0).astype(BF16)
    gated = read_out * silu(gate_proj.astype(F32))
    parts = []
    for g in range(2):
        part = gated[:, g * 512 : (g + 1) * 512]
        parts.append(part * lax.rsqrt(jnp.mean(part * part, axis=-1, keepdims=True) + norm_eps))
    mx[c, z] = (jnp.concatenate(parts, axis=1) * group_gain[...]).astype(BF16)
    for k, e in zc_peers:
        send(mx.at[c, z], mx.at[c, z], ssem.at[9], rsem.at[9], (k, y, x, e))

    landed(rts.at[pl.ds(0, 120)], rsem.at[6], "rt_yx")
    table = rts.reshape(256, 256)[...].astype(F32)
    names, scores = table[:, 0:128], table[:, 128:256]
    lane = lax.broadcasted_iota(jnp.int32, (256, 128), 1)
    live = lane < 4
    hit = jnp.where(live & (names == expert.astype(F32)), 1.0, 0.0)
    shifted = jnp.where(live, scores, -3e38)
    grown = jnp.where(live, jnp.exp(shifted - jnp.max(shifted, axis=1, keepdims=True)), 0.0)
    row_weight = jnp.sum(hit * grown, axis=1, keepdims=True) / jnp.sum(grown, axis=1, keepdims=True)
    chosen = jnp.broadcast_to(jnp.sum(hit, axis=1, keepdims=True), (256, 128))
    rr = lax.broadcasted_iota(jnp.int32, (256, 256), 0)
    cc = lax.broadcasted_iota(jnp.int32, (256, 256), 1)
    chosen16 = chosen.astype(BF16)
    count_col = dot((cc <= rr).astype(BF16), chosen16)
    count_row = dot(chosen16, (rr <= cc).astype(BF16), 0, 0)[0:32]
    chosen_row = dot(chosen16, (rr == cc).astype(BF16), 0, 0)[0:32]
    slot = lax.broadcasted_iota(jnp.int32, (32, 256), 0).astype(F32)
    picks = jnp.where((count_row - 1.0 == slot) & (chosen_row > 0.5), 1.0, 0.0)
    picks_t = jnp.where((count_col - 1.0 == lane.astype(F32)) & (chosen > 0.5), 1.0, 0.0)
    slot_weight = dot(picks, jnp.broadcast_to(row_weight, (256, 128)), precision=highest)[:, 0:1]
    pt[...] = picks_t.astype(BF16)
    turned = ((cc >> 1) & 15) * 16 + (cc >> 5) * 2 + (cc & 1)
    perm[...] = (rr == turned).astype(BF16)
    pz[...] = dot(picks.astype(BF16), perm[...]).astype(BF16)
    gate_line = dense_gate[...]
    g_hi = gate_line.astype(BF16)
    g_mid = (gate_line - g_hi.astype(F32)).astype(BF16)
    g_lo = (gate_line - g_hi.astype(F32) - g_mid.astype(F32)).astype(BF16)
    lines = jnp.concatenate([g_hi, g_mid, g_lo, jnp.zeros((13, 2048), BF16)], axis=0)
    upl[0:16] = dense_up[:, own_span]
    upl[16:32] = jnp.where(c == 0, lines[:, 0:1024], lines[:, 1024:2048])
    landed(upp, rsem.at[12], "upp")
    upl[32:48] = upp[...]

    landed(wo, rsem.at[7], "wo")
    landed(precv_i.at[pl.ds(0, 15)], rsem.at[9], "mixer")
    columns_out = [dot(mx[k].reshape(16, 1024), wo[k].reshape(128, 1024), 1, 1) for k in range(2)]
    osend[...] = (columns_out[0] + columns_out[1]).astype(BF16)
    for k, e in zc_peers:
        send(osend, orecv.at[zc], ssem.at[10], rsem.at[10], (k, y, x, e))
    orecv[zc] = osend[...]
    landed(tkz.at[pl.ds(0, NZ - 1)], rsem.at[11], "tkz")
    landed(orecv.at[pl.ds(0, 15)], rsem.at[10], "out")
    mixed = jnp.concatenate([orecv[k].astype(F32) for k in range(2 * NZ)], axis=1)
    hidden = (tkz[...].reshape(16, 2048).astype(F32) + mixed).astype(BF16)
    hid[...] = hidden.reshape(NZ, 2, 2048)
    normed_mid = rms_scale(hidden.astype(F32), second_gain[...]).astype(BF16)
    rows[c, yx] = jnp.where(c == 0, normed_mid[:, 0:1024], normed_mid[:, 1024:2048])
    for j, i in yx_peers:
        send(rows.at[c, yx], rows.at[c, yx], ssem.at[12], planesem.at[y], (z, j, i, c))

    driven = step_wide * conv_inner
    first_row = lax.broadcasted_iota(jnp.int32, (8, 512), 0) == 0
    for s in range(2):
        for g in range(2):
            lhs = jnp.where(first_row, driven[s : s + 1, g * 512 : (g + 1) * 512], 0.0)
            rhs = jnp.broadcast_to(write_vec[s : s + 1, g * 128 : (g + 1) * 128], (8, 128))
            update = dot(lhs, rhs, 0, 0, highest).reshape(8, 64, 128)
            for h in range(8):
                head = g * 8 + h
                rate = jnp.broadcast_to(decay[s : s + 1, head : head + 1], (64, 128))
                hs[s, head] = rate * hs[s, head] + update[h]

    for i in (3, 4, 5):
        copies[i].wait()

    picked = None
    for d in (0, 1, 3, 2):
        j = y_at[d]
        landed(rows.at[c, pl.ds(0, 3 if d == 0 else 4)], planesem.at[j], "rows_yx")
        block = rows[c, pl.ds(pl.multiple_of(j * NX, NX), NX)].reshape(64, 1024)
        got = dot(pt[pl.ds(pl.multiple_of(j * 64, 64), 64)][:, 0:32], block, 0, 0)
        picked = got if picked is None else picked + got
        if d == 2:
            pickm[...] = picked.astype(BF16)
            send(pickm, pickp, ssem.at[13], rsem.at[13], partner)
        pbuf[j] = dot(upl[...], block, 1, 1)
    sums = jnp.concatenate([pbuf[j] for j in range(NY)], axis=1)
    pmsg[...] = jnp.concatenate([sums[32:48], sums[16:32]], axis=0)
    send(pmsg, pgot, ssem.at[18], rsem.at[18], partner)
    own16 = picked.astype(BF16)
    gate_pre = dot(own16, eg[own_span])
    up_pre = dot(own16, eu[own_span])
    landed(pgot, rsem.at[18], "pgot")
    pre = sums[0:32] + pgot[...]
    weight = sigmoid(jnp.sum(pre[16:19], axis=0, keepdims=True))
    dact[...] = (silu(pre[0:16]).astype(BF16).astype(F32) * weight).astype(BF16)
    send(dact, dactp, ssem.at[15], rsem.at[15], partner)
    landed(pickp, rsem.at[13], "pickp")
    gate_pre = gate_pre + dot(pickp[...], eg[other_span])
    up_pre = up_pre + dot(pickp[...], eu[other_span])
    glu_part = jnp.minimum(gate_pre, clamp_limit)
    lin_part = jnp.clip(up_pre, -clamp_limit, clamp_limit)
    activated = (glu_part * sigmoid(glu_alpha * glu_part) * (lin_part + 1.0)).astype(BF16)
    epart[...] = (dot(activated, ed[:, other_span]) * slot_weight).astype(BF16)
    send(epart, epartp, ssem.at[14], rsem.at[14], partner)
    own_part = dot(activated, ed[:, own_span]) * slot_weight
    landed(ddp, rsem.at[8], "ddp")
    landed(dactp, rsem.at[15], "dact")
    down = jnp.concatenate([dense_down[:, own_span], ddp[...]], axis=0)
    dense_both = jnp.concatenate([dact[...], dactp[...]], axis=0)
    dterm[...] = dot(dense_both, down[:, 0:WIDE], 0, 0).reshape(NY, 64, WIDE)
    dense_turned = dot(dense_both, perm[...]).astype(BF16)
    landed(epartp, rsem.at[14], "epart")
    both = (own_part + epartp[...].astype(F32)).astype(BF16)

    first_z = dot(
        jnp.concatenate([dense_turned, pz[...]], axis=0),
        jnp.concatenate([down[:, WIDE:], both[:, WIDE:]], axis=0), 0, 0,
    )
    zsum[...] = first_z.astype(BF16).reshape(NZ, 32, 1024 - WIDE)
    for k in z_peers:
        send(zsum.at[k], zrs.at[z], ssem.at[20], rsem.at[16], (k, y, x, c))
    zrs[z] = zsum[z]
    for d in (2, 1, 3, 0):
        j = y_at[d]
        span = pl.ds(pl.multiple_of(j * 64, 64), 64)
        total = dterm[j] + dot(pt[span][:, 0:32], both[:, 0:WIDE])
        tsum[pl.ds(pl.multiple_of(j * NX, NX), NX)] = total.astype(BF16).reshape(NX, 16, WIDE)
        for e in (2, 1, 3) if d == 0 else (2, 1, 3, 0):
            i = x_at[e]
            send(tsum.at[j * NX + i], prs.at[yx], ssem.at[16], rsem.at[19], (z, j, i, c))
    prs[yx] = tsum[yx]
    landed(zrs.at[pl.ds(0, NZ - 1)], rsem.at[16], "sum_z1")
    zsend[...] = jnp.sum(zrs[...].astype(F32), axis=0).astype(BF16).reshape(NYX, 2, 1024 - WIDE)
    for j, i in yx_peers:
        for e in c_at:
            send(zsend.at[j * NX + i], zrecv.at[yx * 2 + c], ssem.at[21], rsem.at[20], (z, j, i, e))
    send(zsend.at[yx], zrecv.at[yx * 2 + c], ssem.at[21], rsem.at[20], partner)
    zrecv[yx * 2 + c] = zsend[yx]
    landed(prs.at[pl.ds(0, NYX - 1)], rsem.at[19], "sum_yx")
    fsend[...] = jnp.sum(prs[...].astype(F32), axis=0).astype(BF16).reshape(NZ, 2, WIDE)
    for k, e in zc_peers:
        send(fsend.at[k], frecv.at[zc], ssem.at[17], rsem.at[17], (k, y, x, e))
    frecv[zc] = fsend[z]
    landed(zrecv.at[pl.ds(0, 31)], rsem.at[20], "sum_yx2")
    narrow = [sum(zrecv[2 * i + k].astype(F32) for i in range(NYX)) for k in range(2)]
    landed(frecv.at[pl.ds(0, 15)], rsem.at[17], "sum_z")
    final = []
    for k in range(2):
        total = frecv[k].astype(F32)
        for i in range(1, NZ):
            total = total + frecv[2 * i + k].astype(F32)
        final += [total, narrow[k]]
    result = hid[z].astype(F32) + jnp.concatenate(final, axis=1)
    layer_out[...] = jnp.where(c == 0, result[0:1], result[1:2]).astype(BF16)

    for i, ref in enumerate((
        tok.at[pl.ds(0, NZY - 1)], wi.at[pl.ds(0, NX - 1)], wg.at[pl.ds(0, NX - 1)],
        rts.at[pl.ds(0, NZ - 1)], psend_i.at[pl.ds(0, NZY - 1)], psend_g.at[pl.ds(0, NZY - 1)],
        rts.at[pl.ds(0, 120)], None, ddp, precv_i.at[pl.ds(0, 15)],
        orecv.at[pl.ds(0, 15)], tkz.at[pl.ds(0, NZ - 1)], rows.at[0, pl.ds(0, NYX - 1)],
        pickm, epart, dact, prs.at[pl.ds(0, NYX - 1)], frecv.at[pl.ds(0, 15)], pmsg, upp,
        zrs.at[pl.ds(0, NZ - 1)], zrecv.at[pl.ds(0, 31)],
    )):
        if ref is not None:
            landed(ref, ssem.at[i])

    @pl.when(keeper == c)
    def _():
        landed(rows.at[0, pl.ds(0, NYX - 1)], ssem.at[7])

    @pl.when(keeper != c)
    def _():
        landed(wo, ssem.at[7])


def write_kernel(*refs):
    sems = refs[8]
    copies = [pltpu.make_async_copy(refs[i], refs[4 + i], sems.at[i]) for i in range(4)]
    for i in (3, 0, 1, 2):
        copies[i].start()
    for copy in copies:
        copy.wait()


def local(
    tokens, head_state, conv_state, conv_proj_state, first_gain, gate_weight, inner_weight,
    write_weight, read_weight, step_weight, conv_kernel, conv_proj_kernel, step_bias, log_rate,
    skip_gain, group_gain, out_weight, second_gain, routes, route_logits, expert_gate, expert_up,
    expert_down, dense_up, dense_down, dense_gate,
):
    near = [
        tokens, first_gain[None], step_weight.T, conv_state.transpose(1, 0, 2), conv_proj_state,
        conv_kernel, conv_proj_kernel, step_bias[None], log_rate[None], skip_gain[None],
        group_gain[None], second_gain[None], routes, route_logits, dense_up.T, dense_down,
        dense_gate[None],
    ]
    far = [
        out_weight.T, head_state, gate_weight, inner_weight, write_weight, read_weight, expert_gate,
        expert_up, expert_down,
    ]
    vmem = pl.BlockSpec(memory_space=pltpu.VMEM)
    anywhere = pl.BlockSpec(memory_space=pltpu.HBM)
    V = pltpu.VMEM
    outs = (
        jax.ShapeDtypeStruct((1, 2048), BF16),
        jax.ShapeDtypeStruct((3, 2, 1024), BF16),
        jax.ShapeDtypeStruct((2, 3, 2, 256), BF16),
        jax.ShapeDtypeStruct((2, 16, 64, 128), F32),
    )
    results = pl.pallas_call(
        layer_kernel,
        out_shape=tuple(V(o.shape, o.dtype) for o in outs),
        in_specs=[anywhere] * (len(near) + len(far)),
        out_specs=(vmem, vmem, vmem, vmem),
        scratch_shapes=[
            *[V(a.shape, a.dtype) for a in near],
            V((2048, 256), BF16), V((2048, 256), BF16),
            V((2048, 512), BF16), V((2048, 512), BF16), V((512, 2048), BF16),
            V((NX, 16, 1024), BF16), V((NX, 16, 1024), BF16),
            V((16, 2, 128), BF16), V((NZY, 2, 128), BF16),
            V((NZY, 2, 1024), BF16), V((NZY, 2, 1024), BF16),
            V((NZY, 2, 1024), BF16), V((NZY, 2, 1024), BF16),
            V((128, 2, 256), BF16), V((2, 8, 16, 1024), BF16), V((2, NZ, 2, 1024), BF16),
            V((16, 128), BF16), V((2 * NZ, 16, 128), BF16), V((NZ, 2, 2048), BF16), V((NZ, 2, 2048), BF16),
            V((2, NYX, 16, 1024), BF16), V((16, 1024), BF16), V((16, 256), BF16), V((16, 256), BF16),
            V((32, 1024), BF16), V((32, 1024), BF16),
            V((NYX, 16, WIDE), BF16), V((NYX, 16, WIDE), BF16), V((NZ, 2, WIDE), BF16),
            V((2 * NZ, 2, WIDE), BF16), V((256, 128), BF16), V((48, 1024), BF16),
            V((16, 1024), BF16), V((NY, 48, 64), F32), V((32, 256), F32), V((32, 256), F32),
            V((32, 1024), BF16), V((32, 1024), BF16), V((NY, 64, WIDE), F32),
            V((256, 256), BF16), V((32, 256), BF16), V((NZ, 32, 1024 - WIDE), BF16),
            V((NZ, 32, 1024 - WIDE), BF16), V((NYX, 2, 1024 - WIDE), BF16),
            V((2 * NYX, 2, 1024 - WIDE), BF16),
            pltpu.SemaphoreType.DMA((8,)), pltpu.SemaphoreType.DMA((22,)),
            pltpu.SemaphoreType.DMA((21,)), pltpu.SemaphoreType.DMA((NY,)),
        ],
        compiler_params=pltpu.CompilerParams(
            collective_id=0, has_side_effects=True, vmem_limit_bytes=56 * 1024 * 1024
        ),
        cost_estimate=pl.CostEstimate(flops=2 * 10**9, bytes_accessed=16 * 2**20, transcendentals=10**5),
        name="layer",
    )(*near, *far)
    results = [pltpu.with_memory_space_constraint(r, V) for r in results]
    layer_out, conv_out, conv_proj_out, state_out = pl.pallas_call(
        write_kernel,
        out_shape=outs,
        in_specs=[vmem] * 4,
        out_specs=[anywhere] * 4,
        scratch_shapes=[pltpu.SemaphoreType.DMA((4,))],
        name="write",
    )(*results)
    return (layer_out, state_out, conv_out.transpose(1, 0, 2), conv_proj_out)


def solution(mesh):
    torus = Mesh(mesh.devices.reshape(NZ, NY, NX, mesh.shape["tp"]), EP_TP)
    return jax.shard_map(
        local,
        mesh=torus,
        in_specs=(
            P(EP, None), P(EP, "tp", None, None), P(EP, None, "tp"), P(EP, None, None, "tp"), P(),
            P(EP, "tp"), P(EP, "tp"), P(None, "tp"), P(None, "tp"), P(None, "tp"), P(None, "tp"),
            P(None, None, "tp"), P("tp"), P("tp"), P("tp"), P("tp"), P("tp", EP), P(), P(EP, None),
            P(EP, None), P(EP, None, "tp"), P(EP, None, "tp"), P(EP, "tp", None), P(None, EP_TP),
            P(EP_TP, None), P(),
        ),
        out_specs=(
            P(EP_TP, None), P(EP, "tp", None, None), P(EP, None, "tp"), P(EP, None, None, "tp"),
        ),
        check_vma=False,
    )
```

```python
import functools

import jax
import jax.numpy as jnp
from jax import lax
from jax.experimental import pallas as pl
from jax.experimental.pallas import tpu as pltpu
from jax.sharding import Mesh
from jax.sharding import PartitionSpec as P

EP = ("ep_0", "ep_1", "ep_2")
EP_TP = ("ep_0", "ep_1", "ep_2", "tp")
MESH = pl.DeviceIdType.MESH
F32 = jnp.float32
BF16 = jnp.bfloat16
norm_eps = 1e-05
clamp_limit = 7.0
glu_alpha = 1.702
highest = lax.Precision.HIGHEST
NZ, NY, NX = 8, 4, 4
NZY, NYX = NZ * NY, NY * NX
WIDE = 768


sigmoid = jax.nn.sigmoid
silu = jax.nn.silu


def softplus(v):
    return jnp.maximum(v, 0.0) + jnp.log1p(jnp.exp(-jnp.abs(v)))


def dot(a, b, ca=1, cb=0, precision=None):
    return lax.dot_general(
        a, b, (((ca,), (cb,)), ((), ())), precision=precision, preferred_element_type=F32
    )


def rms_scale(values, gain_vec):
    return values * lax.rsqrt(jnp.mean(values * values, axis=-1, keepdims=True) + norm_eps) * gain_vec


NEAR = 17


def layer_kernel(*refs):
    near_hbm, refs = refs[:NEAR], refs[NEAR:]
    (
        out_weight, head_state, gate_weight, inner_weight, write_weight, read_weight, expert_gate,
        expert_up, expert_down, layer_out, conv_out, conv_proj_out, hs,
    ) = refs[:13]
    near, refs = refs[13 : 13 + NEAR], refs[13 + NEAR :]
    (
        tokens, first_gain, step_weight, conv_state, conv_proj_state, conv_kernel, conv_proj_kernel,
        step_bias, log_rate, skip_gain, group_gain, second_gain, routes, route_logits, dense_up,
        dense_down, dense_gate,
    ) = near
    (
        ww, rw, eg, eu, ed, wg, wi, nblk, tok, psend_i, psend_g, precv_i, precv_g, rts, wo, mx,
        osend, orecv, tkz, hown, hgot, rows, ddp, dact, dactp, epart, epartp, tsum, prs, fsend, frecv,
        pt, upl, upp, pbuf, pmsg, pgot, pickm, pickp, dterm, perm, pz, zsum,
        zrs, zsend, zrecv, pk, lsem, ssem, rsem, planesem, osem,
    ) = refs
    z, y, x, c = [lax.axis_index(n) for n in EP_TP]
    zy = z * NY + y
    yx = y * NX + x
    zc = z * 2 + c
    expert = zy * NX + x
    base = yx * NZ
    other = 1 - c
    partner = (z, y, x, other)

    z_at = [lax.rem(z + d, NZ) for d in range(NZ)]
    y_at = [lax.rem(y + d, NY) for d in range(NY)]
    x_at = [lax.rem(x + d, NX) for d in range(NX)]
    c_at = [c, other]
    zy_peers = [(z_at[d], y_at[e]) for d in (4, 3, 5, 2, 6, 1, 7, 0) for e in (2, 1, 3, 0)][:-1]
    yx_peers = [(y_at[d], x_at[e]) for d in (2, 1, 3, 0) for e in (2, 1, 3, 0)][:-1]
    zc_peers = [(z_at[d], c_at[e]) for d in (4, 3, 5, 2, 6, 1, 7, 0) for e in (1, 0)][:-1]
    z_peers = [z_at[d] for d in (4, 3, 5, 2, 6, 1, 7)]

    def send(src, dst, s, r, device):
        pltpu.make_async_remote_copy(
            src_ref=src, dst_ref=dst, send_sem=s, recv_sem=r, device_id=device, device_id_type=MESH
        ).start()

    def landed(ref, sem, name="tail"):
        with jax.named_scope(name):
            pltpu.make_async_copy(ref, ref, sem).wait()

    barrier = pltpu.get_barrier_semaphore()

    def hello(device):
        pl.semaphore_signal(barrier, inc=1, device_id=device, device_id_type=MESH)

    for k, j in zy_peers:
        hello((k, j, x, c))
    for j, i in yx_peers:
        hello((z, j, i, c))
        hello((z, j, i, other))
    hello(partner)
    for k in z_peers:
        hello((k, y, x, other))

    small = [pltpu.make_async_copy(a, b, ssem.at[i]) for i, (a, b) in enumerate(zip(near_hbm, near))]
    loads = [
        (write_weight, ww), (read_weight, rw), (head_state, hs), (expert_gate.at[0], eg),
        (expert_up.at[0], eu), (expert_down.at[0], ed), (gate_weight, wg.at[x]),
        (inner_weight, wi.at[x]),
    ]
    copies = [pltpu.make_async_copy(a, b, lsem.at[i]) for i, (a, b) in enumerate(loads)]
    for copy in [*small, copies[7], copies[6]]:
        copy.start()
    small[0].wait()
    small[1].wait()

    normed = rms_scale(tokens[...].astype(F32), first_gain[...]).astype(BF16)
    for b in range(16):
        nblk[b] = normed[:, b * 128 : (b + 1) * 128]
    tok[zy] = nblk[zy // 2]
    tkz[z] = tokens[...]
    with jax.named_scope("small"):
        for copy in [*small[2:], copies[7], copies[6]]:
            copy.wait()
    blank = jnp.zeros((2, 124), F32)
    rts[base + z] = jnp.concatenate(
        [routes[...].astype(F32), blank, route_logits[...].astype(F32), blank], axis=1
    ).astype(BF16)

    with jax.named_scope("barrier"):
        pl.semaphore_wait(barrier, (NZY - 1) + (2 * NYX - 1) + (NZ - 1))

    for k, j in zy_peers:
        send(nblk.at[k * 2 + j // 2], tok.at[zy], ssem.at[0], rsem.at[0], (k, j, x, c))
    for k in z_peers:
        send(rts.at[base + z], rts.at[base + z], ssem.at[3], rsem.at[3], (k, y, x, c))
    for i in (x_at[2], x_at[1], x_at[3]):
        send(wi.at[x], wi.at[x], ssem.at[1], rsem.at[1], (z, y, i, c))
    for i in (x_at[2], x_at[1], x_at[3]):
        send(wg.at[x], wg.at[x], ssem.at[2], rsem.at[2], (z, y, i, c))
    for k in z_peers:
        send(tkz.at[z], tkz.at[z], ssem.at[11], rsem.at[11], (k, y, x, c))
    keeper = yx // 8
    place = wo.at[c, yx % 8]

    for j, i in yx_peers:
        send(out_weight, place, ssem.at[7], rsem.at[7], (z, j, i, keeper))

    @pl.when(keeper == c)
    def _():
        pltpu.make_async_copy(out_weight, place, rsem.at[7]).start()

    @pl.when(keeper != c)
    def _():
        send(out_weight, place, ssem.at[7], rsem.at[7], partner)


    for i in (0, 1, 2, 3, 4, 5):
        copies[i].start()
    with jax.named_scope("ww"):
        copies[0].wait()
        copies[1].wait()
    write_proj = dot(normed, ww[...]).astype(BF16)
    read_proj = dot(normed, rw[...]).astype(BF16)
    step_raw = dot(normed, step_weight[...], 1, 1)

    landed(tok.at[pl.ds(0, NZY - 1)], rsem.at[0], "tok")
    landed(rts.at[pl.ds(0, NZ - 1)], rsem.at[3], "rt_z")
    mine8 = pl.ds(base, NZ)
    for j, i in yx_peers:
        send(rts.at[mine8], rts.at[mine8], ssem.at[6], rsem.at[6], (z, j, i, c))
    landed(wi.at[pl.ds(0, NX - 1)], rsem.at[1], "wi")
    all_tok = tok.reshape(2 * NZY, 128)[...]
    low = (y % 2) == 0

    def padded(weight):
        zero = jnp.zeros_like(weight)
        return jnp.concatenate([jnp.where(low, weight, zero), jnp.where(low, zero, weight)], axis=0)

    psend_i.reshape(2 * NZY, 1024)[...] = dot(all_tok, padded(wi.reshape(64, 1024)[...])).astype(BF16)
    for k, j in zy_peers:
        send(psend_i.at[k * NY + j], precv_i.at[zy], ssem.at[4], rsem.at[4], (k, j, x, c))
    precv_i[zy] = psend_i[zy]
    landed(wg.at[pl.ds(0, NX - 1)], rsem.at[2], "wg")
    psend_g.reshape(2 * NZY, 1024)[...] = dot(all_tok, padded(wg.reshape(64, 1024)[...])).astype(BF16)
    for k, j in zy_peers:
        send(psend_g.at[k * NY + j], precv_g.at[zy], ssem.at[5], rsem.at[5], (k, j, x, c))
    precv_g[zy] = psend_g[zy]
    own_span = pl.ds(pl.multiple_of(c * 1024, 1024), 1024)
    other_span = pl.ds(pl.multiple_of(other * 1024, 1024), 1024)
    send(dense_down.at[:, other_span], ddp, ssem.at[8], rsem.at[8], partner)
    send(dense_up.at[:, other_span], upp, ssem.at[19], rsem.at[12], partner)

    cps = conv_proj_state[...].astype(F32)
    cpk = conv_proj_kernel[...]

    def conv_of(w, fresh):
        total = fresh.astype(F32) * cpk[3, w : w + 1]
        for i in range(3):
            total = total + cps[:, i, w, :] * cpk[i, w : w + 1]
        return silu(total)

    write_vec = conv_of(0, write_proj)
    read_vec = conv_of(1, read_proj)
    step_size = softplus(step_raw + step_bias[...])
    decay = jnp.exp(-jnp.exp(log_rate[...]) * step_size)
    head_of = lax.broadcasted_iota(jnp.int32, (16, 1024), 1) // 64
    spread = (head_of == lax.broadcasted_iota(jnp.int32, (16, 1024), 0)).astype(F32)
    step_wide = dot(step_size, spread, precision=highest)
    skip_wide = dot(skip_gain[...], spread, precision=highest)
    decay_wide = dot(decay, spread, precision=highest)
    ck = conv_kernel[...]
    early = sum(conv_state[i].astype(F32) * ck[i : i + 1] for i in range(3))
    for i in range(2):
        conv_out[i] = conv_state[i + 1]
        conv_proj_out[:, i] = conv_proj_state[:, i + 1]
    for s in range(2):
        conv_proj_out[s, 2] = jnp.concatenate([write_proj[s : s + 1], read_proj[s : s + 1]], axis=0)
    copies[2].wait()
    held, met = [], []
    for s in range(2):
        for g in range(2):
            span = slice(g * 128, (g + 1) * 128)
            reader = read_vec[s : s + 1, span]
            group = hs[s, g * 8 : (g + 1) * 8].reshape(512, 128)
            held.append(dot(jnp.broadcast_to(reader, (8, 128)), group, 1, 1, highest)[0:1])
            product = jnp.sum(write_vec[s : s + 1, span] * reader, axis=1, keepdims=True)
            met.append(jnp.broadcast_to(product, (1, 512)))

    def by_sequence(four):
        return jnp.concatenate(
            [jnp.concatenate(four[0:2], axis=1), jnp.concatenate(four[2:4], axis=1)], axis=0
        )

    kept = decay_wide * by_sequence(held)
    direct = step_wide * by_sequence(met) + skip_wide

    landed(precv_i.at[pl.ds(0, NZY - 1)], rsem.at[4], "p_inner")
    inner_proj = jnp.sum(precv_i[...].astype(F32), axis=0).astype(BF16)
    conv_out[2] = inner_proj
    conv_inner = silu(early + inner_proj.astype(F32) * ck[3:4])
    read_out = kept + direct * conv_inner

    landed(precv_g.at[pl.ds(0, NZY - 1)], rsem.at[5], "p_gate")
    gate_proj = jnp.sum(precv_g[...].astype(F32), axis=0).astype(BF16)
    gated = read_out * silu(gate_proj.astype(F32))
    parts = []
    for g in range(2):
        part = gated[:, g * 512 : (g + 1) * 512]
        parts.append(part * lax.rsqrt(jnp.mean(part * part, axis=-1, keepdims=True) + norm_eps))
    mx[c, z] = (jnp.concatenate(parts, axis=1) * group_gain[...]).astype(BF16)
    for k, e in zc_peers:
        send(mx.at[c, z], mx.at[c, z], ssem.at[9], rsem.at[9], (k, y, x, e))

    landed(rts.at[pl.ds(0, 120)], rsem.at[6], "rt_yx")
    table = rts.reshape(256, 256)[...].astype(F32)
    names, scores = table[:, 0:128], table[:, 128:256]
    lane = lax.broadcasted_iota(jnp.int32, (256, 128), 1)
    live = lane < 4
    hit = jnp.where(live & (names == expert.astype(F32)), 1.0, 0.0)
    shifted = jnp.where(live, scores, -3e38)
    grown = jnp.where(live, jnp.exp(shifted - jnp.max(shifted, axis=1, keepdims=True)), 0.0)
    row_weight = jnp.sum(hit * grown, axis=1, keepdims=True) / jnp.sum(grown, axis=1, keepdims=True)
    chosen = jnp.broadcast_to(jnp.sum(hit, axis=1, keepdims=True), (256, 128))
    rr = lax.broadcasted_iota(jnp.int32, (256, 256), 0)
    cc = lax.broadcasted_iota(jnp.int32, (256, 256), 1)
    chosen16 = chosen.astype(BF16)
    count_col = dot((cc <= rr).astype(BF16), chosen16)
    count_row = dot(chosen16, (rr <= cc).astype(BF16), 0, 0)[0:32]
    chosen_row = dot(chosen16, (rr == cc).astype(BF16), 0, 0)[0:32]
    slot = lax.broadcasted_iota(jnp.int32, (32, 256), 0).astype(F32)
    picks = jnp.where((count_row - 1.0 == slot) & (chosen_row > 0.5), 1.0, 0.0)
    picks_t = jnp.where((count_col - 1.0 == lane.astype(F32)) & (chosen > 0.5), 1.0, 0.0)
    slot_weight = dot(picks, jnp.broadcast_to(row_weight, (256, 128)), precision=highest)[:, 0:1]
    pt[...] = picks_t.astype(BF16)
    pk[...] = picks
    turned = ((cc >> 1) & 15) * 16 + (cc >> 5) * 2 + (cc & 1)
    perm[...] = (rr == turned).astype(BF16)
    pz[...] = dot(picks.astype(BF16), perm[...]).astype(BF16)
    gate_line = dense_gate[...]
    g_hi = gate_line.astype(BF16)
    g_mid = (gate_line - g_hi.astype(F32)).astype(BF16)
    g_lo = (gate_line - g_hi.astype(F32) - g_mid.astype(F32)).astype(BF16)
    lines = jnp.concatenate([g_hi, g_mid, g_lo, jnp.zeros((13, 2048), BF16)], axis=0)
    upl[0:16] = dense_up[:, own_span]
    upl[16:32] = jnp.where(c == 0, lines[:, 0:1024], lines[:, 1024:2048])
    landed(upp, rsem.at[12], "upp")
    upl[32:48] = upp[...]

    landed(wo, rsem.at[7], "wo")
    landed(precv_i.at[pl.ds(0, 15)], rsem.at[9], "mixer")
    columns_out = [dot(mx[k].reshape(16, 1024), wo[k].reshape(128, 1024), 1, 1) for k in range(2)]
    landed(tkz.at[pl.ds(0, NZ - 1)], rsem.at[11], "tkz")
    mine128 = tkz[:, :, pl.ds(pl.multiple_of(zc * 128, 128), 128)].reshape(16, 128)
    osend[...] = (mine128.astype(F32) + columns_out[0] + columns_out[1]).astype(BF16)
    holder = z // 4
    place8 = (z % 4) * 2 + c
    third = (z % 4) // 2
    for k in z_peers:
        send(osend, orecv.at[place8], ssem.at[10], osem.at[third], (k, y, x, holder))

    @pl.when(holder != c)
    def _():
        send(osend, orecv.at[place8], ssem.at[10], osem.at[third], partner)

    @pl.when(holder == c)
    def _():
        orecv[place8] = osend[...]

    near_group = third + (1 - 2 * third) * (holder + c - 2 * holder * c)
    own_rows = []
    for n in range(2):
        q = near_group + n * (1 - 2 * near_group)
        if n == 0:

            @pl.when(holder == c)
            def _():
                landed(orecv.at[pl.ds(0, 3)], osem.at[q], "out")

            @pl.when(holder != c)
            def _():
                landed(orecv.at[pl.ds(0, 4)], osem.at[q], "out")
        else:
            landed(orecv.at[pl.ds(0, 4)], osem.at[q], "out2")
        for i in range(4):
            rows[q, yx, :, i * 128 : (i + 1) * 128] = orecv[q * 4 + i]
        for j, i in yx_peers:
            send(rows.at[q, yx], rows.at[q, yx], ssem.at[12], planesem.at[y], (z, j, i, c))
    row_of = lax.broadcasted_iota(jnp.int32, (8, 16), 0) + 2 * z
    sel = (row_of == lax.broadcasted_iota(jnp.int32, (8, 16), 1)).astype(BF16)
    hown[...] = jnp.concatenate([dot(sel, rows[q, yx])[0:2] for q in range(2)], axis=1).astype(BF16)
    send(hown, hgot, ssem.at[22], rsem.at[21], partner)

    driven = step_wide * conv_inner
    first_row = lax.broadcasted_iota(jnp.int32, (8, 512), 0) == 0
    for s in range(2):
        for g in range(2):
            lhs = jnp.where(first_row, driven[s : s + 1, g * 512 : (g + 1) * 512], 0.0)
            rhs = jnp.broadcast_to(write_vec[s : s + 1, g * 128 : (g + 1) * 128], (8, 128))
            update = dot(lhs, rhs, 0, 0, highest).reshape(8, 64, 128)
            for h in range(8):
                head = g * 8 + h
                rate = jnp.broadcast_to(decay[s : s + 1, head : head + 1], (64, 128))
                hs[s, head] = rate * hs[s, head] + update[h]

    for i in (3, 4, 5):
        copies[i].wait()

    picked = None
    gain_half = second_gain[:, own_span]
    ones = jnp.ones((16, 1024), BF16)
    for d in (0, 1, 3, 2):
        j = y_at[d]
        landed(ww.at[pl.ds(0, 192 if d == 0 else 256)], planesem.at[j], "rows_yx")
        four = pl.ds(pl.multiple_of(j * NX, NX), NX)
        plain = jnp.concatenate(
            [rows[q, four].reshape(64, 512) for q in range(2)], axis=1
        ).astype(F32)
        block = (plain * gain_half).astype(BF16)
        got = dot(pt[pl.ds(pl.multiple_of(j * 64, 64), 64)][:, 0:32], block, 0, 0)
        picked = got if picked is None else picked + got
        if d == 2:
            pickm[...] = picked.astype(BF16)
            send(pickm, pickp, ssem.at[13], rsem.at[13], partner)
        pbuf[j] = jnp.concatenate(
            [dot(upl[...], block, 1, 1), dot(ones, (plain * plain).astype(BF16), 1, 1)], axis=0
        )
    sums = jnp.concatenate([pbuf[j] for j in range(NY)], axis=1)
    pmsg[...] = jnp.concatenate([sums[32:48], sums[16:24], sums[48:56]], axis=0)
    send(pmsg, pgot, ssem.at[18], rsem.at[18], partner)
    own16 = picked.astype(BF16)
    gate_pre = dot(own16, eg[own_span])
    up_pre = dot(own16, eu[own_span])
    landed(pgot, rsem.at[18], "pgot")
    pre = jnp.concatenate([sums[0:24], sums[48:56]], axis=0) + pgot[...]
    scale = lax.rsqrt(pre[24:25] * (1.0 / 2048.0) + norm_eps)
    slot_scale = jnp.sum(pk[...] * scale, axis=1, keepdims=True)
    weight = sigmoid(jnp.sum(pre[16:19], axis=0, keepdims=True) * scale)
    dact[...] = (silu(pre[0:16] * scale).astype(BF16).astype(F32) * weight).astype(BF16)
    send(dact, dactp, ssem.at[15], rsem.at[15], partner)
    landed(pickp, rsem.at[13], "pickp")
    gate_pre = (gate_pre + dot(pickp[...], eg[other_span])) * slot_scale
    up_pre = (up_pre + dot(pickp[...], eu[other_span])) * slot_scale
    glu_part = jnp.minimum(gate_pre, clamp_limit)
    lin_part = jnp.clip(up_pre, -clamp_limit, clamp_limit)
    activated = (glu_part * sigmoid(glu_alpha * glu_part) * (lin_part + 1.0)).astype(BF16)
    epart[...] = (dot(activated, ed[:, other_span]) * slot_weight).astype(BF16)
    send(epart, epartp, ssem.at[14], rsem.at[14], partner)
    own_part = dot(activated, ed[:, own_span]) * slot_weight
    landed(ddp, rsem.at[8], "ddp")
    landed(dactp, rsem.at[15], "dact")
    down = jnp.concatenate([dense_down[:, own_span], ddp[...]], axis=0)
    dense_both = jnp.concatenate([dact[...], dactp[...]], axis=0)
    dterm[...] = dot(dense_both, down[:, 0:WIDE], 0, 0).reshape(NY, 64, WIDE)
    dense_turned = dot(dense_both, perm[...]).astype(BF16)
    landed(epartp, rsem.at[14], "epart")
    both = (own_part + epartp[...].astype(F32)).astype(BF16)

    first_z = dot(
        jnp.concatenate([dense_turned, pz[...]], axis=0),
        jnp.concatenate([down[:, WIDE:], both[:, WIDE:]], axis=0), 0, 0,
    )
    zsum[...] = first_z.astype(BF16).reshape(NZ, 32, 1024 - WIDE)
    for k in z_peers:
        send(zsum.at[k], zrs.at[z], ssem.at[20], rsem.at[16], (k, y, x, c))
    zrs[z] = zsum[z]
    for d in (2, 1, 3, 0):
        j = y_at[d]
        span = pl.ds(pl.multiple_of(j * 64, 64), 64)
        total = dterm[j] + dot(pt[span][:, 0:32], both[:, 0:WIDE])
        tsum[pl.ds(pl.multiple_of(j * NX, NX), NX)] = total.astype(BF16).reshape(NX, 16, WIDE)
        for e in (2, 1, 3) if d == 0 else (2, 1, 3, 0):
            i = x_at[e]
            send(tsum.at[j * NX + i], prs.at[yx], ssem.at[16], rsem.at[19], (z, j, i, c))
    prs[yx] = tsum[yx]
    landed(zrs.at[pl.ds(0, NZ - 1)], rsem.at[16], "sum_z1")
    zsend[...] = jnp.sum(zrs[...].astype(F32), axis=0).astype(BF16).reshape(NYX, 2, 1024 - WIDE)
    for j, i in yx_peers:
        for e in c_at:
            send(zsend.at[j * NX + i], zrecv.at[yx * 2 + c], ssem.at[21], rsem.at[20], (z, j, i, e))
    send(zsend.at[yx], zrecv.at[yx * 2 + c], ssem.at[21], rsem.at[20], partner)
    zrecv[yx * 2 + c] = zsend[yx]
    landed(prs.at[pl.ds(0, NYX - 1)], rsem.at[19], "sum_yx")
    fsend[...] = jnp.sum(prs[...].astype(F32), axis=0).astype(BF16).reshape(NZ, 2, WIDE)
    for k, e in zc_peers:
        send(fsend.at[k], frecv.at[zc], ssem.at[17], rsem.at[17], (k, y, x, e))
    frecv[zc] = fsend[z]
    landed(zrecv.at[pl.ds(0, 31)], rsem.at[20], "sum_yx2")
    narrow = [sum(zrecv[2 * i + k].astype(F32) for i in range(NYX)) for k in range(2)]
    landed(frecv.at[pl.ds(0, 15)], rsem.at[17], "sum_z")
    final = []
    for k in range(2):
        total = frecv[k].astype(F32)
        for i in range(1, NZ):
            total = total + frecv[2 * i + k].astype(F32)
        final += [total, narrow[k]]
    landed(hgot, rsem.at[21], "hgot")
    own_half, other_half = hown[...].astype(F32), hgot[...].astype(F32)
    hidden = jnp.concatenate(
        [jnp.where(c == 0, own_half, other_half), jnp.where(c == 0, other_half, own_half)], axis=1
    )
    result = hidden + jnp.concatenate(final, axis=1)
    layer_out[...] = jnp.where(c == 0, result[0:1], result[1:2]).astype(BF16)

    for i, ref in enumerate((
        tok.at[pl.ds(0, NZY - 1)], wi.at[pl.ds(0, NX - 1)], wg.at[pl.ds(0, NX - 1)],
        rts.at[pl.ds(0, NZ - 1)], psend_i.at[pl.ds(0, NZY - 1)], psend_g.at[pl.ds(0, NZY - 1)],
        rts.at[pl.ds(0, 120)], None, ddp, precv_i.at[pl.ds(0, 15)],
        None, tkz.at[pl.ds(0, NZ - 1)], ww.at[pl.ds(0, 960)],
        pickm, epart, dact, prs.at[pl.ds(0, NYX - 1)], frecv.at[pl.ds(0, 15)], pmsg, upp,
        zrs.at[pl.ds(0, NZ - 1)], zrecv.at[pl.ds(0, 31)], hown,
    )):
        if ref is not None:
            landed(ref, ssem.at[i])

    @pl.when(keeper == c)
    def _():
        landed(ww.at[pl.ds(0, 960)], ssem.at[7])

    @pl.when(keeper != c)
    def _():
        landed(wo, ssem.at[7])

    @pl.when(holder == c)
    def _():
        landed(orecv.at[pl.ds(0, NZ - 1)], ssem.at[10])

    @pl.when(holder != c)
    def _():
        landed(orecv, ssem.at[10])


def write_kernel(*refs):
    sems = refs[8]
    copies = [pltpu.make_async_copy(refs[i], refs[4 + i], sems.at[i]) for i in range(4)]
    for i in (3, 0, 1, 2):
        copies[i].start()
    for copy in copies:
        copy.wait()


def local(
    tokens, head_state, conv_state, conv_proj_state, first_gain, gate_weight, inner_weight,
    write_weight, read_weight, step_weight, conv_kernel, conv_proj_kernel, step_bias, log_rate,
    skip_gain, group_gain, out_weight, second_gain, routes, route_logits, expert_gate, expert_up,
    expert_down, dense_up, dense_down, dense_gate,
):
    near = [
        tokens, first_gain[None], step_weight.T, conv_state.transpose(1, 0, 2), conv_proj_state,
        conv_kernel, conv_proj_kernel, step_bias[None], log_rate[None], skip_gain[None],
        group_gain[None], second_gain[None], routes, route_logits, dense_up.T, dense_down,
        dense_gate[None],
    ]
    far = [
        out_weight.T, head_state, gate_weight, inner_weight, write_weight, read_weight, expert_gate,
        expert_up, expert_down,
    ]
    vmem = pl.BlockSpec(memory_space=pltpu.VMEM)
    anywhere = pl.BlockSpec(memory_space=pltpu.HBM)
    V = pltpu.VMEM
    outs = (
        jax.ShapeDtypeStruct((1, 2048), BF16),
        jax.ShapeDtypeStruct((3, 2, 1024), BF16),
        jax.ShapeDtypeStruct((2, 3, 2, 256), BF16),
        jax.ShapeDtypeStruct((2, 16, 64, 128), F32),
    )
    results = pl.pallas_call(
        layer_kernel,
        out_shape=tuple(V(o.shape, o.dtype) for o in outs),
        in_specs=[anywhere] * (len(near) + len(far)),
        out_specs=(vmem, vmem, vmem, vmem),
        scratch_shapes=[
            *[V(a.shape, a.dtype) for a in near],
            V((2048, 256), BF16), V((2048, 256), BF16),
            V((2048, 512), BF16), V((2048, 512), BF16), V((512, 2048), BF16),
            V((NX, 16, 1024), BF16), V((NX, 16, 1024), BF16),
            V((16, 2, 128), BF16), V((NZY, 2, 128), BF16),
            V((NZY, 2, 1024), BF16), V((NZY, 2, 1024), BF16),
            V((NZY, 2, 1024), BF16), V((NZY, 2, 1024), BF16),
            V((128, 2, 256), BF16), V((2, 8, 16, 1024), BF16), V((2, NZ, 2, 1024), BF16),
            V((16, 128), BF16), V((8, 16, 128), BF16), V((NZ, 2, 2048), BF16), V((2, 1024), BF16),
            V((2, 1024), BF16),
            V((2, NYX, 16, 512), BF16), V((16, 1024), BF16), V((16, 256), BF16), V((16, 256), BF16),
            V((32, 1024), BF16), V((32, 1024), BF16),
            V((NYX, 16, WIDE), BF16), V((NYX, 16, WIDE), BF16), V((NZ, 2, WIDE), BF16),
            V((2 * NZ, 2, WIDE), BF16), V((256, 128), BF16), V((48, 1024), BF16),
            V((16, 1024), BF16), V((NY, 64, 64), F32), V((32, 256), F32), V((32, 256), F32),
            V((32, 1024), BF16), V((32, 1024), BF16), V((NY, 64, WIDE), F32),
            V((256, 256), BF16), V((32, 256), BF16), V((NZ, 32, 1024 - WIDE), BF16),
            V((NZ, 32, 1024 - WIDE), BF16), V((NYX, 2, 1024 - WIDE), BF16),
            V((2 * NYX, 2, 1024 - WIDE), BF16), V((32, 256), F32),
            pltpu.SemaphoreType.DMA((8,)), pltpu.SemaphoreType.DMA((23,)),
            pltpu.SemaphoreType.DMA((22,)), pltpu.SemaphoreType.DMA((NY,)),
            pltpu.SemaphoreType.DMA((2,)),
        ],
        compiler_params=pltpu.CompilerParams(
            collective_id=0, has_side_effects=True, vmem_limit_bytes=56 * 1024 * 1024
        ),
        cost_estimate=pl.CostEstimate(flops=2 * 10**9, bytes_accessed=16 * 2**20, transcendentals=10**5),
        name="layer",
    )(*near, *far)
    results = [pltpu.with_memory_space_constraint(r, V) for r in results]
    layer_out, conv_out, conv_proj_out, state_out = pl.pallas_call(
        write_kernel,
        out_shape=outs,
        in_specs=[vmem] * 4,
        out_specs=[anywhere] * 4,
        scratch_shapes=[pltpu.SemaphoreType.DMA((4,))],
        name="write",
    )(*results)
    return (layer_out, state_out, conv_out.transpose(1, 0, 2), conv_proj_out)


def solution(mesh):
    torus = Mesh(mesh.devices.reshape(NZ, NY, NX, mesh.shape["tp"]), EP_TP)
    return jax.shard_map(
        local,
        mesh=torus,
        in_specs=(
            P(EP, None), P(EP, "tp", None, None), P(EP, None, "tp"), P(EP, None, None, "tp"), P(),
            P(EP, "tp"), P(EP, "tp"), P(None, "tp"), P(None, "tp"), P(None, "tp"), P(None, "tp"),
            P(None, None, "tp"), P("tp"), P("tp"), P("tp"), P("tp"), P("tp", EP), P(), P(EP, None),
            P(EP, None), P(EP, None, "tp"), P(EP, None, "tp"), P(EP, "tp", None), P(None, EP_TP),
            P(EP_TP, None), P(),
        ),
        out_specs=(
            P(EP_TP, None), P(EP, "tp", None, None), P(EP, None, "tp"), P(EP, None, None, "tp"),
        ),
        check_vma=False,
    )
```

```python
import functools

import jax
import jax.numpy as jnp
from jax import lax
from jax.experimental import pallas as pl
from jax.experimental.pallas import tpu as pltpu
from jax.sharding import Mesh
from jax.sharding import PartitionSpec as P

EP = ("ep_0", "ep_1", "ep_2")
EP_TP = ("ep_0", "ep_1", "ep_2", "tp")
MESH = pl.DeviceIdType.MESH
F32 = jnp.float32
BF16 = jnp.bfloat16
norm_eps = 1e-05
clamp_limit = 7.0
glu_alpha = 1.702
highest = lax.Precision.HIGHEST
NZ, NY, NX = 8, 4, 4
NZY, NYX = NZ * NY, NY * NX
FAR = 12
WIDE = 768


sigmoid = jax.nn.sigmoid
silu = jax.nn.silu


def softplus(v):
    return jnp.maximum(v, 0.0) + jnp.log1p(jnp.exp(-jnp.abs(v)))


def dot(a, b, ca=1, cb=0, precision=None):
    return lax.dot_general(
        a, b, (((ca,), (cb,)), ((), ())), precision=precision, preferred_element_type=F32
    )


def rms_scale(values, gain_vec):
    return values * lax.rsqrt(jnp.mean(values * values, axis=-1, keepdims=True) + norm_eps) * gain_vec


NEAR = 17


def layer_kernel(*refs):
    near_hbm, refs = refs[:NEAR], refs[NEAR:]
    (
        out_weight, head_state, gate_weight, inner_weight, write_weight, read_weight, expert_gate,
        expert_up, expert_down, layer_out, conv_out, conv_proj_out, hs,
    ) = refs[:13]
    near, refs = refs[13 : 13 + NEAR], refs[13 + NEAR :]
    (
        tokens, first_gain, step_weight, conv_state, conv_proj_state, conv_kernel, conv_proj_kernel,
        step_bias, log_rate, skip_gain, group_gain, second_gain, routes, route_logits, dense_up,
        dense_down, dense_gate,
    ) = near
    (
        ww, rw, eg, eu, ed, wg, wi, nblk, tok, psend_i, psend_g, precv_i, precv_g, rts, wo, mx,
        osend, orecv, tkz, hown, hgot, rows, ddp, dact, dactp, epart, epartp, tsum, prs, fsend, frecv,
        pt, upl, upp, pbuf, pmsg, pgot, pickm, pickp, dterm, perm, pz, zsum,
        zrs, zsend, zrecv, pk, lsem, ssem, rsem, planesem, osem,
    ) = refs
    z, y, x, c = [lax.axis_index(n) for n in EP_TP]
    zy = z * NY + y
    yx = y * NX + x
    zc = z * 2 + c
    expert = zy * NX + x
    base = yx * NZ
    other = 1 - c
    partner = (z, y, x, other)

    z_at = [lax.rem(z + d, NZ) for d in range(NZ)]
    y_at = [lax.rem(y + d, NY) for d in range(NY)]
    x_at = [lax.rem(x + d, NX) for d in range(NX)]
    c_at = [c, other]
    zy_peers = [(z_at[d], y_at[e]) for d in (4, 3, 5, 2, 6, 1, 7, 0) for e in (2, 1, 3, 0)][:-1]
    yx_peers = [(y_at[d], x_at[e]) for d in (2, 1, 3, 0) for e in (2, 1, 3, 0)][:-1]
    zc_peers = [(z_at[d], c_at[e]) for d in (4, 3, 5, 2, 6, 1, 7, 0) for e in (1, 0)][:-1]
    z_peers = [z_at[d] for d in (4, 3, 5, 2, 6, 1, 7)]

    def send(src, dst, s, r, device):
        pltpu.make_async_remote_copy(
            src_ref=src, dst_ref=dst, send_sem=s, recv_sem=r, device_id=device, device_id_type=MESH
        ).start()

    def landed(ref, sem, name="tail"):
        with jax.named_scope(name):
            pltpu.make_async_copy(ref, ref, sem).wait()

    barrier = pltpu.get_barrier_semaphore()

    def hello(device):
        pl.semaphore_signal(barrier, inc=1, device_id=device, device_id_type=MESH)

    for k, j in zy_peers:
        hello((k, j, x, c))
    for j, i in yx_peers:
        hello((z, j, i, c))
        hello((z, j, i, other))
    hello(partner)
    for k in z_peers:
        hello((k, y, x, other))

    small = [pltpu.make_async_copy(a, b, ssem.at[i]) for i, (a, b) in enumerate(zip(near_hbm, near))]
    loads = [
        (write_weight, ww), (read_weight, rw), (head_state, hs), (expert_gate.at[0], eg),
        (expert_up.at[0], eu), (expert_down.at[0], ed), (gate_weight, wg.at[x]),
        (inner_weight, wi.at[x]),
    ]
    copies = [pltpu.make_async_copy(a, b, lsem.at[i]) for i, (a, b) in enumerate(loads)]
    for copy in [*small, copies[7], copies[6]]:
        copy.start()
    small[0].wait()
    small[1].wait()

    normed = rms_scale(tokens[...].astype(F32), first_gain[...]).astype(BF16)
    for b in range(16):
        nblk[b] = normed[:, b * 128 : (b + 1) * 128]
    tok[zy] = nblk[zy // 2]
    tkz[z] = tokens[...]
    with jax.named_scope("small"):
        for copy in [*small[2:], copies[7], copies[6]]:
            copy.wait()
    blank = jnp.zeros((2, 124), F32)
    rts[base + z] = jnp.concatenate(
        [routes[...].astype(F32), blank, route_logits[...].astype(F32), blank], axis=1
    ).astype(BF16)

    with jax.named_scope("barrier"):
        pl.semaphore_wait(barrier, (NZY - 1) + (2 * NYX - 1) + (NZ - 1))

    for i in (x_at[2], x_at[1], x_at[3]):
        send(wi.at[x], wi.at[x], ssem.at[1], rsem.at[1], (z, y, i, c))
    for n, (k, j) in enumerate(zy_peers):
        arrival = rsem.at[0] if n < FAR else rsem.at[22]
        send(nblk.at[k * 2 + j // 2], tok.at[zy], ssem.at[0], arrival, (k, j, x, c))
    for k in z_peers:
        send(rts.at[base + z], rts.at[base + z], ssem.at[3], rsem.at[3], (k, y, x, c))
    for i in (x_at[2], x_at[1], x_at[3]):
        send(wg.at[x], wg.at[x], ssem.at[2], rsem.at[2], (z, y, i, c))
    for k in z_peers:
        send(tkz.at[z], tkz.at[z], ssem.at[11], rsem.at[11], (k, y, x, c))
    keeper = yx // 8
    place = wo.at[c, yx % 8]

    for j, i in yx_peers:
        send(out_weight, place, ssem.at[7], rsem.at[7], (z, j, i, keeper))

    @pl.when(keeper == c)
    def _():
        pltpu.make_async_copy(out_weight, place, rsem.at[7]).start()

    @pl.when(keeper != c)
    def _():
        send(out_weight, place, ssem.at[7], rsem.at[7], partner)


    for i in (0, 1, 2, 3, 4, 5):
        copies[i].start()
    with jax.named_scope("ww"):
        copies[0].wait()
        copies[1].wait()
    write_proj = dot(normed, ww[...]).astype(BF16)
    read_proj = dot(normed, rw[...]).astype(BF16)
    step_raw = dot(normed, step_weight[...], 1, 1)

    low = (y % 2) == 0

    def padded(weights):
        weight = weights.reshape(64, 1024)[...]
        zero = jnp.zeros_like(weight)
        return jnp.concatenate([jnp.where(low, weight, zero), jnp.where(low, zero, weight)], axis=0)

    def terms(lhs, rhs, out, places):
        result = dot(lhs, rhs).astype(BF16)
        for n, d in enumerate(places):
            span = pl.ds(pl.multiple_of(z_at[d] * NY, NY), NY)
            out[span] = result[8 * n : 8 * n + 8].reshape(NY, 2, 1024)

    def tokens_of(places):
        spans = [pl.ds(pl.multiple_of(z_at[d] * NY, NY), NY) for d in places]
        return jnp.concatenate([tok[span].reshape(2 * NY, 128) for span in spans], axis=0)

    def scatter(out, into, n, peers):
        for k, j in peers:
            send(out.at[k * NY + j], into.at[zy], ssem.at[n], rsem.at[n], (k, j, x, c))

    near, far = (2, 6, 1, 7, 0), (4, 3, 5)
    landed(wi.at[pl.ds(0, NX - 1)], rsem.at[1], "wi")
    landed(tok.at[pl.ds(0, NZY - 1 - FAR)], rsem.at[22], "tok_near")
    inner_rows = padded(wi)
    near_tok = tokens_of(near)
    terms(near_tok, inner_rows, psend_i, near)
    scatter(psend_i, precv_i, 4, zy_peers[FAR:])
    landed(rts.at[pl.ds(0, NZ - 1)], rsem.at[3], "rt_z")
    mine8 = pl.ds(base, NZ)
    for j, i in yx_peers:
        send(rts.at[mine8], rts.at[mine8], ssem.at[6], rsem.at[6], (z, j, i, c))
    landed(tok.at[pl.ds(0, FAR)], rsem.at[0], "tok")
    far_tok = tokens_of(far)
    terms(far_tok, inner_rows, psend_i, far)
    scatter(psend_i, precv_i, 4, zy_peers[:FAR])
    landed(wg.at[pl.ds(0, NX - 1)], rsem.at[2], "wg")
    gate_rows = padded(wg)
    terms(far_tok, gate_rows, psend_g, far)
    scatter(psend_g, precv_g, 5, zy_peers[:FAR])
    terms(near_tok, gate_rows, psend_g, near)
    scatter(psend_g, precv_g, 5, zy_peers[FAR:])
    precv_i[zy] = psend_i[zy]
    precv_g[zy] = psend_g[zy]
    own_span = pl.ds(pl.multiple_of(c * 1024, 1024), 1024)
    other_span = pl.ds(pl.multiple_of(other * 1024, 1024), 1024)
    send(dense_down.at[:, other_span], ddp, ssem.at[8], rsem.at[8], partner)
    send(dense_up.at[:, other_span], upp, ssem.at[19], rsem.at[12], partner)

    cps = conv_proj_state[...].astype(F32)
    cpk = conv_proj_kernel[...]

    def conv_of(w, fresh):
        total = fresh.astype(F32) * cpk[3, w : w + 1]
        for i in range(3):
            total = total + cps[:, i, w, :] * cpk[i, w : w + 1]
        return silu(total)

    write_vec = conv_of(0, write_proj)
    read_vec = conv_of(1, read_proj)
    step_size = softplus(step_raw + step_bias[...])
    decay = jnp.exp(-jnp.exp(log_rate[...]) * step_size)
    head_of = lax.broadcasted_iota(jnp.int32, (16, 1024), 1) // 64
    spread = (head_of == lax.broadcasted_iota(jnp.int32, (16, 1024), 0)).astype(F32)
    step_wide = dot(step_size, spread, precision=highest)
    skip_wide = dot(skip_gain[...], spread, precision=highest)
    decay_wide = dot(decay, spread, precision=highest)
    ck = conv_kernel[...]
    early = sum(conv_state[i].astype(F32) * ck[i : i + 1] for i in range(3))
    for i in range(2):
        conv_out[i] = conv_state[i + 1]
        conv_proj_out[:, i] = conv_proj_state[:, i + 1]
    for s in range(2):
        conv_proj_out[s, 2] = jnp.concatenate([write_proj[s : s + 1], read_proj[s : s + 1]], axis=0)
    copies[2].wait()
    held, met = [], []
    for s in range(2):
        for g in range(2):
            span = slice(g * 128, (g + 1) * 128)
            reader = read_vec[s : s + 1, span]
            group = hs[s, g * 8 : (g + 1) * 8].reshape(512, 128)
            held.append(dot(jnp.broadcast_to(reader, (8, 128)), group, 1, 1, highest)[0:1])
            product = jnp.sum(write_vec[s : s + 1, span] * reader, axis=1, keepdims=True)
            met.append(jnp.broadcast_to(product, (1, 512)))

    def by_sequence(four):
        return jnp.concatenate(
            [jnp.concatenate(four[0:2], axis=1), jnp.concatenate(four[2:4], axis=1)], axis=0
        )

    kept = decay_wide * by_sequence(held)
    direct = step_wide * by_sequence(met) + skip_wide

    landed(precv_i.at[pl.ds(0, NZY - 1)], rsem.at[4], "p_inner")
    inner_proj = jnp.sum(precv_i[...].astype(F32), axis=0).astype(BF16)
    conv_out[2] = inner_proj
    conv_inner = silu(early + inner_proj.astype(F32) * ck[3:4])
    read_out = kept + direct * conv_inner

    landed(precv_g.at[pl.ds(0, NZY - 1)], rsem.at[5], "p_gate")
    gate_proj = jnp.sum(precv_g[...].astype(F32), axis=0).astype(BF16)
    gated = read_out * silu(gate_proj.astype(F32))
    parts = []
    for g in range(2):
        part = gated[:, g * 512 : (g + 1) * 512]
        parts.append(part * lax.rsqrt(jnp.mean(part * part, axis=-1, keepdims=True) + norm_eps))
    mx[c, z] = (jnp.concatenate(parts, axis=1) * group_gain[...]).astype(BF16)
    for k, e in zc_peers:
        send(mx.at[c, z], mx.at[c, z], ssem.at[9], rsem.at[9], (k, y, x, e))

    landed(rts.at[pl.ds(0, 120)], rsem.at[6], "rt_yx")
    table = rts.reshape(256, 256)[...].astype(F32)
    names, scores = table[:, 0:128], table[:, 128:256]
    lane = lax.broadcasted_iota(jnp.int32, (256, 128), 1)
    live = lane < 4
    hit = jnp.where(live & (names == expert.astype(F32)), 1.0, 0.0)
    shifted = jnp.where(live, scores, -3e38)
    grown = jnp.where(live, jnp.exp(shifted - jnp.max(shifted, axis=1, keepdims=True)), 0.0)
    row_weight = jnp.sum(hit * grown, axis=1, keepdims=True) / jnp.sum(grown, axis=1, keepdims=True)
    chosen = jnp.broadcast_to(jnp.sum(hit, axis=1, keepdims=True), (256, 128))
    rr = lax.broadcasted_iota(jnp.int32, (256, 256), 0)
    cc = lax.broadcasted_iota(jnp.int32, (256, 256), 1)
    chosen16 = chosen.astype(BF16)
    count_col = dot((cc <= rr).astype(BF16), chosen16)
    count_row = dot(chosen16, (rr <= cc).astype(BF16), 0, 0)[0:32]
    chosen_row = dot(chosen16, (rr == cc).astype(BF16), 0, 0)[0:32]
    slot = lax.broadcasted_iota(jnp.int32, (32, 256), 0).astype(F32)
    picks = jnp.where((count_row - 1.0 == slot) & (chosen_row > 0.5), 1.0, 0.0)
    picks_t = jnp.where((count_col - 1.0 == lane.astype(F32)) & (chosen > 0.5), 1.0, 0.0)
    slot_weight = dot(picks, jnp.broadcast_to(row_weight, (256, 128)), precision=highest)[:, 0:1]
    pt[...] = picks_t.astype(BF16)
    pk[...] = picks
    turned = ((cc >> 1) & 15) * 16 + (cc >> 5) * 2 + (cc & 1)
    perm[...] = (rr == turned).astype(BF16)
    pz[...] = dot(picks.astype(BF16), perm[...]).astype(BF16)
    gate_line = dense_gate[...]
    g_hi = gate_line.astype(BF16)
    g_mid = (gate_line - g_hi.astype(F32)).astype(BF16)
    g_lo = (gate_line - g_hi.astype(F32) - g_mid.astype(F32)).astype(BF16)
    lines = jnp.concatenate([g_hi, g_mid, g_lo, jnp.zeros((13, 2048), BF16)], axis=0)
    upl[0:16] = dense_up[:, own_span]
    upl[16:32] = jnp.where(c == 0, lines[:, 0:1024], lines[:, 1024:2048])
    landed(upp, rsem.at[12], "upp")
    upl[32:48] = upp[...]

    landed(wo, rsem.at[7], "wo")
    landed(precv_i.at[pl.ds(0, 15)], rsem.at[9], "mixer")
    columns_out = [dot(mx[k].reshape(16, 1024), wo[k].reshape(128, 1024), 1, 1) for k in range(2)]
    landed(tkz.at[pl.ds(0, NZ - 1)], rsem.at[11], "tkz")
    mine128 = tkz[:, :, pl.ds(pl.multiple_of(zc * 128, 128), 128)].reshape(16, 128)
    osend[...] = (mine128.astype(F32) + columns_out[0] + columns_out[1]).astype(BF16)
    holder = z // 4
    place8 = (z % 4) * 2 + c
    third = (z % 4) // 2
    for k in z_peers:
        send(osend, orecv.at[place8], ssem.at[10], osem.at[third], (k, y, x, holder))

    @pl.when(holder != c)
    def _():
        send(osend, orecv.at[place8], ssem.at[10], osem.at[third], partner)

    @pl.when(holder == c)
    def _():
        orecv[place8] = osend[...]

    near_group = third + (1 - 2 * third) * (holder + c - 2 * holder * c)
    own_rows = []
    for n in range(2):
        q = near_group + n * (1 - 2 * near_group)
        if n == 0:

            @pl.when(holder == c)
            def _():
                landed(orecv.at[pl.ds(0, 3)], osem.at[q], "out")

            @pl.when(holder != c)
            def _():
                landed(orecv.at[pl.ds(0, 4)], osem.at[q], "out")
        else:
            landed(orecv.at[pl.ds(0, 4)], osem.at[q], "out2")
        for i in range(4):
            rows[q, yx, :, i * 128 : (i + 1) * 128] = orecv[q * 4 + i]
        for j, i in yx_peers:
            send(rows.at[q, yx], rows.at[q, yx], ssem.at[12], planesem.at[y], (z, j, i, c))
    row_of = lax.broadcasted_iota(jnp.int32, (8, 16), 0) + 2 * z
    sel = (row_of == lax.broadcasted_iota(jnp.int32, (8, 16), 1)).astype(BF16)
    hown[...] = jnp.concatenate([dot(sel, rows[q, yx])[0:2] for q in range(2)], axis=1).astype(BF16)
    send(hown, hgot, ssem.at[22], rsem.at[21], partner)

    driven = step_wide * conv_inner
    first_row = lax.broadcasted_iota(jnp.int32, (8, 512), 0) == 0
    for s in range(2):
        for g in range(2):
            lhs = jnp.where(first_row, driven[s : s + 1, g * 512 : (g + 1) * 512], 0.0)
            rhs = jnp.broadcast_to(write_vec[s : s + 1, g * 128 : (g + 1) * 128], (8, 128))
            update = dot(lhs, rhs, 0, 0, highest).reshape(8, 64, 128)
            for h in range(8):
                head = g * 8 + h
                rate = jnp.broadcast_to(decay[s : s + 1, head : head + 1], (64, 128))
                hs[s, head] = rate * hs[s, head] + update[h]

    for i in (3, 4, 5):
        copies[i].wait()

    picked = None
    gain_half = second_gain[:, own_span]
    ones = jnp.ones((16, 1024), BF16)
    for d in (0, 1, 3, 2):
        j = y_at[d]
        landed(ww.at[pl.ds(0, 192 if d == 0 else 256)], planesem.at[j], "rows_yx")
        four = pl.ds(pl.multiple_of(j * NX, NX), NX)
        plain = jnp.concatenate(
            [rows[q, four].reshape(64, 512) for q in range(2)], axis=1
        ).astype(F32)
        block = (plain * gain_half).astype(BF16)
        got = dot(pt[pl.ds(pl.multiple_of(j * 64, 64), 64)][:, 0:32], block, 0, 0)
        picked = got if picked is None else picked + got
        if d == 2:
            pickm[...] = picked.astype(BF16)
            send(pickm, pickp, ssem.at[13], rsem.at[13], partner)
        pbuf[j] = jnp.concatenate(
            [dot(upl[...], block, 1, 1), dot(ones, (plain * plain).astype(BF16), 1, 1)], axis=0
        )
    sums = jnp.concatenate([pbuf[j] for j in range(NY)], axis=1)
    pmsg[...] = jnp.concatenate([sums[32:48], sums[16:24], sums[48:56]], axis=0)
    send(pmsg, pgot, ssem.at[18], rsem.at[18], partner)
    own16 = picked.astype(BF16)
    gate_pre = dot(own16, eg[own_span])
    up_pre = dot(own16, eu[own_span])
    landed(pickp, rsem.at[13], "pickp")
    landed(pgot, rsem.at[18], "pgot")
    gate_pre = gate_pre + dot(pickp[...], eg[other_span])
    up_pre = up_pre + dot(pickp[...], eu[other_span])
    pre = jnp.concatenate([sums[0:24], sums[48:56]], axis=0) + pgot[...]
    scale = lax.rsqrt(pre[24:25] * (1.0 / 2048.0) + norm_eps)
    slot_scale = jnp.sum(pk[...] * scale, axis=1, keepdims=True)
    weight = sigmoid(jnp.sum(pre[16:19], axis=0, keepdims=True) * scale)
    dact[...] = (silu(pre[0:16] * scale).astype(BF16).astype(F32) * weight).astype(BF16)
    send(dact, dactp, ssem.at[15], rsem.at[15], partner)
    gate_pre = gate_pre * slot_scale
    up_pre = up_pre * slot_scale
    glu_part = jnp.minimum(gate_pre, clamp_limit)
    lin_part = jnp.clip(up_pre, -clamp_limit, clamp_limit)
    activated = (glu_part * sigmoid(glu_alpha * glu_part) * (lin_part + 1.0)).astype(BF16)
    epart[...] = (dot(activated, ed[:, other_span]) * slot_weight).astype(BF16)
    send(epart, epartp, ssem.at[14], rsem.at[14], partner)
    own_part = dot(activated, ed[:, own_span]) * slot_weight
    landed(ddp, rsem.at[8], "ddp")
    landed(dactp, rsem.at[15], "dact")
    down = jnp.concatenate([dense_down[:, own_span], ddp[...]], axis=0)
    dense_both = jnp.concatenate([dact[...], dactp[...]], axis=0)
    dterm[...] = dot(dense_both, down[:, 0:WIDE], 0, 0).reshape(NY, 64, WIDE)
    dense_turned = dot(dense_both, perm[...]).astype(BF16)
    landed(epartp, rsem.at[14], "epart")
    both = (own_part + epartp[...].astype(F32)).astype(BF16)

    for d in (2, 1, 3, 0):
        j = y_at[d]
        span = pl.ds(pl.multiple_of(j * 64, 64), 64)
        total = dterm[j] + dot(pt[span][:, 0:32], both[:, 0:WIDE])
        tsum[pl.ds(pl.multiple_of(j * NX, NX), NX)] = total.astype(BF16).reshape(NX, 16, WIDE)
        for e in (2, 1, 3) if d == 0 else (2, 1, 3, 0):
            i = x_at[e]
            send(tsum.at[j * NX + i], prs.at[yx], ssem.at[16], rsem.at[19], (z, j, i, c))
    prs[yx] = tsum[yx]
    first_z = dot(
        jnp.concatenate([dense_turned, pz[...]], axis=0),
        jnp.concatenate([down[:, WIDE:], both[:, WIDE:]], axis=0), 0, 0,
    )
    zsum[...] = first_z.astype(BF16).reshape(NZ, 32, 1024 - WIDE)
    for k in z_peers:
        send(zsum.at[k], zrs.at[z], ssem.at[20], rsem.at[16], (k, y, x, c))
    zrs[z] = zsum[z]
    landed(zrs.at[pl.ds(0, NZ - 1)], rsem.at[16], "sum_z1")
    zsend[...] = jnp.sum(zrs[...].astype(F32), axis=0).astype(BF16).reshape(NYX, 2, 1024 - WIDE)
    for j, i in yx_peers:
        for e in c_at:
            send(zsend.at[j * NX + i], zrecv.at[yx * 2 + c], ssem.at[21], rsem.at[20], (z, j, i, e))
    send(zsend.at[yx], zrecv.at[yx * 2 + c], ssem.at[21], rsem.at[20], partner)
    zrecv[yx * 2 + c] = zsend[yx]
    landed(prs.at[pl.ds(0, NYX - 1)], rsem.at[19], "sum_yx")
    fsend[...] = jnp.sum(prs[...].astype(F32), axis=0).astype(BF16).reshape(NZ, 2, WIDE)
    for k, e in zc_peers:
        send(fsend.at[k], frecv.at[zc], ssem.at[17], rsem.at[17], (k, y, x, e))
    frecv[zc] = fsend[z]
    landed(zrecv.at[pl.ds(0, 31)], rsem.at[20], "sum_yx2")
    narrow = [sum(zrecv[2 * i + k].astype(F32) for i in range(NYX)) for k in range(2)]
    landed(frecv.at[pl.ds(0, 15)], rsem.at[17], "sum_z")
    final = []
    for k in range(2):
        total = frecv[k].astype(F32)
        for i in range(1, NZ):
            total = total + frecv[2 * i + k].astype(F32)
        final += [total, narrow[k]]
    landed(hgot, rsem.at[21], "hgot")
    own_half, other_half = hown[...].astype(F32), hgot[...].astype(F32)
    hidden = jnp.concatenate(
        [jnp.where(c == 0, own_half, other_half), jnp.where(c == 0, other_half, own_half)], axis=1
    )
    result = hidden + jnp.concatenate(final, axis=1)
    layer_out[...] = jnp.where(c == 0, result[0:1], result[1:2]).astype(BF16)

    for i, ref in enumerate((
        tok.at[pl.ds(0, NZY - 1)], wi.at[pl.ds(0, NX - 1)], wg.at[pl.ds(0, NX - 1)],
        rts.at[pl.ds(0, NZ - 1)], psend_i.at[pl.ds(0, NZY - 1)], psend_g.at[pl.ds(0, NZY - 1)],
        rts.at[pl.ds(0, 120)], None, ddp, precv_i.at[pl.ds(0, 15)],
        None, tkz.at[pl.ds(0, NZ - 1)], ww.at[pl.ds(0, 960)],
        pickm, epart, dact, prs.at[pl.ds(0, NYX - 1)], frecv.at[pl.ds(0, 15)], pmsg, upp,
        zrs.at[pl.ds(0, NZ - 1)], zrecv.at[pl.ds(0, 31)], hown,
    )):
        if ref is not None:
            landed(ref, ssem.at[i])

    @pl.when(keeper == c)
    def _():
        landed(ww.at[pl.ds(0, 960)], ssem.at[7])

    @pl.when(keeper != c)
    def _():
        landed(wo, ssem.at[7])

    @pl.when(holder == c)
    def _():
        landed(orecv.at[pl.ds(0, NZ - 1)], ssem.at[10])

    @pl.when(holder != c)
    def _():
        landed(orecv, ssem.at[10])


def write_kernel(*refs):
    sems = refs[8]
    copies = [pltpu.make_async_copy(refs[i], refs[4 + i], sems.at[i]) for i in range(4)]
    for i in (3, 0, 1, 2):
        copies[i].start()
    for copy in copies:
        copy.wait()


def local(
    tokens, head_state, conv_state, conv_proj_state, first_gain, gate_weight, inner_weight,
    write_weight, read_weight, step_weight, conv_kernel, conv_proj_kernel, step_bias, log_rate,
    skip_gain, group_gain, out_weight, second_gain, routes, route_logits, expert_gate, expert_up,
    expert_down, dense_up, dense_down, dense_gate,
):
    near = [
        tokens, first_gain[None], step_weight.T, conv_state.transpose(1, 0, 2), conv_proj_state,
        conv_kernel, conv_proj_kernel, step_bias[None], log_rate[None], skip_gain[None],
        group_gain[None], second_gain[None], routes, route_logits, dense_up.T, dense_down,
        dense_gate[None],
    ]
    far = [
        out_weight.T, head_state, gate_weight, inner_weight, write_weight, read_weight, expert_gate,
        expert_up, expert_down,
    ]
    vmem = pl.BlockSpec(memory_space=pltpu.VMEM)
    anywhere = pl.BlockSpec(memory_space=pltpu.HBM)
    V = pltpu.VMEM
    outs = (
        jax.ShapeDtypeStruct((1, 2048), BF16),
        jax.ShapeDtypeStruct((3, 2, 1024), BF16),
        jax.ShapeDtypeStruct((2, 3, 2, 256), BF16),
        jax.ShapeDtypeStruct((2, 16, 64, 128), F32),
    )
    results = pl.pallas_call(
        layer_kernel,
        out_shape=tuple(V(o.shape, o.dtype) for o in outs),
        in_specs=[anywhere] * (len(near) + len(far)),
        out_specs=(vmem, vmem, vmem, vmem),
        scratch_shapes=[
            *[V(a.shape, a.dtype) for a in near],
            V((2048, 256), BF16), V((2048, 256), BF16),
            V((2048, 512), BF16), V((2048, 512), BF16), V((512, 2048), BF16),
            V((NX, 16, 1024), BF16), V((NX, 16, 1024), BF16),
            V((16, 2, 128), BF16), V((NZY, 2, 128), BF16),
            V((NZY, 2, 1024), BF16), V((NZY, 2, 1024), BF16),
            V((NZY, 2, 1024), BF16), V((NZY, 2, 1024), BF16),
            V((128, 2, 256), BF16), V((2, 8, 16, 1024), BF16), V((2, NZ, 2, 1024), BF16),
            V((16, 128), BF16), V((8, 16, 128), BF16), V((NZ, 2, 2048), BF16), V((2, 1024), BF16),
            V((2, 1024), BF16),
            V((2, NYX, 16, 512), BF16), V((16, 1024), BF16), V((16, 256), BF16), V((16, 256), BF16),
            V((32, 1024), BF16), V((32, 1024), BF16),
            V((NYX, 16, WIDE), BF16), V((NYX, 16, WIDE), BF16), V((NZ, 2, WIDE), BF16),
            V((2 * NZ, 2, WIDE), BF16), V((256, 128), BF16), V((48, 1024), BF16),
            V((16, 1024), BF16), V((NY, 64, 64), F32), V((32, 256), F32), V((32, 256), F32),
            V((32, 1024), BF16), V((32, 1024), BF16), V((NY, 64, WIDE), F32),
            V((256, 256), BF16), V((32, 256), BF16), V((NZ, 32, 1024 - WIDE), BF16),
            V((NZ, 32, 1024 - WIDE), BF16), V((NYX, 2, 1024 - WIDE), BF16),
            V((2 * NYX, 2, 1024 - WIDE), BF16), V((32, 256), F32),
            pltpu.SemaphoreType.DMA((8,)), pltpu.SemaphoreType.DMA((23,)),
            pltpu.SemaphoreType.DMA((23,)), pltpu.SemaphoreType.DMA((NY,)),
            pltpu.SemaphoreType.DMA((2,)),
        ],
        compiler_params=pltpu.CompilerParams(
            collective_id=0, has_side_effects=True, vmem_limit_bytes=56 * 1024 * 1024
        ),
        cost_estimate=pl.CostEstimate(flops=2 * 10**9, bytes_accessed=16 * 2**20, transcendentals=10**5),
        name="layer",
    )(*near, *far)
    results = [pltpu.with_memory_space_constraint(r, V) for r in results]
    layer_out, conv_out, conv_proj_out, state_out = pl.pallas_call(
        write_kernel,
        out_shape=outs,
        in_specs=[vmem] * 4,
        out_specs=[anywhere] * 4,
        scratch_shapes=[pltpu.SemaphoreType.DMA((4,))],
        name="write",
    )(*results)
    return (layer_out, state_out, conv_out.transpose(1, 0, 2), conv_proj_out)


def solution(mesh):
    torus = Mesh(mesh.devices.reshape(NZ, NY, NX, mesh.shape["tp"]), EP_TP)
    return jax.shard_map(
        local,
        mesh=torus,
        in_specs=(
            P(EP, None), P(EP, "tp", None, None), P(EP, None, "tp"), P(EP, None, None, "tp"), P(),
            P(EP, "tp"), P(EP, "tp"), P(None, "tp"), P(None, "tp"), P(None, "tp"), P(None, "tp"),
            P(None, None, "tp"), P("tp"), P("tp"), P("tp"), P("tp"), P("tp", EP), P(), P(EP, None),
            P(EP, None), P(EP, None, "tp"), P(EP, None, "tp"), P(EP, "tp", None), P(None, EP_TP),
            P(EP_TP, None), P(),
        ),
        out_specs=(
            P(EP_TP, None), P(EP, "tp", None, None), P(EP, None, "tp"), P(EP, None, None, "tp"),
        ),
        check_vma=False,
    )
```

```python
import functools

import jax
import jax.numpy as jnp
from jax import lax
from jax.experimental import pallas as pl
from jax.experimental.pallas import tpu as pltpu
from jax.sharding import Mesh
from jax.sharding import PartitionSpec as P

EP = ("ep_0", "ep_1", "ep_2")
EP_TP = ("ep_0", "ep_1", "ep_2", "tp")
MESH = pl.DeviceIdType.MESH
F32 = jnp.float32
BF16 = jnp.bfloat16
norm_eps = 1e-05
clamp_limit = 7.0
glu_alpha = 1.702
highest = lax.Precision.HIGHEST
NZ, NY, NX = 8, 4, 4
NZY, NYX = NZ * NY, NY * NX
FAR = 12
WIDE = 768


sigmoid = jax.nn.sigmoid
silu = jax.nn.silu


def softplus(v):
    return jnp.maximum(v, 0.0) + jnp.log1p(jnp.exp(-jnp.abs(v)))


def dot(a, b, ca=1, cb=0, precision=None):
    return lax.dot_general(
        a, b, (((ca,), (cb,)), ((), ())), precision=precision, preferred_element_type=F32
    )


def rms_scale(values, gain_vec):
    return values * lax.rsqrt(jnp.mean(values * values, axis=-1, keepdims=True) + norm_eps) * gain_vec


NEAR = 17


def layer_kernel(*refs):
    near_hbm, refs = refs[:NEAR], refs[NEAR:]
    (
        out_weight, head_state, gate_weight, inner_weight, write_weight, read_weight, expert_gate,
        expert_up, expert_down, layer_out, conv_out, conv_proj_out, hs,
    ) = refs[:13]
    near, refs = refs[13 : 13 + NEAR], refs[13 + NEAR :]
    (
        tokens, first_gain, step_weight, conv_state, conv_proj_state, conv_kernel, conv_proj_kernel,
        step_bias, log_rate, skip_gain, group_gain, second_gain, routes, route_logits, dense_up,
        dense_down, dense_gate,
    ) = near
    (
        ww, rw, eg, eu, ed, wg, wi, nblk, tok, psend_i, psend_g, precv_i, precv_g, rts, wo, mx,
        osend, orecv, tkz, hown, hgot, rows, ddp, dact, dactp, epart, epartp, tsum, prs, fsend, frecv,
        pt, upl, upp, pbuf, pmsg, pgot, pickm, pickp, dterm, perm, pz, zsum,
        zrs, zsend, zrecv, pk, lsem, ssem, rsem, planesem, osem,
    ) = refs
    z, y, x, c = [lax.axis_index(n) for n in EP_TP]
    zy = z * NY + y
    yx = y * NX + x
    zc = z * 2 + c
    expert = zy * NX + x
    base = yx * NZ
    other = 1 - c
    partner = (z, y, x, other)

    z_at = [lax.rem(z + d, NZ) for d in range(NZ)]
    y_at = [lax.rem(y + d, NY) for d in range(NY)]
    x_at = [lax.rem(x + d, NX) for d in range(NX)]
    c_at = [c, other]
    zy_peers = [(z_at[d], y_at[e]) for d in (4, 3, 5, 2, 6, 1, 7, 0) for e in (2, 1, 3, 0)][:-1]
    yx_peers = [(y_at[d], x_at[e]) for d in (2, 1, 3, 0) for e in (2, 1, 3, 0)][:-1]
    zc_peers = [(z_at[d], c_at[e]) for d in (4, 3, 5, 2, 6, 1, 7, 0) for e in (1, 0)][:-1]
    z_peers = [z_at[d] for d in (4, 3, 5, 2, 6, 1, 7)]

    def send(src, dst, s, r, device):
        pltpu.make_async_remote_copy(
            src_ref=src, dst_ref=dst, send_sem=s, recv_sem=r, device_id=device, device_id_type=MESH
        ).start()

    def landed(ref, sem, name="tail"):
        with jax.named_scope(name):
            pltpu.make_async_copy(ref, ref, sem).wait()

    barrier = pltpu.get_barrier_semaphore()

    def hello(device):
        pl.semaphore_signal(barrier, inc=1, device_id=device, device_id_type=MESH)

    for k, j in zy_peers:
        hello((k, j, x, c))
    for j, i in yx_peers:
        hello((z, j, i, c))
        hello((z, j, i, other))
    hello(partner)
    for k in z_peers:
        hello((k, y, x, other))

    small = [pltpu.make_async_copy(a, b, ssem.at[i]) for i, (a, b) in enumerate(zip(near_hbm, near))]
    loads = [
        (write_weight, ww), (read_weight, rw), (head_state, hs), (expert_gate.at[0], eg),
        (expert_up.at[0], eu), (expert_down.at[0], ed), (gate_weight, wg.at[x]),
        (inner_weight, wi.at[x]),
    ]
    copies = [pltpu.make_async_copy(a, b, lsem.at[i]) for i, (a, b) in enumerate(loads)]
    for copy in [*small, copies[7], copies[6]]:
        copy.start()
    small[0].wait()
    small[1].wait()

    normed = rms_scale(tokens[...].astype(F32), first_gain[...]).astype(BF16)
    for b in range(16):
        nblk[b] = normed[:, b * 128 : (b + 1) * 128]
    tok[zy] = nblk[zy // 2]
    tkz[z] = tokens[...]
    with jax.named_scope("small"):
        for copy in [*small[2:], copies[7], copies[6]]:
            copy.wait()
    blank = jnp.zeros((2, 124), F32)
    rts[base + z] = jnp.concatenate(
        [routes[...].astype(F32), blank, route_logits[...].astype(F32), blank], axis=1
    ).astype(BF16)

    with jax.named_scope("barrier"):
        pl.semaphore_wait(barrier, (NZY - 1) + (2 * NYX - 1) + (NZ - 1))

    for i in (x_at[2], x_at[1], x_at[3]):
        send(wi.at[x], wi.at[x], ssem.at[1], rsem.at[1], (z, y, i, c))
    for n, (k, j) in enumerate(zy_peers):
        arrival = rsem.at[0] if n < FAR else rsem.at[22]
        send(nblk.at[k * 2 + j // 2], tok.at[zy], ssem.at[0], arrival, (k, j, x, c))
    for k in z_peers:
        send(rts.at[base + z], rts.at[base + z], ssem.at[3], rsem.at[3], (k, y, x, c))
    for i in (x_at[2], x_at[1], x_at[3]):
        send(wg.at[x], wg.at[x], ssem.at[2], rsem.at[2], (z, y, i, c))
    for k in z_peers:
        send(tkz.at[z], tkz.at[z], ssem.at[11], rsem.at[11], (k, y, x, c))
    keeper = yx // 8
    place = wo.at[c, yx % 8]

    for j, i in yx_peers:
        send(out_weight, place, ssem.at[7], rsem.at[7], (z, j, i, keeper))

    @pl.when(keeper == c)
    def _():
        pltpu.make_async_copy(out_weight, place, rsem.at[7]).start()

    @pl.when(keeper != c)
    def _():
        send(out_weight, place, ssem.at[7], rsem.at[7], partner)


    for i in (0, 1, 2, 3, 4, 5):
        copies[i].start()
    with jax.named_scope("ww"):
        copies[0].wait()
        copies[1].wait()
    write_proj = dot(normed, ww[...]).astype(BF16)
    read_proj = dot(normed, rw[...]).astype(BF16)
    step_raw = dot(normed, step_weight[...], 1, 1)

    low = (y % 2) == 0

    def padded(weights):
        weight = weights.reshape(64, 1024)[...]
        zero = jnp.zeros_like(weight)
        return jnp.concatenate([jnp.where(low, weight, zero), jnp.where(low, zero, weight)], axis=0)

    def terms(lhs, rhs, out, places):
        result = dot(lhs, rhs).astype(BF16)
        for n, d in enumerate(places):
            span = pl.ds(pl.multiple_of(z_at[d] * NY, NY), NY)
            out[span] = result[8 * n : 8 * n + 8].reshape(NY, 2, 1024)

    def tokens_of(places):
        spans = [pl.ds(pl.multiple_of(z_at[d] * NY, NY), NY) for d in places]
        return jnp.concatenate([tok[span].reshape(2 * NY, 128) for span in spans], axis=0)

    def scatter(out, into, n, peers):
        for k, j in peers:
            send(out.at[k * NY + j], into.at[zy], ssem.at[n], rsem.at[n], (k, j, x, c))

    near, far = (2, 6, 1, 7, 0), (4, 3, 5)
    landed(wi.at[pl.ds(0, NX - 1)], rsem.at[1], "wi")
    landed(tok.at[pl.ds(0, NZY - 1 - FAR)], rsem.at[22], "tok_near")
    inner_rows = padded(wi)
    near_tok = tokens_of(near)
    terms(near_tok, inner_rows, psend_i, near)
    scatter(psend_i, precv_i, 4, zy_peers[FAR:])
    landed(rts.at[pl.ds(0, NZ - 1)], rsem.at[3], "rt_z")
    mine8 = pl.ds(base, NZ)
    for j, i in yx_peers:
        send(rts.at[mine8], rts.at[mine8], ssem.at[6], rsem.at[6], (z, j, i, c))
    landed(tok.at[pl.ds(0, FAR)], rsem.at[0], "tok")
    far_tok = tokens_of(far)
    terms(far_tok, inner_rows, psend_i, far)
    scatter(psend_i, precv_i, 4, zy_peers[:FAR])
    landed(wg.at[pl.ds(0, NX - 1)], rsem.at[2], "wg")
    gate_rows = padded(wg)
    terms(far_tok, gate_rows, psend_g, far)
    scatter(psend_g, precv_g, 5, zy_peers[:FAR])
    terms(near_tok, gate_rows, psend_g, near)
    scatter(psend_g, precv_g, 5, zy_peers[FAR:])
    precv_i[zy] = psend_i[zy]
    precv_g[zy] = psend_g[zy]
    own_span = pl.ds(pl.multiple_of(c * 1024, 1024), 1024)
    other_span = pl.ds(pl.multiple_of(other * 1024, 1024), 1024)
    send(dense_down.at[:, other_span], ddp, ssem.at[8], rsem.at[8], partner)
    send(dense_up.at[:, other_span], upp, ssem.at[19], rsem.at[12], partner)

    cps = conv_proj_state[...].astype(F32)
    cpk = conv_proj_kernel[...]

    def conv_of(w, fresh):
        total = fresh.astype(F32) * cpk[3, w : w + 1]
        for i in range(3):
            total = total + cps[:, i, w, :] * cpk[i, w : w + 1]
        return silu(total)

    write_vec = conv_of(0, write_proj)
    read_vec = conv_of(1, read_proj)
    step_size = softplus(step_raw + step_bias[...])
    decay = jnp.exp(-jnp.exp(log_rate[...]) * step_size)
    head_of = lax.broadcasted_iota(jnp.int32, (16, 1024), 1) // 64
    spread = (head_of == lax.broadcasted_iota(jnp.int32, (16, 1024), 0)).astype(F32)
    step_wide = dot(step_size, spread, precision=highest)
    skip_wide = dot(skip_gain[...], spread, precision=highest)
    decay_wide = dot(decay, spread, precision=highest)
    ck = conv_kernel[...]
    early = sum(conv_state[i].astype(F32) * ck[i : i + 1] for i in range(3))
    for i in range(2):
        conv_out[i] = conv_state[i + 1]
        conv_proj_out[:, i] = conv_proj_state[:, i + 1]
    for s in range(2):
        conv_proj_out[s, 2] = jnp.concatenate([write_proj[s : s + 1], read_proj[s : s + 1]], axis=0)
    copies[2].wait()
    held, met = [], []
    for s in range(2):
        for g in range(2):
            span = slice(g * 128, (g + 1) * 128)
            reader = read_vec[s : s + 1, span]
            group = hs[s, g * 8 : (g + 1) * 8].reshape(512, 128)
            held.append(dot(jnp.broadcast_to(reader, (8, 128)), group, 1, 1, highest)[0:1])
            product = jnp.sum(write_vec[s : s + 1, span] * reader, axis=1, keepdims=True)
            met.append(jnp.broadcast_to(product, (1, 512)))

    def by_sequence(four):
        return jnp.concatenate(
            [jnp.concatenate(four[0:2], axis=1), jnp.concatenate(four[2:4], axis=1)], axis=0
        )

    kept = decay_wide * by_sequence(held)
    direct = step_wide * by_sequence(met) + skip_wide

    landed(precv_i.at[pl.ds(0, NZY - 1)], rsem.at[4], "p_inner")
    inner_proj = jnp.sum(precv_i[...].astype(F32), axis=0).astype(BF16)
    conv_out[2] = inner_proj
    conv_inner = silu(early + inner_proj.astype(F32) * ck[3:4])
    read_out = kept + direct * conv_inner

    landed(precv_g.at[pl.ds(0, NZY - 1)], rsem.at[5], "p_gate")
    gate_proj = jnp.sum(precv_g[...].astype(F32), axis=0).astype(BF16)
    gated = read_out * silu(gate_proj.astype(F32))
    parts = []
    for g in range(2):
        part = gated[:, g * 512 : (g + 1) * 512]
        parts.append(part * lax.rsqrt(jnp.mean(part * part, axis=-1, keepdims=True) + norm_eps))
    mx[c, z] = (jnp.concatenate(parts, axis=1) * group_gain[...]).astype(BF16)
    for k, e in zc_peers:
        send(mx.at[c, z], mx.at[c, z], ssem.at[9], rsem.at[9], (k, y, x, e))

    landed(rts.at[pl.ds(0, 120)], rsem.at[6], "rt_yx")
    table = rts.reshape(256, 256)[...].astype(F32)
    names, scores = table[:, 0:128], table[:, 128:256]
    lane = lax.broadcasted_iota(jnp.int32, (256, 128), 1)
    live = lane < 4
    hit = jnp.where(live & (names == expert.astype(F32)), 1.0, 0.0)
    shifted = jnp.where(live, scores, -3e38)
    grown = jnp.where(live, jnp.exp(shifted - jnp.max(shifted, axis=1, keepdims=True)), 0.0)
    row_weight = jnp.sum(hit * grown, axis=1, keepdims=True) / jnp.sum(grown, axis=1, keepdims=True)
    chosen = jnp.broadcast_to(jnp.sum(hit, axis=1, keepdims=True), (256, 128))
    rr = lax.broadcasted_iota(jnp.int32, (256, 256), 0)
    cc = lax.broadcasted_iota(jnp.int32, (256, 256), 1)
    chosen16 = chosen.astype(BF16)
    count_col = dot((cc <= rr).astype(BF16), chosen16)
    count_row = dot(chosen16, (rr <= cc).astype(BF16), 0, 0)[0:32]
    chosen_row = dot(chosen16, (rr == cc).astype(BF16), 0, 0)[0:32]
    slot = lax.broadcasted_iota(jnp.int32, (32, 256), 0).astype(F32)
    picks = jnp.where((count_row - 1.0 == slot) & (chosen_row > 0.5), 1.0, 0.0)
    picks_t = jnp.where((count_col - 1.0 == lane.astype(F32)) & (chosen > 0.5), 1.0, 0.0)
    slot_weight = dot(picks, jnp.broadcast_to(row_weight, (256, 128)), precision=highest)[:, 0:1]
    pt[...] = picks_t.astype(BF16)
    pk[...] = picks
    turned = ((cc >> 1) & 15) * 16 + (cc >> 5) * 2 + (cc & 1)
    perm[...] = (rr == turned).astype(BF16)
    pz[...] = dot(picks.astype(BF16), perm[...]).astype(BF16)
    gate_line = dense_gate[...]
    g_hi = gate_line.astype(BF16)
    g_mid = (gate_line - g_hi.astype(F32)).astype(BF16)
    g_lo = (gate_line - g_hi.astype(F32) - g_mid.astype(F32)).astype(BF16)
    lines = jnp.concatenate([g_hi, g_mid, g_lo, jnp.zeros((13, 2048), BF16)], axis=0)
    upl[0:16] = dense_up[:, own_span]
    upl[16:32] = jnp.where(c == 0, lines[:, 0:1024], lines[:, 1024:2048])
    landed(upp, rsem.at[12], "upp")
    upl[32:48] = upp[...]

    landed(wo, rsem.at[7], "wo")
    landed(precv_i.at[pl.ds(0, 15)], rsem.at[9], "mixer")
    columns_out = [dot(mx[k].reshape(16, 1024), wo[k].reshape(128, 1024), 1, 1) for k in range(2)]
    landed(tkz.at[pl.ds(0, NZ - 1)], rsem.at[11], "tkz")
    mine128 = tkz[:, :, pl.ds(pl.multiple_of(zc * 128, 128), 128)].reshape(16, 128)
    osend[...] = (mine128.astype(F32) + columns_out[0] + columns_out[1]).astype(BF16)
    holder = z // 4
    place8 = (z % 4) * 2 + c
    third = (z % 4) // 2
    for k in z_peers:
        send(osend, orecv.at[place8], ssem.at[10], osem.at[third], (k, y, x, holder))

    @pl.when(holder != c)
    def _():
        send(osend, orecv.at[place8], ssem.at[10], osem.at[third], partner)

    @pl.when(holder == c)
    def _():
        orecv[place8] = osend[...]

    near_group = third + (1 - 2 * third) * (holder + c - 2 * holder * c)
    own_rows = []
    for n in range(2):
        q = near_group + n * (1 - 2 * near_group)
        if n == 0:

            @pl.when(holder == c)
            def _():
                landed(orecv.at[pl.ds(0, 3)], osem.at[q], "out")

            @pl.when(holder != c)
            def _():
                landed(orecv.at[pl.ds(0, 4)], osem.at[q], "out")
        else:
            landed(orecv.at[pl.ds(0, 4)], osem.at[q], "out2")
        for i in range(4):
            rows[q, yx, :, i * 128 : (i + 1) * 128] = orecv[q * 4 + i]
        for j, i in yx_peers:
            send(rows.at[q, yx], rows.at[q, yx], ssem.at[12], planesem.at[q * NY + y], (z, j, i, c))
    row_of = lax.broadcasted_iota(jnp.int32, (8, 16), 0) + 2 * z
    sel = (row_of == lax.broadcasted_iota(jnp.int32, (8, 16), 1)).astype(BF16)
    hown[...] = jnp.concatenate([dot(sel, rows[q, yx])[0:2] for q in range(2)], axis=1).astype(BF16)
    send(hown, hgot, ssem.at[22], rsem.at[21], partner)

    driven = step_wide * conv_inner
    first_row = lax.broadcasted_iota(jnp.int32, (8, 512), 0) == 0
    for s in range(2):
        for g in range(2):
            lhs = jnp.where(first_row, driven[s : s + 1, g * 512 : (g + 1) * 512], 0.0)
            rhs = jnp.broadcast_to(write_vec[s : s + 1, g * 128 : (g + 1) * 128], (8, 128))
            update = dot(lhs, rhs, 0, 0, highest).reshape(8, 64, 128)
            for h in range(8):
                head = g * 8 + h
                rate = jnp.broadcast_to(decay[s : s + 1, head : head + 1], (64, 128))
                hs[s, head] = rate * hs[s, head] + update[h]

    for i in (3, 4, 5):
        copies[i].wait()

    ones = jnp.ones((16, 512), BF16)
    own16 = []
    for n in range(2):
        q = near_group + n * (1 - 2 * near_group)
        within = pl.ds(pl.multiple_of(q * 512, 512), 512)
        span = pl.ds(pl.multiple_of(c * 1024 + q * 512, 512), 512)
        gain_part = second_gain[:, span]
        picked = None
        for d in (2, 1, 3, 0):
            j = y_at[d]
            landed(ww.at[pl.ds(0, 96 if d == 0 else 128)], planesem.at[q * NY + j], "rows_yx")
            plain = rows[q, pl.ds(pl.multiple_of(j * NX, NX), NX)].reshape(64, 512).astype(F32)
            block = (plain * gain_part).astype(BF16)
            got = dot(pt[pl.ds(pl.multiple_of(j * 64, 64), 64)][:, 0:32], block, 0, 0)
            picked = got if picked is None else picked + got
            if d == 0:
                pickm[q] = picked.astype(BF16)
                arrival = rsem.at[13 + 10 * n]
                send(pickm.at[q], pickp.at[q], ssem.at[13 + 10 * n], arrival, partner)
            both_sums = jnp.concatenate(
                [dot(upl[:, within], block, 1, 1), dot(ones, (plain * plain).astype(BF16), 1, 1)],
                axis=0,
            )
            pbuf[j] = both_sums if n == 0 else pbuf[j] + both_sums
        own16.append(picked.astype(BF16))
        if n == 0:
            gate_pre = dot(own16[0], eg[span])
            up_pre = dot(own16[0], eu[span])
    sums = jnp.concatenate([pbuf[j] for j in range(NY)], axis=1)
    pmsg[...] = jnp.concatenate([sums[32:48], sums[16:24], sums[48:56]], axis=0)
    send(pmsg, pgot, ssem.at[18], rsem.at[18], partner)
    gate_pre = gate_pre + dot(own16[1], eg[span])
    up_pre = up_pre + dot(own16[1], eu[span])
    landed(pickp.at[0], rsem.at[13], "pickp")
    landed(pickp.at[0], rsem.at[23], "pickp2")
    other16 = jnp.concatenate([pickp[0], pickp[1]], axis=1)
    landed(pgot, rsem.at[18], "pgot")
    gate_pre = gate_pre + dot(other16, eg[other_span])
    up_pre = up_pre + dot(other16, eu[other_span])
    pre = jnp.concatenate([sums[0:24], sums[48:56]], axis=0) + pgot[...]
    scale = lax.rsqrt(pre[24:25] * (1.0 / 2048.0) + norm_eps)
    slot_scale = jnp.sum(pk[...] * scale, axis=1, keepdims=True)
    weight = sigmoid(jnp.sum(pre[16:19], axis=0, keepdims=True) * scale)
    dact[...] = (silu(pre[0:16] * scale).astype(BF16).astype(F32) * weight).astype(BF16)
    send(dact, dactp, ssem.at[15], rsem.at[15], partner)
    gate_pre = gate_pre * slot_scale
    up_pre = up_pre * slot_scale
    glu_part = jnp.minimum(gate_pre, clamp_limit)
    lin_part = jnp.clip(up_pre, -clamp_limit, clamp_limit)
    activated = (glu_part * sigmoid(glu_alpha * glu_part) * (lin_part + 1.0)).astype(BF16)
    epart[...] = (dot(activated, ed[:, other_span]) * slot_weight).astype(BF16)
    send(epart, epartp, ssem.at[14], rsem.at[14], partner)
    own_part = dot(activated, ed[:, own_span]) * slot_weight
    landed(ddp, rsem.at[8], "ddp")
    landed(dactp, rsem.at[15], "dact")
    down = jnp.concatenate([dense_down[:, own_span], ddp[...]], axis=0)
    dense_both = jnp.concatenate([dact[...], dactp[...]], axis=0)
    dterm[...] = dot(dense_both, down[:, 0:WIDE], 0, 0).reshape(NY, 64, WIDE)
    dense_turned = dot(dense_both, perm[...]).astype(BF16)
    landed(epartp, rsem.at[14], "epart")
    both = (own_part + epartp[...].astype(F32)).astype(BF16)

    for d in (2, 1, 3, 0):
        j = y_at[d]
        span = pl.ds(pl.multiple_of(j * 64, 64), 64)
        total = dterm[j] + dot(pt[span][:, 0:32], both[:, 0:WIDE])
        tsum[pl.ds(pl.multiple_of(j * NX, NX), NX)] = total.astype(BF16).reshape(NX, 16, WIDE)
        for e in (2, 1, 3) if d == 0 else (2, 1, 3, 0):
            i = x_at[e]
            send(tsum.at[j * NX + i], prs.at[yx], ssem.at[16], rsem.at[19], (z, j, i, c))
    prs[yx] = tsum[yx]
    first_z = dot(
        jnp.concatenate([dense_turned, pz[...]], axis=0),
        jnp.concatenate([down[:, WIDE:], both[:, WIDE:]], axis=0), 0, 0,
    )
    zsum[...] = first_z.astype(BF16).reshape(NZ, 32, 1024 - WIDE)
    for k in z_peers:
        send(zsum.at[k], zrs.at[z], ssem.at[20], rsem.at[16], (k, y, x, c))
    zrs[z] = zsum[z]
    landed(zrs.at[pl.ds(0, NZ - 1)], rsem.at[16], "sum_z1")
    zsend[...] = jnp.sum(zrs[...].astype(F32), axis=0).astype(BF16).reshape(NYX, 2, 1024 - WIDE)
    for j, i in yx_peers:
        for e in c_at:
            send(zsend.at[j * NX + i], zrecv.at[yx * 2 + c], ssem.at[21], rsem.at[20], (z, j, i, e))
    send(zsend.at[yx], zrecv.at[yx * 2 + c], ssem.at[21], rsem.at[20], partner)
    zrecv[yx * 2 + c] = zsend[yx]
    landed(prs.at[pl.ds(0, NYX - 1)], rsem.at[19], "sum_yx")
    fsend[...] = jnp.sum(prs[...].astype(F32), axis=0).astype(BF16).reshape(NZ, 2, WIDE)
    for k, e in zc_peers:
        send(fsend.at[k], frecv.at[zc], ssem.at[17], rsem.at[17], (k, y, x, e))
    frecv[zc] = fsend[z]
    landed(zrecv.at[pl.ds(0, 31)], rsem.at[20], "sum_yx2")
    narrow = [sum(zrecv[2 * i + k].astype(F32) for i in range(NYX)) for k in range(2)]
    landed(frecv.at[pl.ds(0, 15)], rsem.at[17], "sum_z")
    final = []
    for k in range(2):
        total = frecv[k].astype(F32)
        for i in range(1, NZ):
            total = total + frecv[2 * i + k].astype(F32)
        final += [total, narrow[k]]
    landed(hgot, rsem.at[21], "hgot")
    own_half, other_half = hown[...].astype(F32), hgot[...].astype(F32)
    hidden = jnp.concatenate(
        [jnp.where(c == 0, own_half, other_half), jnp.where(c == 0, other_half, own_half)], axis=1
    )
    result = hidden + jnp.concatenate(final, axis=1)
    layer_out[...] = jnp.where(c == 0, result[0:1], result[1:2]).astype(BF16)

    for i, ref in enumerate((
        tok.at[pl.ds(0, NZY - 1)], wi.at[pl.ds(0, NX - 1)], wg.at[pl.ds(0, NX - 1)],
        rts.at[pl.ds(0, NZ - 1)], psend_i.at[pl.ds(0, NZY - 1)], psend_g.at[pl.ds(0, NZY - 1)],
        rts.at[pl.ds(0, 120)], None, ddp, precv_i.at[pl.ds(0, 15)],
        None, tkz.at[pl.ds(0, NZ - 1)], ww.at[pl.ds(0, 960)],
        pickm.at[0], epart, dact, prs.at[pl.ds(0, NYX - 1)], frecv.at[pl.ds(0, 15)], pmsg, upp,
        zrs.at[pl.ds(0, NZ - 1)], zrecv.at[pl.ds(0, 31)], hown,
        pickm.at[0],
    )):
        if ref is not None:
            landed(ref, ssem.at[i])

    @pl.when(keeper == c)
    def _():
        landed(ww.at[pl.ds(0, 960)], ssem.at[7])

    @pl.when(keeper != c)
    def _():
        landed(wo, ssem.at[7])

    @pl.when(holder == c)
    def _():
        landed(orecv.at[pl.ds(0, NZ - 1)], ssem.at[10])

    @pl.when(holder != c)
    def _():
        landed(orecv, ssem.at[10])


def write_kernel(*refs):
    sems = refs[8]
    copies = [pltpu.make_async_copy(refs[i], refs[4 + i], sems.at[i]) for i in range(4)]
    for i in (3, 0, 1, 2):
        copies[i].start()
    for copy in copies:
        copy.wait()


def local(
    tokens, head_state, conv_state, conv_proj_state, first_gain, gate_weight, inner_weight,
    write_weight, read_weight, step_weight, conv_kernel, conv_proj_kernel, step_bias, log_rate,
    skip_gain, group_gain, out_weight, second_gain, routes, route_logits, expert_gate, expert_up,
    expert_down, dense_up, dense_down, dense_gate,
):
    near = [
        tokens, first_gain[None], step_weight.T, conv_state.transpose(1, 0, 2), conv_proj_state,
        conv_kernel, conv_proj_kernel, step_bias[None], log_rate[None], skip_gain[None],
        group_gain[None], second_gain[None], routes, route_logits, dense_up.T, dense_down,
        dense_gate[None],
    ]
    far = [
        out_weight.T, head_state, gate_weight, inner_weight, write_weight, read_weight, expert_gate,
        expert_up, expert_down,
    ]
    vmem = pl.BlockSpec(memory_space=pltpu.VMEM)
    anywhere = pl.BlockSpec(memory_space=pltpu.HBM)
    V = pltpu.VMEM
    outs = (
        jax.ShapeDtypeStruct((1, 2048), BF16),
        jax.ShapeDtypeStruct((3, 2, 1024), BF16),
        jax.ShapeDtypeStruct((2, 3, 2, 256), BF16),
        jax.ShapeDtypeStruct((2, 16, 64, 128), F32),
    )
    results = pl.pallas_call(
        layer_kernel,
        out_shape=tuple(V(o.shape, o.dtype) for o in outs),
        in_specs=[anywhere] * (len(near) + len(far)),
        out_specs=(vmem, vmem, vmem, vmem),
        scratch_shapes=[
            *[V(a.shape, a.dtype) for a in near],
            V((2048, 256), BF16), V((2048, 256), BF16),
            V((2048, 512), BF16), V((2048, 512), BF16), V((512, 2048), BF16),
            V((NX, 16, 1024), BF16), V((NX, 16, 1024), BF16),
            V((16, 2, 128), BF16), V((NZY, 2, 128), BF16),
            V((NZY, 2, 1024), BF16), V((NZY, 2, 1024), BF16),
            V((NZY, 2, 1024), BF16), V((NZY, 2, 1024), BF16),
            V((128, 2, 256), BF16), V((2, 8, 16, 1024), BF16), V((2, NZ, 2, 1024), BF16),
            V((16, 128), BF16), V((8, 16, 128), BF16), V((NZ, 2, 2048), BF16), V((2, 1024), BF16),
            V((2, 1024), BF16),
            V((2, NYX, 16, 512), BF16), V((16, 1024), BF16), V((16, 256), BF16), V((16, 256), BF16),
            V((32, 1024), BF16), V((32, 1024), BF16),
            V((NYX, 16, WIDE), BF16), V((NYX, 16, WIDE), BF16), V((NZ, 2, WIDE), BF16),
            V((2 * NZ, 2, WIDE), BF16), V((256, 128), BF16), V((48, 1024), BF16),
            V((16, 1024), BF16), V((NY, 64, 64), F32), V((32, 256), F32), V((32, 256), F32),
            V((2, 32, 512), BF16), V((2, 32, 512), BF16), V((NY, 64, WIDE), F32),
            V((256, 256), BF16), V((32, 256), BF16), V((NZ, 32, 1024 - WIDE), BF16),
            V((NZ, 32, 1024 - WIDE), BF16), V((NYX, 2, 1024 - WIDE), BF16),
            V((2 * NYX, 2, 1024 - WIDE), BF16), V((32, 256), F32),
            pltpu.SemaphoreType.DMA((8,)), pltpu.SemaphoreType.DMA((24,)),
            pltpu.SemaphoreType.DMA((24,)), pltpu.SemaphoreType.DMA((2 * NY,)),
            pltpu.SemaphoreType.DMA((2,)),
        ],
        compiler_params=pltpu.CompilerParams(
            collective_id=0, has_side_effects=True, vmem_limit_bytes=56 * 1024 * 1024
        ),
        cost_estimate=pl.CostEstimate(flops=2 * 10**9, bytes_accessed=16 * 2**20, transcendentals=10**5),
        name="layer",
    )(*near, *far)
    results = [pltpu.with_memory_space_constraint(r, V) for r in results]
    layer_out, conv_out, conv_proj_out, state_out = pl.pallas_call(
        write_kernel,
        out_shape=outs,
        in_specs=[vmem] * 4,
        out_specs=[anywhere] * 4,
        scratch_shapes=[pltpu.SemaphoreType.DMA((4,))],
        name="write",
    )(*results)
    return (layer_out, state_out, conv_out.transpose(1, 0, 2), conv_proj_out)


def solution(mesh):
    torus = Mesh(mesh.devices.reshape(NZ, NY, NX, mesh.shape["tp"]), EP_TP)
    return jax.shard_map(
        local,
        mesh=torus,
        in_specs=(
            P(EP, None), P(EP, "tp", None, None), P(EP, None, "tp"), P(EP, None, None, "tp"), P(),
            P(EP, "tp"), P(EP, "tp"), P(None, "tp"), P(None, "tp"), P(None, "tp"), P(None, "tp"),
            P(None, None, "tp"), P("tp"), P("tp"), P("tp"), P("tp"), P("tp", EP), P(), P(EP, None),
            P(EP, None), P(EP, None, "tp"), P(EP, None, "tp"), P(EP, "tp", None), P(None, EP_TP),
            P(EP_TP, None), P(),
        ),
        out_specs=(
            P(EP_TP, None), P(EP, "tp", None, None), P(EP, None, "tp"), P(EP, None, None, "tp"),
        ),
        check_vma=False,
    )
```
